32 devices in a mesh: ep: 4 (over y, x), tp: 8 (over z, core).
Axes of the slice: x: 2, y: 2, z: 4, core: 2. Of those that a mesh axis runs over, the one named last changes fastest.
Arguments:
- mixer_input: bfloat16 [6144, 1024], P(('ep', 'tp')), may hold values from -6 to 6
- mixer_gain: float32 [1024], replicated, may hold values from 0.1 to 1.9
- group_weight: bfloat16 [4, 256, 256], replicated, may hold values from -0.375 to 0.375
- mixer_scale: float32 [1024], replicated, may hold values from 0.1 to 1.9
- expert_input: bfloat16 [6144, 1024], P(('ep', 'tp')), may hold values from -6 to 6
- expert_gain: float32 [1024], replicated, may hold values from 0.1 to 1.9
- routes: int32 [6144, 2], P(('ep', 'tp')), may hold values from 0 to 3, all different within a row; in each aligned block of 192 rows (0 to 191, 192 to 383, ...) at most 144 rows name the same one
- route_weight: float32 [6144, 2], P(('ep', 'tp')), may hold values from 0.2 to 1
- w_gate: bfloat16 [4, 1024, 4096], P('ep', None, 'tp'), may hold values from -0.1875 to 0.1875
- w_up: bfloat16 [4, 1024, 4096], P('ep', None, 'tp'), may hold values from -0.1875 to 0.1875
- w_down: bfloat16 [4, 4096, 1024], P('ep', 'tp'), may hold values from -0.09375 to 0.09375
Outputs:
- mixer_out: bfloat16 [6144, 1024], P(('ep', 'tp'))
- expert_out: bfloat16 [6144, 1024], P(('ep', 'tp'))
The draws below stay inside these ranges and needn't reach their ends.
Inputs may be any that keep to these rules, and one draw needn't show every extreme that they name: `routes`: each row names 2 different experts. Among the rows of one device no expert is named by more than 144 rows, and in some device's rows some expert is named exactly 144 times.
All inputs are finite; a program needn't handle non-finite values.
Results may differ from the reference program's by a relative error of at most 0.0076.
Values may be sent and summed in bfloat16 or wider, within the bound.
A program may use at most 128 MiB of HBM per device.

```python
import math
import jax
import jax.numpy as jnp
import numpy as np
from jax import lax

D = 1024
GROUP_WIDTH = 256
FFE = 4096
TOPK = 2
TOK_DEV = 192
EXPERTS = 4
CAP = 144
TOKENS = 6144
N_TP = 8
DEVICES = 32


def block_levels(rng, dims, pieces, low, largest):
    factor_of = 1.0
    for dim, blocks in pieces:
        heights = jax.random.uniform(jax.random.fold_in(jax.random.fold_in(rng, 6), dim), (blocks,), jnp.float32, low / len(pieces), largest / len(pieces))
        factor_of = factor_of * jnp.repeat(jnp.exp(heights), dims[dim] // blocks).reshape((-1,) + (1,) * (len(dims) - 1 - dim))
    return factor_of


def deal_out(own_key, own, number, rows, amount, top, bound, lean):
    ranking = jax.random.permutation(own_key, amount)
    crowded, ordinary = shares(amount, rows * top, bound, lean, True), shares(amount, rows * top, bound, lean, False)
    places = jnp.arange(amount)

    def named(tallies, turn):
        used = int((tallies > 0).sum())
        fixed = max(1, used // 4)
        passed = fixed + (places - fixed + turn * (used - fixed)) % max(1, amount - fixed)
        return jnp.zeros((amount,), jnp.int32).at[ranking[jnp.where(places < fixed, places, passed)]].set(jnp.asarray(tallies, jnp.int32))

    tallies = jnp.where(number % 4 == 0, named(crowded, number // 4), named(ordinary, number - number // 4 - 1))
    mixed = jax.random.permutation(jax.random.fold_in(own, 3), amount)
    giver, taker = mixed[0:amount // 2 * 2:2], mixed[1:amount // 2 * 2:2]
    room = jnp.minimum(tallies[giver] - 1, bound - tallies[taker]) // 2
    room = jnp.where((giver == ranking[0]) | (taker == ranking[0]) | (tallies[taker] == 0), 0, jnp.maximum(room, 0))
    passed = jax.random.randint(jax.random.fold_in(own, 4), (amount // 2,), 0, 1 << 20) % (room + 1)
    tallies = tallies.at[giver].add(-passed).at[taker].add(passed)
    labels = jnp.searchsorted(jnp.cumsum(tallies), jnp.arange(rows * top), side="right").astype(jnp.int32)
    listing = labels.reshape(top, rows).T
    listing = listing[jax.random.permutation(jax.random.fold_in(own, 1), rows)]
    turn = jax.random.randint(jax.random.fold_in(own, 2), (rows, 1), 0, top)
    return jnp.take_along_axis(listing, (jnp.arange(top)[None, :] + turn) % top, axis=1)


def shares(count, total, most, lean, full):
    portions = [(1 << 20) // math.isqrt(rank ** lean) + 1 for rank in range(1, count + 1)]
    largest = most if full else min(most, max(-(-total // count), total * portions[0] // sum(portions)))
    least = 1 if total - largest >= count - 1 else 0
    given, spare = [largest] + [least] * (count - 1), total - largest - least * (count - 1)
    while spare > 0:
        free = [i for i in range(1, count) if given[i] < largest] or [i for i in range(1, count) if given[i] < most]
        pool, budget = sum([portions[i] for i in free]), spare
        for i in free:
            more = min(most - given[i], max(1, budget * portions[i] // pool), spare)
            given[i] = given[i] + more
            spare = spare - more
    return np.array(given)


def normal_values(stream_key, dims, width, bound, shards=(), kind=jnp.bfloat16):
    values = jax.random.normal(stream_key, dims, jnp.float32) * width
    if len(shards) > 0:
        values = block_levels(stream_key, dims, shards, -0.22, 0.18) * values
    return jnp.clip(values, min=-bound, max=bound).astype(kind)


def setup_inputs(seed: int = 0) -> dict:
    key_of = jax.random.split(jax.random.key(seed), 12)
    mixer_input = normal_values(key_of[0], (TOKENS, D), 1.0, 6.0, ((0, 32),))
    mixer_gain = jnp.clip(1.0 + 0.18 * jax.random.normal(key_of[1], (D,), jnp.float32), 0.1, 1.9)
    group_weight = normal_values(key_of[2], (4, GROUP_WIDTH, GROUP_WIDTH), GROUP_WIDTH ** -0.5, 0.375)
    mixer_scale = jnp.clip(1.0 + 0.18 * jax.random.normal(key_of[3], (D,), jnp.float32), 0.1, 1.9)
    expert_input = normal_values(key_of[4], (TOKENS, D), 1.0, 6.0, ((0, 32),))
    expert_gain = jnp.clip(1.0 + 0.18 * jax.random.normal(key_of[5], (D,), jnp.float32), 0.1, 1.9)
    routes_keys = jax.random.split(jax.random.fold_in(key_of[6], 1), TOKENS // TOK_DEV)
    routes_turns = jax.random.permutation(jax.random.fold_in(key_of[6], 3), TOKENS // TOK_DEV)
    routes = jax.vmap(lambda own, number: deal_out(jax.random.fold_in(key_of[6], 2), own, number, TOK_DEV, EXPERTS, TOPK, CAP, 2))(routes_keys, routes_turns).reshape((TOKENS, TOPK))
    route_weight = jnp.clip(0.2 + 0.8 * jax.random.uniform(key_of[7], (TOKENS, TOPK), jnp.float32) ** block_levels(key_of[7], (TOKENS, TOPK), ((0, 32),), -0.2, 0.2), 0.2, 1.0)
    w_gate = normal_values(key_of[8], (EXPERTS, D, FFE), D ** -0.5, 0.1875, ((0, 4), (2, 8)))
    w_up = normal_values(key_of[9], (EXPERTS, D, FFE), D ** -0.5, 0.1875, ((0, 4), (2, 8)))
    w_down = normal_values(key_of[10], (EXPERTS, FFE, D), FFE ** -0.5, 0.09375, ((0, 4), (1, 8)))
    return dict(mixer_input=mixer_input, mixer_gain=mixer_gain, group_weight=group_weight, mixer_scale=mixer_scale, expert_input=expert_input, expert_gain=expert_gain, routes=routes, route_weight=route_weight, w_gate=w_gate, w_up=w_up, w_down=w_down)


epsilon = 1e-06

def normalize(row_values, gain):
    values = row_values.astype(jnp.float32)
    scaled = values * lax.rsqrt(lax.optimization_barrier(jnp.mean(values * values, axis=-1, keepdims=True)) + epsilon)
    return (scaled * gain).astype(jnp.bfloat16)

def pool_groups(padded, start_row, row_count, seq_length):
    group_width = padded.shape[1] // 4
    position = start_row + jnp.arange(row_count, dtype=jnp.int32)
    centre = padded[8:8 + row_count]
    pooled_parts = []
    for group_index in range(4):
        window = 2 ** (group_index + 1)
        reach_left = window // 2
        reach_right = window - 1 - reach_left
        group_cols = padded[:, group_index * group_width:(group_index + 1) * group_width]
        window_sum = group_cols[8 - reach_left:8 - reach_left + row_count]
        for offset in range(1 - reach_left, reach_right + 1):
            window_sum = window_sum + group_cols[8 + offset:8 + offset + row_count]
        cover = (jnp.minimum(position + reach_right + 1, seq_length) - jnp.maximum(position - reach_left, 0)).astype(jnp.float32)
        pooled_parts.append(window_sum / cover[:, None] - centre[:, group_index * group_width:(group_index + 1) * group_width])
    return jnp.stack(pooled_parts, axis=1).astype(jnp.bfloat16)

def reference(mixer_input, mixer_gain, group_weight, mixer_scale, expert_input, expert_gain, routes, route_weight, w_gate, w_up, w_down):
    normed = normalize(mixer_input, mixer_gain)
    padded = jnp.pad(normed.astype(jnp.float32), ((8, 8), (0, 0)))
    pooled = pool_groups(padded, 0, TOKENS, TOKENS)
    mixed_groups = jnp.einsum('tgi,gio->tgo', pooled.astype(jnp.float32), group_weight.astype(jnp.float32))
    mixer_out = (mixed_groups.reshape(TOKENS, D) * mixer_scale).astype(jnp.bfloat16)
    expert_normed = normalize(expert_input, expert_gain)
    flat_route = routes.reshape(-1).astype(jnp.int32)
    flat_weight = route_weight.reshape(-1)
    most_rows = DEVICES * CAP
    block_width = FFE // N_TP

    def one_expert(running_out, inputs):
        gate_w, up_w, down_w, expert_index = inputs
        matches = flat_route == expert_index
        chosen = jnp.nonzero(matches, size=most_rows, fill_value=0)[0].astype(jnp.int32)
        live_rows = (jnp.arange(most_rows, dtype=jnp.int32) < jnp.sum(matches.astype(jnp.int32))).astype(jnp.float32)
        token_index = chosen // TOPK
        row_values = jnp.take(expert_normed, token_index, axis=0)
        gate_part = jnp.dot(row_values, gate_w, preferred_element_type=jnp.float32)
        up_part = jnp.dot(row_values, up_w, preferred_element_type=jnp.float32)
        hidden = (jax.nn.silu(gate_part) * up_part).astype(jnp.bfloat16)
        hidden_blocks = jnp.transpose(hidden.reshape(most_rows, N_TP, block_width), (1, 0, 2))
        weight_blocks = down_w.reshape(N_TP, block_width, D)

        def add_block(running, block_pair):
            hidden_block, weight_block = block_pair
            block_partial = lax.optimization_barrier(jnp.dot(hidden_block, weight_block, preferred_element_type=jnp.float32).astype(jnp.bfloat16))
            return (running + block_partial.astype(jnp.float32), None)
        summed, _ = lax.scan(add_block, jnp.zeros((most_rows, D), jnp.float32), (hidden_blocks, weight_blocks))
        expert_result = lax.optimization_barrier(summed.astype(jnp.bfloat16)).astype(jnp.float32)
        weights_here = jnp.take(flat_weight, chosen) * live_rows
        return (running_out.at[token_index].add(weights_here[:, None] * expert_result), None)
    total_out, _ = lax.scan(one_expert, jnp.zeros((TOKENS, D), jnp.float32), (w_gate, w_up, w_down, jnp.arange(EXPERTS, dtype=jnp.int32)))
    return (mixer_out, total_out.astype(jnp.bfloat16))
```

```python
import functools
import math

import jax
import jax.numpy as jnp
from jax import lax
from jax.experimental import pallas as pl
from jax.experimental.pallas import tpu as pltpu
from jax.sharding import PartitionSpec as P

epsilon = 1e-06
vmem_share = 2**24


def padded_2(value, sides, width):
    for axis, dim in sides:
        size, length = (lax.axis_size(axis), value.shape[dim])
        up = [(i, (i + 1) % size) for i in range(size - 1)]
        down = [(j, i) for i, j in up]
        last = lax.slice_in_dim(value, length - width, length, axis=dim)
        leading = lax.slice_in_dim(value, 0, width, axis=dim)
        before = lax.ppermute(last, axis, up)
        after = lax.ppermute(leading, axis, down)
        value = jnp.concatenate([before, value, after], axis=dim)
    return value


def normalize(row_values, gain):
    values = row_values.astype(jnp.float32)
    scaled = values * lax.rsqrt(jnp.mean(values * values, axis=-1, keepdims=True) + epsilon)
    return (scaled * gain).astype(jnp.bfloat16)


def pool_groups(padded, start_row, row_count, seq_length):
    group_width = padded.shape[1] // 4
    position = start_row + jnp.arange(row_count, dtype=jnp.int32)
    centre = padded[8 : 8 + row_count]
    pooled_parts = []
    for group_index in range(4):
        window = 2 ** (group_index + 1)
        reach_left = window // 2
        reach_right = window - 1 - reach_left
        group_cols = padded[:, group_index * group_width : (group_index + 1) * group_width]
        window_sum = group_cols[8 - reach_left : 8 - reach_left + row_count]
        for offset in range(1 - reach_left, reach_right + 1):
            window_sum = window_sum + group_cols[8 + offset : 8 + offset + row_count]
        cover = (
            jnp.minimum(position + reach_right + 1, seq_length)
            - jnp.maximum(position - reach_left, 0)
        ).astype(jnp.float32)
        pooled_parts.append(
            window_sum / cover[:, None]
            - centre[:, group_index * group_width : (group_index + 1) * group_width]
        )
    return jnp.stack(pooled_parts, axis=1).astype(jnp.bfloat16)


def mixer(mixer_input, mixer_gain, group_weight, mixer_scale):
    row_count = mixer_input.shape[0]
    normed = normalize(mixer_input, mixer_gain)
    padded = padded_2(normed, ((("ep", "tp"), 0),), 8)
    start_row = lax.axis_index(("ep", "tp")) * row_count
    seq_length = row_count * lax.axis_size(("ep", "tp"))
    pooled = pool_groups(padded.astype(jnp.float32), start_row, row_count, seq_length)
    mixed_groups = jnp.einsum(
        "tgi,gio->tgo", pooled, group_weight, preferred_element_type=jnp.float32
    )
    return (mixed_groups.reshape(row_count, -1) * mixer_scale).astype(jnp.bfloat16)


def routed_plan(expert_input, expert_gain, routes, route_weight, w_gate, w_up, w_down):
    row_count = expert_input.shape[0]
    top_count = routes.shape[1]
    experts = lax.axis_size("ep") * w_gate.shape[0]
    capacity = 3 * top_count * row_count // (2 * experts)
    normed = normalize(expert_input, expert_gain)
    flat_route = routes.reshape(-1)
    onehot = (flat_route[:, None] == jnp.arange(experts, dtype=jnp.int32)[None, :]).astype(
        jnp.int32
    )
    before = jnp.cumsum(onehot, axis=0) - onehot
    slot_index = flat_route * capacity + jnp.sum(before * onehot, axis=1)
    places = (
        slot_index.reshape(row_count, top_count)[None, :, :]
        == jnp.arange(experts * capacity, dtype=jnp.int32)[:, None, None]
    )
    dispatch = jnp.any(places, axis=2).astype(jnp.bfloat16)
    outgoing = jnp.dot(dispatch, normed, preferred_element_type=jnp.float32).astype(jnp.bfloat16)
    arrived = lax.all_to_all(outgoing, "ep", split_axis=0, concat_axis=0, tiled=True)
    down_w = w_down[0]
    paired = jnp.stack((w_gate[0], w_up[0]), axis=0)
    portion = lax.all_gather(paired, "tp", axis=2, tiled=True)
    gate_part = jnp.dot(arrived, portion[0], preferred_element_type=jnp.float32)
    up_part = jnp.dot(arrived, portion[1], preferred_element_type=jnp.float32)
    hidden = (jax.nn.silu(gate_part) * up_part).astype(jnp.bfloat16)
    block_width = down_w.shape[0]
    portion = lax.all_gather(down_w, "tp", axis=0, tiled=True)
    blocks = portion.shape[0] // block_width
    hidden_part = hidden
    hidden_part = hidden_part.reshape(hidden_part.shape[0], blocks, block_width)
    block_terms = jnp.einsum(
        "rkf,kfd->krd",
        hidden_part,
        portion.reshape(blocks, block_width, portion.shape[1]),
        preferred_element_type=jnp.float32,
    )
    rounded = lax.optimization_barrier(block_terms.astype(jnp.bfloat16)).astype(jnp.float32)
    result = jnp.sum(rounded, axis=0)
    returned = lax.all_to_all(
        result.astype(jnp.bfloat16), "ep", split_axis=0, concat_axis=0, tiled=True
    )
    picked = (
        jnp.take(returned, slot_index, axis=0).astype(jnp.float32).reshape(row_count, top_count, -1)
    )
    expert_out = jnp.sum(picked * route_weight[:, :, None], axis=1).astype(jnp.bfloat16)
    return expert_out


def slots(routes, route_weight, experts):
    chosen = routes[:, :, None] == jnp.arange(experts, dtype=jnp.int32)[None, None, :]
    named = jnp.any(chosen, axis=1)
    weight = jnp.sum(jnp.where(chosen, route_weight[:, :, None], 0.0), axis=1)
    rows = routes.shape[0]
    earlier = jnp.arange(rows)[None, :] < jnp.arange(rows)[:, None]
    place = jnp.dot(
        earlier.astype(jnp.bfloat16), named.astype(jnp.bfloat16), preferred_element_type=jnp.float32
    )
    place = jnp.where(named, place, -1.0)
    high = lax.reduce_precision(weight, 8, 7)
    return jnp.concatenate([place, high, weight - high], axis=1).T.astype(jnp.bfloat16)


def near_first(length):
    return [sorted(range(length), key=lambda other: abs(other - at)) for at in range(length)]


def stream_kernel(
    depth, capacity, experts,
    token_ref, gate_ref, up_ref, down_ref, out_ref,
    tok, blk, part, from_core, out_right, out_left, out_far, relay_right, relay_left,
    from_right, from_left, local, dense, dense_above, dense_below,
    far_above, far_below, home_left, home_right, far_back,
    send_sem, recv_sem, local_sem,
):
    column, line = lax.axis_index("ep"), lax.axis_index("tp")
    level, core = line // 2, line % 2
    other = 1 - core
    tall = token_ref.shape[0]
    rows = out_ref.shape[0]
    low = -(-capacity // 32) * 16
    high = capacity - low
    piece = math.gcd(rows, capacity)
    right_column, left_column, far_column = (2 * column + 1) % 5, (3 * column + 2) % 5, 3 - column
    right, left = (right_column, line), (left_column, line)
    beside = (column, level * 2 + other)
    above, below = (column, line + 2), (column, line - 2)
    has_above, has_below = level < depth - 1, level > 0
    f32, bf16 = jnp.float32, jnp.bfloat16

    def level_of(step):
        value = 0
        for at, order in enumerate(near_first(depth)):
            for turn, there in enumerate(order):
                value = value + there * jnp.where((level == at) & (step == turn), 1, 0)
        return value

    def link(src, dst, kind, at, target):
        return pltpu.make_async_remote_copy(
            src_ref=src, dst_ref=dst, send_sem=send_sem.at[kind, at],
            recv_sem=recv_sem.at[kind, at], device_id=target,
            device_id_type=pl.DeviceIdType.MESH,
        )

    def up(at):
        return link(tok.at[at], tok.at[at], 0, at, above)

    def down(at):
        return link(tok.at[at], tok.at[at], 1, at, below)

    def to_right(at):
        return link(out_right.at[at], blk.at[at, 1, core], 2, at, right)

    def to_left(at):
        return link(out_left.at[at], blk.at[at, 2, core], 3, at, left)

    def far_right():
        return link(out_far.at[pl.ds(0, low)], relay_right, 4, 0, right)

    def far_left():
        return link(out_far.at[pl.ds(low, high)], relay_left, 5, 0, left)

    def on_right():
        return link(relay_right, blk.at[level, 3, core, pl.ds(0, low)], 6, 0, right)

    def on_left():
        return link(relay_left, blk.at[level, 3, core, pl.ds(low, high)], 7, 0, left)

    def far_up(at):
        return link(blk.at[at, 3, core], blk.at[at, 3, core], 8, at, above)

    def far_down(at):
        return link(blk.at[at, 3, core], blk.at[at, 3, core], 9, at, below)

    def share(at, q):
        return link(blk.at[at, q, core], blk.at[at, q, core], 10 + q, at, beside)

    def shared_in(at, q):
        return link(blk.at[at, q, other], blk.at[at, q, other], 10 + q, at, beside)

    def give(at, q):
        return link(part.at[at, q, other], from_core.at[at, q], 14 + q, at, beside)

    def back_left(at):
        return link(part.at[at, 1, core], from_right.at[at], 18, at, left)

    def back_right(at):
        return link(part.at[at, 2, core], from_left.at[at], 19, at, right)

    def sum_down(at):
        return link(dense.at[at], dense_above.at[at], 20, at, below)

    def sum_up(at):
        return link(dense.at[at], dense_below.at[at], 21, at, above)

    def far_sum_down(at):
        return link(part.at[at, 3, core], far_above.at[at], 22, at, below)

    def far_sum_up(at):
        return link(part.at[at, 3, core], far_below.at[at], 23, at, above)

    def home_low():
        return link(part.at[level, 3, core, pl.ds(0, low)], home_left, 24, 0, left)

    def home_high():
        return link(part.at[level, 3, core, pl.ds(low, high)], home_right, 25, 0, right)

    def last_low():
        return link(home_left, far_back.at[pl.ds(0, low)], 26, 0, left)

    def last_high():
        return link(home_right, far_back.at[pl.ds(low, high)], 27, 0, right)

    barrier = pltpu.get_barrier_semaphore()

    def greet(target):
        pl.semaphore_signal(
            barrier, inc=1, device_id=target, device_id_type=pl.DeviceIdType.MESH
        )

    greet(right)
    greet(left)
    greet(beside)
    pl.when(has_above)(lambda: greet(above))
    pl.when(has_below)(lambda: greet(below))
    own_copy = pltpu.make_async_copy(token_ref, tok.at[level], local_sem)
    own_copy.start()
    own_copy.wait()
    pl.semaphore_wait(barrier, 3 + jnp.where(has_above, 1, 0) + jnp.where(has_below, 1, 0))

    def table(at):
        listed = tok[at, pl.ds(rows, tall - rows), pl.ds(0, rows)].astype(f32)
        listing = lax.broadcasted_iota(jnp.int32, listed.shape, 0)
        index = lax.broadcasted_iota(jnp.int32, (capacity, rows), 0).astype(f32)

        def row_of(at_row):
            return jnp.sum(jnp.where(listing == at_row, listed, 0.0), axis=0, keepdims=True)

        def hits(expert):
            return index == row_of(expert)

        return row_of, hits

    def picked(at, chosen):
        _, hits = table(at)
        picks = [jnp.where(hits(expert), 1.0, 0.0).astype(bf16) for expert in chosen]
        return jnp.dot(
            jnp.concatenate(picks, axis=0), tok[at, pl.ds(0, rows)], preferred_element_type=f32
        ).astype(bf16)

    def placed(at, chosen, results):
        row_of, hits = table(at)
        total = None
        for kind in (1, 2):
            weights = [
                jnp.where(hits(expert), row_of(kind * experts + expert), 0.0).astype(bf16)
                for expert in chosen
            ]
            term = lax.dot_general(
                jnp.concatenate(weights, axis=0), results,
                (((0,), (0,)), ((), ())), preferred_element_type=f32,
            )
            total = term if total is None else total + term
        return total

    def compute(at, q):
        gathered = jnp.concatenate([blk[at, q, 0], blk[at, q, 1]], axis=0)
        gate_part = jnp.dot(gathered, gate_ref[...], preferred_element_type=f32)
        up_part = jnp.dot(gathered, up_ref[...], preferred_element_type=f32)
        hidden = (gate_part / (1.0 + jnp.exp(-gate_part)) * up_part).astype(bf16)
        partial = jnp.dot(hidden, down_ref[...], preferred_element_type=f32).astype(bf16)
        for lane in range(2):
            part[at, q, lane] = partial[lane * capacity : (lane + 1) * capacity]

    def by_piece(count, body):
        def one(i, carry):
            body(pl.ds(pl.multiple_of(i * piece, piece), piece))
            return carry

        lax.fori_loop(0, count // piece, one, 0)

    def paired(at, q):
        give(at, q).wait_recv()

        def body(span):
            total = part[at, q, core, span].astype(f32) + from_core[at, q, span].astype(f32)
            part[at, q, core, span] = total.astype(bf16)

        by_piece(capacity, body)

    def with_incoming(above_too, below_too, action):
        both = above_too & below_too
        pl.when(both)(lambda: action(True, True))
        pl.when(above_too & jnp.logical_not(both))(lambda: action(True, False))
        pl.when(below_too & jnp.logical_not(both))(lambda: action(False, True))
        pl.when(jnp.logical_not(above_too | below_too))(lambda: action(False, False))

    def far_total(at):
        give(at, 3).wait_recv()
        above_too, below_too = (at <= level) & has_above, (at >= level) & has_below
        pl.when(above_too)(lambda: far_sum_down(at).wait_recv())
        pl.when(below_too)(lambda: far_sum_up(at).wait_recv())

        def action(from_up, from_down):
            def body(span):
                total = part[at, 3, core, span].astype(f32) + from_core[at, 3, span].astype(f32)
                if from_up:
                    total = total + far_above[at, span].astype(f32)
                if from_down:
                    total = total + far_below[at, span].astype(f32)
                part[at, 3, core, span] = total.astype(bf16)

            by_piece(capacity, body)

        with_incoming(above_too, below_too, action)

    def dense_total(at):
        above_too, below_too = (at <= level) & has_above, (at >= level) & has_below
        pl.when(above_too)(lambda: sum_down(at).wait_recv())
        pl.when(below_too)(lambda: sum_up(at).wait_recv())

        def action(from_up, from_down):
            def body(span):
                total = local[at, span]
                if from_up:
                    total = total + dense_above[at, span].astype(f32)
                if from_down:
                    total = total + dense_below[at, span].astype(f32)
                dense[at, span] = total.astype(bf16)

            by_piece(rows, body)

        with_incoming(above_too, below_too, action)

    def expand(at):
        give(at, 0).wait_recv()
        back_left(at).wait_recv()
        back_right(at).wait_recv()
        own = (part[at, 0, core].astype(f32) + from_core[at, 0].astype(f32)).astype(bf16)
        results = jnp.concatenate([own, from_right[at], from_left[at]], axis=0)
        local[at] = placed(at, (column, right_column, left_column), results)

    def arrive(turn):
        at = level_of(turn)
        pl.when(at < level)(lambda: up(at).wait_recv())
        pl.when(at > level)(lambda: down(at).wait_recv())
        pl.when((at <= level) & has_above)(lambda: up(at).start())
        pl.when((at >= level) & has_below)(lambda: down(at).start())

        @pl.when(at == level)
        def _():
            out_far[...] = picked(at, (far_column,))
            far_right().start()
            far_left().start()

        sent = picked(at, (right_column, left_column, column))
        out_right[at] = sent[:capacity]
        out_left[at] = sent[capacity : 2 * capacity]
        to_right(at).start()
        to_left(at).start()
        blk[at, 0, core] = sent[2 * capacity :]
        share(at, 0).start()

    def sides_in(at):
        to_right(at).wait_recv()
        share(at, 1).start()
        to_left(at).wait_recv()
        share(at, 2).start()

    def far_in(at):
        @pl.when(at == level)
        def _():
            on_right().wait_recv()
            on_left().wait_recv()

        pl.when(at < level)(lambda: far_up(at).wait_recv())
        pl.when(at > level)(lambda: far_down(at).wait_recv())
        pl.when((at <= level) & has_above)(lambda: far_up(at).start())
        pl.when((at >= level) & has_below)(lambda: far_down(at).start())
        share(at, 3).start()

    def relay():
        far_right().wait_recv()
        on_right().start()
        far_left().wait_recv()
        on_left().start()

    def stage(turn, carry):
        pl.when(turn < depth)(lambda: arrive(turn))

        def one(q, inner):
            step = turn - jnp.where(q > 0, 1, 0)

            @pl.when((step >= 0) & (step < depth))
            def _():
                at = level_of(step)
                pl.when(q == 1)(lambda: sides_in(at))
                pl.when(q == 3)(lambda: far_in(at))
                shared_in(at, q).wait_recv()
                compute(at, q)
                give(at, q).start()

                @pl.when(q == 2)
                def _():
                    paired(at, 1)
                    back_left(at).start()

                @pl.when(q == 3)
                def _():
                    paired(at, 2)
                    back_right(at).start()

            pl.when((q == 0) & (turn == 0))(relay)
            return inner

        lax.fori_loop(0, 4, one, 0)
        pl.when((turn >= 3) & (turn < depth + 2))(lambda: expand(level_of(turn - 2)))

        def chain(at, inner):
            climb = jnp.where(
                at < level, 2 * (depth - 1) - at - level, at + level
            ) + 2

            @pl.when((at != level) & (turn == climb))
            def _():
                far_total(at)
                pl.when(at < level)(lambda: far_sum_down(at).start())
                pl.when(at > level)(lambda: far_sum_up(at).start())
                dense_total(at)
                pl.when(at < level)(lambda: sum_down(at).start())
                pl.when(at > level)(lambda: sum_up(at).start())

            return inner

        lax.fori_loop(0, depth, chain, 0)
        return carry

    lax.fori_loop(0, 2 * depth, stage, 0)

    far_total(level)
    home_low().start()
    home_high().start()
    expand(level)
    dense_total(level)
    home_low().wait_recv()
    last_low().start()
    home_high().wait_recv()
    last_high().start()
    last_low().wait_recv()
    last_high().wait_recv()
    total = placed(level, (far_column,), far_back[...])
    out_ref[...] = (dense[level].astype(f32) + total).astype(bf16)

    def drain(at, carry):
        upward, downward = (at <= level) & has_above, (at >= level) & has_below
        for copy in (up, far_up):
            pl.when(upward)(lambda copy=copy: copy(at).wait_send())
        for copy in (down, far_down):
            pl.when(downward)(lambda copy=copy: copy(at).wait_send())
        for copy in (to_right, to_left, back_left, back_right):
            copy(at).wait_send()
        for q in range(4):
            share(at, q).wait_send()
            give(at, q).wait_send()
        for copy in (sum_down, far_sum_down):
            pl.when(at < level)(lambda copy=copy: copy(at).wait_send())
        for copy in (sum_up, far_sum_up):
            pl.when(at > level)(lambda copy=copy: copy(at).wait_send())
        return carry

    lax.fori_loop(0, depth, drain, 0)
    for copy in (
        far_right, far_left, on_right, on_left, home_low, home_high, last_low, last_high
    ):
        copy().wait_send()


def dense_plan(expert_input, expert_gain, routes, route_weight, w_gate, w_up, w_down):
    row_count, width = expert_input.shape
    experts = lax.axis_size("ep")
    depth = lax.axis_size("tp") // 2
    capacity = 3 * routes.shape[1] * row_count // (2 * experts)
    normed = normalize(expert_input, expert_gain)
    listed = slots(routes, route_weight, experts)
    pad = -(-3 * experts // 16) * 16
    listed = jnp.pad(listed, ((0, pad - 3 * experts), (0, width - row_count)))
    sent = jnp.concatenate([normed, listed], axis=0)
    bf16 = jnp.bfloat16
    low = -(-capacity // 32) * 16
    high = capacity - low
    vmem = pl.BlockSpec(memory_space=pltpu.VMEM)
    compact = pltpu.VMEM((depth, capacity, width), bf16)
    dense = pltpu.VMEM((depth, row_count, width), bf16)
    return pl.pallas_call(
        functools.partial(stream_kernel, depth, capacity, experts),
        out_shape=jax.ShapeDtypeStruct((row_count, width), bf16),
        in_specs=[vmem] * 4,
        out_specs=vmem,
        scratch_shapes=[
            pltpu.VMEM((depth, row_count + pad, width), bf16),
            pltpu.VMEM((depth, 4, 2, capacity, width), bf16),
            pltpu.VMEM((depth, 4, 2, capacity, width), bf16),
            pltpu.VMEM((depth, 4, capacity, width), bf16),
            compact,
            compact,
            pltpu.VMEM((capacity, width), bf16),
            pltpu.VMEM((low, width), bf16),
            pltpu.VMEM((high, width), bf16),
            compact,
            compact,
            pltpu.VMEM((depth, row_count, width), jnp.float32),
            dense,
            dense,
            dense,
            compact,
            compact,
            pltpu.VMEM((low, width), bf16),
            pltpu.VMEM((high, width), bf16),
            pltpu.VMEM((capacity, width), bf16),
            pltpu.SemaphoreType.DMA((28, depth)),
            pltpu.SemaphoreType.DMA((28, depth)),
            pltpu.SemaphoreType.DMA,
        ],
        compiler_params=pltpu.CompilerParams(
            collective_id=0, has_side_effects=True, vmem_limit_bytes=60 * 2**20
        ),
    )(sent, w_gate[0], w_up[0], w_down[0])


def on_device(
    mixer_input, mixer_gain, group_weight, mixer_scale,
    expert_input, expert_gain, routes, route_weight, w_gate, w_up, w_down,
):
    devices = lax.axis_size(("ep", "tp"))
    gathered_bytes = 2 * devices * expert_input.size
    square = lax.axis_size("ep") == 4
    plan = dense_plan if square and gathered_bytes <= vmem_share else routed_plan
    expert_out = plan(expert_input, expert_gain, routes, route_weight, w_gate, w_up, w_down)
    return (mixer(mixer_input, mixer_gain, group_weight, mixer_scale), expert_out)


def solution(mesh):
    placed = (
        P(("ep", "tp"), None),
        P(),
        P(),
        P(),
        P(("ep", "tp"), None),
        P(),
        P(("ep", "tp"), None),
        P(("ep", "tp"), None),
        P("ep", None, "tp"),
        P("ep", None, "tp"),
        P("ep", "tp", None),
    )
    return jax.shard_map(
        on_device,
        mesh=mesh,
        in_specs=placed,
        out_specs=(P(("ep", "tp"), None), P(("ep", "tp"), None)),
        check_vma=False,
    )
```

```python
import functools
import math

import jax
import jax.numpy as jnp
from jax import lax
from jax.experimental import pallas as pl
from jax.experimental.pallas import tpu as pltpu
from jax.sharding import PartitionSpec as P

epsilon = 1e-06
vmem_share = 2**24


def padded_2(value, sides, width):
    for axis, dim in sides:
        size, length = (lax.axis_size(axis), value.shape[dim])
        up = [(i, (i + 1) % size) for i in range(size - 1)]
        down = [(j, i) for i, j in up]
        last = lax.slice_in_dim(value, length - width, length, axis=dim)
        leading = lax.slice_in_dim(value, 0, width, axis=dim)
        before = lax.ppermute(last, axis, up)
        after = lax.ppermute(leading, axis, down)
        value = jnp.concatenate([before, value, after], axis=dim)
    return value


def normalize(row_values, gain):
    values = row_values.astype(jnp.float32)
    scaled = values * lax.rsqrt(jnp.mean(values * values, axis=-1, keepdims=True) + epsilon)
    return (scaled * gain).astype(jnp.bfloat16)


def pool_groups(padded, start_row, row_count, seq_length):
    group_width = padded.shape[1] // 4
    position = start_row + jnp.arange(row_count, dtype=jnp.int32)
    centre = padded[8 : 8 + row_count]
    pooled_parts = []
    for group_index in range(4):
        window = 2 ** (group_index + 1)
        reach_left = window // 2
        reach_right = window - 1 - reach_left
        group_cols = padded[:, group_index * group_width : (group_index + 1) * group_width]
        window_sum = group_cols[8 - reach_left : 8 - reach_left + row_count]
        for offset in range(1 - reach_left, reach_right + 1):
            window_sum = window_sum + group_cols[8 + offset : 8 + offset + row_count]
        cover = (
            jnp.minimum(position + reach_right + 1, seq_length)
            - jnp.maximum(position - reach_left, 0)
        ).astype(jnp.float32)
        pooled_parts.append(
            window_sum / cover[:, None]
            - centre[:, group_index * group_width : (group_index + 1) * group_width]
        )
    return jnp.stack(pooled_parts, axis=1).astype(jnp.bfloat16)


def mixer(mixer_input, mixer_gain, group_weight, mixer_scale):
    row_count = mixer_input.shape[0]
    normed = normalize(mixer_input, mixer_gain)
    padded = padded_2(normed, ((("ep", "tp"), 0),), 8)
    start_row = lax.axis_index(("ep", "tp")) * row_count
    seq_length = row_count * lax.axis_size(("ep", "tp"))
    pooled = pool_groups(padded.astype(jnp.float32), start_row, row_count, seq_length)
    mixed_groups = jnp.einsum(
        "tgi,gio->tgo", pooled, group_weight, preferred_element_type=jnp.float32
    )
    return (mixed_groups.reshape(row_count, -1) * mixer_scale).astype(jnp.bfloat16)


def routed_plan(expert_input, expert_gain, routes, route_weight, w_gate, w_up, w_down):
    row_count = expert_input.shape[0]
    top_count = routes.shape[1]
    experts = lax.axis_size("ep") * w_gate.shape[0]
    capacity = 3 * top_count * row_count // (2 * experts)
    normed = normalize(expert_input, expert_gain)
    flat_route = routes.reshape(-1)
    onehot = (flat_route[:, None] == jnp.arange(experts, dtype=jnp.int32)[None, :]).astype(
        jnp.int32
    )
    before = jnp.cumsum(onehot, axis=0) - onehot
    slot_index = flat_route * capacity + jnp.sum(before * onehot, axis=1)
    places = (
        slot_index.reshape(row_count, top_count)[None, :, :]
        == jnp.arange(experts * capacity, dtype=jnp.int32)[:, None, None]
    )
    dispatch = jnp.any(places, axis=2).astype(jnp.bfloat16)
    outgoing = jnp.dot(dispatch, normed, preferred_element_type=jnp.float32).astype(jnp.bfloat16)
    arrived = lax.all_to_all(outgoing, "ep", split_axis=0, concat_axis=0, tiled=True)
    down_w = w_down[0]
    paired = jnp.stack((w_gate[0], w_up[0]), axis=0)
    portion = lax.all_gather(paired, "tp", axis=2, tiled=True)
    gate_part = jnp.dot(arrived, portion[0], preferred_element_type=jnp.float32)
    up_part = jnp.dot(arrived, portion[1], preferred_element_type=jnp.float32)
    hidden = (jax.nn.silu(gate_part) * up_part).astype(jnp.bfloat16)
    block_width = down_w.shape[0]
    portion = lax.all_gather(down_w, "tp", axis=0, tiled=True)
    blocks = portion.shape[0] // block_width
    hidden_part = hidden
    hidden_part = hidden_part.reshape(hidden_part.shape[0], blocks, block_width)
    block_terms = jnp.einsum(
        "rkf,kfd->krd",
        hidden_part,
        portion.reshape(blocks, block_width, portion.shape[1]),
        preferred_element_type=jnp.float32,
    )
    rounded = lax.optimization_barrier(block_terms.astype(jnp.bfloat16)).astype(jnp.float32)
    result = jnp.sum(rounded, axis=0)
    returned = lax.all_to_all(
        result.astype(jnp.bfloat16), "ep", split_axis=0, concat_axis=0, tiled=True
    )
    picked = (
        jnp.take(returned, slot_index, axis=0).astype(jnp.float32).reshape(row_count, top_count, -1)
    )
    expert_out = jnp.sum(picked * route_weight[:, :, None], axis=1).astype(jnp.bfloat16)
    return expert_out


def slots(routes, route_weight, experts):
    chosen = routes[:, :, None] == jnp.arange(experts, dtype=jnp.int32)[None, None, :]
    named = jnp.any(chosen, axis=1)
    weight = jnp.sum(jnp.where(chosen, route_weight[:, :, None], 0.0), axis=1)
    rows = routes.shape[0]
    earlier = jnp.arange(rows)[None, :] < jnp.arange(rows)[:, None]
    place = jnp.dot(
        earlier.astype(jnp.bfloat16), named.astype(jnp.bfloat16), preferred_element_type=jnp.float32
    )
    place = jnp.where(named, place, -1.0)
    high = lax.reduce_precision(weight, 8, 7)
    return jnp.concatenate([place, high, weight - high], axis=1).T.astype(jnp.bfloat16)


ORDERS = (
    (
        ("D", 0, 1), ("D", 0, 0), ("X", 0, 0), ("Y", 0, 0), ("M", 0, 0), ("D", 1, 0), ("G", 0, 0),
        ("D", 1, 1), ("M", 1, 0), ("D", 2, 1), ("D", 2, 0), ("C", 0, 0), ("M", 2, 0), ("C", 2, 0),
        ("I", 0, 0), ("C", 0, 2), ("C", 0, 1), ("D", 3, 1), ("D", 3, 0), ("M", 3, 0), ("I", 2, 0),
        ("G", 1, 0), ("P", 0, 1), ("C", 2, 2), ("C", 1, 3), ("C", 2, 1), ("I", 3, 0), ("F", 1, 0),
        ("I", 1, 0), ("G", 2, 0), ("C", 3, 2), ("F", 1, 1), ("C", 2, 3), ("C", 3, 1), ("F", 2, 0),
        ("P", 3, 2), ("C", 1, 2), ("P", 2, 2), ("P", 3, 1), ("P", 2, 1), ("F", 2, 1), ("G", 3, 0),
        ("C", 3, 3), ("C", 1, 0), ("F", 3, 0), ("F", 3, 1), ("C", 3, 0), ("C", 0, 3), ("C", 1, 1),
        ("E", 3, 0), ("P", 1, 2), ("P", 1, 1), ("P", 0, 2), ("S", 3, 0), ("S", 3, 1), ("E", 2, 0),
        ("S", 2, 0), ("S", 2, 1), ("F", 0, 0), ("E", 1, 0), ("S", 1, 0), ("F", 0, 1), ("V", 0, 0),
        ("V", 0, 1), ("E", 0, 0), ("S", 1, 1), ("S", 0, 0), ("S", 0, 1), ("Z", 0, 0),
    ),
    (
        ("D", 1, 0), ("D", 1, 1), ("X", 1, 0), ("M", 1, 0), ("Y", 1, 0), ("D", 2, 0), ("D", 0, 0),
        ("D", 2, 1), ("I", 1, 0), ("D", 0, 1), ("M", 0, 0), ("D", 3, 0), ("C", 1, 1), ("D", 3, 1),
        ("M", 3, 0), ("I", 0, 0), ("G", 1, 0), ("C", 0, 1), ("P", 0, 1), ("C", 1, 3), ("G", 0, 0),
        ("I", 3, 0), ("G", 2, 0), ("C", 0, 3), ("C", 3, 2), ("M", 2, 0), ("C", 3, 1), ("P", 3, 2),
        ("C", 0, 2), ("G", 3, 0), ("P", 3, 1), ("C", 1, 2), ("C", 2, 0), ("C", 1, 0), ("C", 3, 3),
        ("I", 2, 0), ("C", 2, 3), ("P", 0, 2), ("P", 1, 1), ("C", 2, 2), ("C", 2, 1), ("C", 0, 0),
        ("P", 1, 2), ("F", 2, 0), ("F", 2, 1), ("C", 3, 0), ("F", 3, 0), ("F", 1, 0), ("P", 2, 2),
        ("F", 3, 1), ("P", 2, 1), ("F", 0, 0), ("E", 3, 0), ("S", 3, 0), ("E", 1, 0), ("E", 0, 0),
        ("F", 1, 1), ("V", 1, 0), ("F", 0, 1), ("S", 3, 1), ("E", 2, 0), ("S", 0, 0), ("S", 2, 0),
        ("S", 0, 1), ("S", 2, 1), ("V", 1, 1), ("S", 1, 0), ("S", 1, 1), ("Z", 1, 0),
    ),
)


def coded_orders(depth, kinds):
    base = len(kinds) * 4 * depth + 1
    per_word = 1
    while base ** (per_word + 1) < 2**31:
        per_word += 1
    idle = base - 1
    words = []
    for order in ORDERS:
        codes = [(kinds.index(kind) * depth + at) * 4 + q for kind, at, q in order]
        codes += [idle] * (-len(codes) % per_word)
        words.append([
            sum(code * base**n for n, code in enumerate(codes[first : first + per_word]))
            for first in range(0, len(codes), per_word)
        ])
    return words, per_word, base


def stream_kernel(
    depth, capacity, experts,
    token_ref, table_ref, gate_ref, up_ref, down_ref, out_ref,
    tok, tables, blk, part, from_core, out_right, out_left, out_far, relay_right, relay_left,
    from_right, from_left, local, dense, dense_above, dense_below,
    far_above, far_below, home_left, home_right, far_back,
    send_sem, recv_sem, local_sem,
):
    column, line = lax.axis_index("ep"), lax.axis_index("tp")
    level, core = line // 2, line % 2
    other = 1 - core
    rows = out_ref.shape[0]
    half = rows // 2
    low = -(-capacity // 32) * 16
    high = capacity - low
    piece = math.gcd(half, capacity)
    step_rows = math.gcd(low, high)
    right_column, left_column, far_column = (2 * column + 1) % 5, (3 * column + 2) % 5, 3 - column
    right, left = (right_column, line), (left_column, line)
    beside = (column, level * 2 + other)
    above, below = (column, line + 2), (column, line - 2)
    has_above, has_below = level < depth - 1, level > 0
    f32, bf16 = jnp.float32, jnp.bfloat16

    def link(src, dst, kind, at, target):
        return pltpu.make_async_remote_copy(
            src_ref=src, dst_ref=dst, send_sem=send_sem.at[kind, at],
            recv_sem=recv_sem.at[kind, at], device_id=target,
            device_id_type=pl.DeviceIdType.MESH,
        )

    def part_of(h):
        return pl.ds(pl.multiple_of(h * half, half), half)

    def up(at, h):
        return link(tok.at[at, part_of(h)], tok.at[at, part_of(h)], h, at, above)

    def down(at, h):
        return link(tok.at[at, part_of(h)], tok.at[at, part_of(h)], 2 + h, at, below)

    def table_up(at):
        return link(tables.at[at], tables.at[at], 4, at, above)

    def table_down(at):
        return link(tables.at[at], tables.at[at], 5, at, below)

    def to_right(at):
        return link(out_right.at[at], blk.at[at, 1, core], 6, at, right)

    def to_left(at):
        return link(out_left.at[at], blk.at[at, 2, core], 7, at, left)

    def far_right():
        return link(out_far.at[pl.ds(0, low)], relay_right, 8, 0, right)

    def far_left():
        return link(out_far.at[pl.ds(low, high)], relay_left, 9, 0, left)

    def on_right():
        return link(relay_right, blk.at[level, 3, core, pl.ds(0, low)], 10, 0, right)

    def on_left():
        return link(relay_left, blk.at[level, 3, core, pl.ds(low, high)], 11, 0, left)

    def far_up(at):
        return link(blk.at[at, 3, core], blk.at[at, 3, core], 12, at, above)

    def far_down(at):
        return link(blk.at[at, 3, core], blk.at[at, 3, core], 13, at, below)

    def share(at, q):
        return link(blk.at[at, q, core], blk.at[at, q, core], 14 + q, at, beside)

    def shared_in(at, q):
        return link(blk.at[at, q, other], blk.at[at, q, other], 14 + q, at, beside)

    def give(at, q):
        return link(part.at[at, q, other], from_core.at[at, q], 18 + q, at, beside)

    def back_left(at):
        return link(part.at[at, 1, core], from_right.at[at], 22, at, left)

    def back_right(at):
        return link(part.at[at, 2, core], from_left.at[at], 23, at, right)

    def sum_down(at, h):
        return link(dense.at[at, part_of(h)], dense_above.at[at, part_of(h)], 24 + h, at, below)

    def sum_up(at, h):
        return link(dense.at[at, part_of(h)], dense_below.at[at, part_of(h)], 26 + h, at, above)

    cuts = (pl.ds(0, low), pl.ds(low, high))

    def far_sum_down(at, h):
        return link(part.at[at, 3, core, cuts[h]], far_above.at[at, cuts[h]], 28 + h, at, below)

    def far_sum_up(at, h):
        return link(part.at[at, 3, core, cuts[h]], far_below.at[at, cuts[h]], 30 + h, at, above)

    def home_low():
        return link(part.at[level, 3, core, cuts[0]], home_left, 32, 0, left)

    def home_high():
        return link(part.at[level, 3, core, cuts[1]], home_right, 33, 0, right)

    def last_low():
        return link(home_left, far_back.at[cuts[0]], 34, 0, left)

    def last_high():
        return link(home_right, far_back.at[cuts[1]], 35, 0, right)

    barrier = pltpu.get_barrier_semaphore()

    def greet(target):
        pl.semaphore_signal(
            barrier, inc=1, device_id=target, device_id_type=pl.DeviceIdType.MESH
        )

    greet(right)
    greet(left)
    greet(beside)
    pl.when(has_above)(lambda: greet(above))
    pl.when(has_below)(lambda: greet(below))
    own_copy = pltpu.make_async_copy(token_ref, tok.at[level], local_sem)
    own_copy.start()
    own_copy.wait()
    own_table = pltpu.make_async_copy(table_ref, tables.at[level], local_sem)
    own_table.start()
    own_table.wait()
    pl.semaphore_wait(barrier, 3 + jnp.where(has_above, 1, 0) + jnp.where(has_below, 1, 0))

    def table(at):
        listed = tables[at, :, pl.ds(0, rows)].astype(f32)
        listing = lax.broadcasted_iota(jnp.int32, listed.shape, 0)
        index = lax.broadcasted_iota(jnp.int32, (capacity, rows), 0).astype(f32)

        def row_of(at_row):
            return jnp.sum(jnp.where(listing == at_row, listed, 0.0), axis=0, keepdims=True)

        def hits(expert):
            return index == row_of(expert)

        return row_of, hits

    def picked(at, chosen):
        _, hits = table(at)
        picks = [jnp.where(hits(expert), 1.0, 0.0).astype(bf16) for expert in chosen]
        return jnp.dot(
            jnp.concatenate(picks, axis=0), tok[at], preferred_element_type=f32
        ).astype(bf16)

    def placed(at, chosen, results):
        row_of, hits = table(at)
        total = None
        for kind in (1, 2):
            weights = [
                jnp.where(hits(expert), row_of(kind * experts + expert), 0.0).astype(bf16)
                for expert in chosen
            ]
            term = lax.dot_general(
                jnp.concatenate(weights, axis=0), results,
                (((0,), (0,)), ((), ())), preferred_element_type=f32,
            )
            total = term if total is None else total + term
        return total

    def compute(at, q):
        gathered = jnp.concatenate([blk[at, q, 0], blk[at, q, 1]], axis=0)
        gate_part = jnp.dot(gathered, gate_ref[...], preferred_element_type=f32)
        up_part = jnp.dot(gathered, up_ref[...], preferred_element_type=f32)
        hidden = (gate_part / (1.0 + jnp.exp(-gate_part)) * up_part).astype(bf16)
        partial = jnp.dot(hidden, down_ref[...], preferred_element_type=f32).astype(bf16)
        for lane in range(2):
            part[at, q, lane] = partial[lane * capacity : (lane + 1) * capacity]

    def by_piece(start, count, width, body):
        def one(i, carry):
            body(pl.ds(pl.multiple_of(start + i * width, width), width))
            return carry

        lax.fori_loop(0, count // width, one, 0)

    def paired(at, q):
        give(at, q).wait_recv()

        def body(span):
            total = part[at, q, core, span].astype(f32) + from_core[at, q, span].astype(f32)
            part[at, q, core, span] = total.astype(bf16)

        by_piece(0, capacity, piece, body)

    def with_incoming(above_too, below_too, action):
        both = above_too & below_too
        pl.when(both)(lambda: action(True, True))
        pl.when(above_too & jnp.logical_not(both))(lambda: action(True, False))
        pl.when(below_too & jnp.logical_not(both))(lambda: action(False, True))
        pl.when(jnp.logical_not(above_too | below_too))(lambda: action(False, False))

    def far_total(at, h):
        above_too, below_too = (at <= level) & has_above, (at >= level) & has_below
        pl.when(above_too)(lambda: far_sum_down(at, h).wait_recv())
        pl.when(below_too)(lambda: far_sum_up(at, h).wait_recv())

        def action(from_up, from_down):
            def body(span):
                total = part[at, 3, core, span].astype(f32) + from_core[at, 3, span].astype(f32)
                if from_up:
                    total = total + far_above[at, span].astype(f32)
                if from_down:
                    total = total + far_below[at, span].astype(f32)
                part[at, 3, core, span] = total.astype(bf16)

            by_piece((0, low)[h], (low, high)[h], step_rows, body)

        with_incoming(above_too, below_too, action)
        pl.when(at < level)(lambda: far_sum_down(at, h).start())
        pl.when(at > level)(lambda: far_sum_up(at, h).start())
        pl.when(at == level)(lambda: (home_low, home_high)[h]().start())

    def far_step(at, h):
        pl.when(h == 0)(lambda: give(at, 3).wait_recv())
        pl.when(h == 0)(lambda: far_total(at, 0))
        pl.when(h == 1)(lambda: far_total(at, 1))

    def dense_step(at, h):
        above_too, below_too = (at <= level) & has_above, (at >= level) & has_below
        pl.when(above_too)(lambda: sum_down(at, h).wait_recv())
        pl.when(below_too)(lambda: sum_up(at, h).wait_recv())

        def action(from_up, from_down):
            def body(span):
                total = local[at, span]
                if from_up:
                    total = total + dense_above[at, span].astype(f32)
                if from_down:
                    total = total + dense_below[at, span].astype(f32)
                dense[at, span] = total.astype(bf16)

            by_piece(h * half, half, piece, body)

        with_incoming(above_too, below_too, action)
        pl.when(at < level)(lambda: sum_down(at, h).start())
        pl.when(at > level)(lambda: sum_up(at, h).start())

    def expand(at, _):
        give(at, 0).wait_recv()
        back_left(at).wait_recv()
        back_right(at).wait_recv()
        own = (part[at, 0, core].astype(f32) + from_core[at, 0].astype(f32)).astype(bf16)
        results = jnp.concatenate([own, from_right[at], from_left[at]], axis=0)
        local[at] = placed(at, (column, right_column, left_column), results)

    def arrive(at, h):
        upward, downward = (at <= level) & has_above, (at >= level) & has_below

        @pl.when(h == 0)
        def _():
            pl.when(at < level)(lambda: table_up(at).wait_recv())
            pl.when(at > level)(lambda: table_down(at).wait_recv())
            pl.when(upward)(lambda: table_up(at).start())
            pl.when(downward)(lambda: table_down(at).start())

        pl.when(at < level)(lambda: up(at, h).wait_recv())
        pl.when(at > level)(lambda: down(at, h).wait_recv())
        pl.when(upward)(lambda: up(at, h).start())
        pl.when(downward)(lambda: down(at, h).start())

    def far_out(at, _):
        out_far[...] = picked(at, (far_column,))
        far_right().start()
        far_left().start()

    def relay(at, _):
        far_right().wait_recv()
        on_right().start()
        far_left().wait_recv()
        on_left().start()

    def sides_out(at, _):
        sent = picked(at, (right_column, left_column, column))
        out_right[at] = sent[:capacity]
        out_left[at] = sent[capacity : 2 * capacity]
        to_right(at).start()
        to_left(at).start()
        blk[at, 0, core] = sent[2 * capacity :]
        share(at, 0).start()

    def sides_in(at, _):
        to_right(at).wait_recv()
        share(at, 1).start()
        to_left(at).wait_recv()
        share(at, 2).start()

    def far_in(at, _):
        @pl.when(at == level)
        def _():
            on_right().wait_recv()
            on_left().wait_recv()

        pl.when(at < level)(lambda: far_up(at).wait_recv())
        pl.when(at > level)(lambda: far_down(at).wait_recv())
        pl.when((at <= level) & has_above)(lambda: far_up(at).start())
        pl.when((at >= level) & has_below)(lambda: far_down(at).start())
        share(at, 3).start()

    def multiply(at, q):
        shared_in(at, q).wait_recv()
        compute(at, q)
        give(at, q).start()

    def back(at, q):
        paired(at, q)
        pl.when(q == 1)(lambda: back_left(at).start())
        pl.when(q == 2)(lambda: back_right(at).start())

    def home_relay(at, h):
        @pl.when(h == 0)
        def _():
            home_low().wait_recv()
            last_low().start()

        @pl.when(h == 1)
        def _():
            home_high().wait_recv()
            last_high().start()

    def finish(at, _):
        last_low().wait_recv()
        last_high().wait_recv()
        total = placed(level, (far_column,), far_back[...])
        out_ref[...] = (dense[level].astype(f32) + total).astype(bf16)

    actions = dict(
        D=arrive, M=sides_out, I=sides_in, G=far_in,
        C=multiply, P=back, F=far_step, S=dense_step,
        E=expand, X=far_out, Y=relay, V=home_relay, Z=finish,
    )
    kinds = list(actions)
    words, per_word, base = coded_orders(depth, kinds)
    mirrored = level >= depth // 2
    row = jnp.where(mirrored, depth - 1 - level, level)

    def one_word(place, carry):
        word = 0
        for at, listing in enumerate(words):
            for turn, value in enumerate(listing):
                word = word + jnp.where((row == at) & (place == turn), value, 0)

        def one_step(_, rest):
            code = rest % base
            kind, at, q = code // (4 * depth), code // 4 % depth, code % 4
            at = jnp.where(mirrored, depth - 1 - at, at)
            for first in range(0, len(kinds), 4):

                @pl.when((kind >= first) & (kind < first + 4))
                def _():
                    for number in range(first, min(first + 4, len(kinds))):
                        pl.when(kind == number)(
                            functools.partial(actions[kinds[number]], at, q)
                        )

            return rest // base

        lax.fori_loop(0, per_word, one_step, word)
        return carry

    lax.fori_loop(0, len(words[0]), one_word, 0)

    def drain(at, carry):
        upward, downward = (at <= level) & has_above, (at >= level) & has_below

        def settle(use, copy, *more):
            pl.when(use)(lambda: copy(at, *more).wait_send())

        settle(upward, table_up)
        settle(downward, table_down)
        settle(upward, far_up)
        settle(downward, far_down)
        for h in range(2):
            settle(upward, up, h)
            settle(downward, down, h)
            settle(at < level, sum_down, h)
            settle(at > level, sum_up, h)
            settle(at < level, far_sum_down, h)
            settle(at > level, far_sum_up, h)
        for copy in (to_right, to_left, back_left, back_right):
            copy(at).wait_send()
        for q in range(4):
            share(at, q).wait_send()
            give(at, q).wait_send()
        return carry

    lax.fori_loop(0, depth, drain, 0)
    for copy in (
        far_right, far_left, on_right, on_left, home_low, home_high, last_low, last_high
    ):
        copy().wait_send()


def dense_plan(expert_input, expert_gain, routes, route_weight, w_gate, w_up, w_down):
    row_count, width = expert_input.shape
    experts = lax.axis_size("ep")
    depth = lax.axis_size("tp") // 2
    capacity = 3 * routes.shape[1] * row_count // (2 * experts)
    normed = normalize(expert_input, expert_gain)
    listed = slots(routes, route_weight, experts)
    pad = -(-3 * experts // 16) * 16
    lanes = -(-row_count // 128) * 128
    listed = jnp.pad(listed, ((0, pad - 3 * experts), (0, lanes - row_count)))
    bf16 = jnp.bfloat16
    low = -(-capacity // 32) * 16
    high = capacity - low
    vmem = pl.BlockSpec(memory_space=pltpu.VMEM)
    compact = pltpu.VMEM((depth, capacity, width), bf16)
    dense = pltpu.VMEM((depth, row_count, width), bf16)
    return pl.pallas_call(
        functools.partial(stream_kernel, depth, capacity, experts),
        out_shape=jax.ShapeDtypeStruct((row_count, width), bf16),
        in_specs=[vmem] * 5,
        out_specs=vmem,
        scratch_shapes=[
            pltpu.VMEM((depth, row_count, width), bf16),
            pltpu.VMEM((depth, pad, lanes), bf16),
            pltpu.VMEM((depth, 4, 2, capacity, width), bf16),
            pltpu.VMEM((depth, 4, 2, capacity, width), bf16),
            pltpu.VMEM((depth, 4, capacity, width), bf16),
            compact,
            compact,
            pltpu.VMEM((capacity, width), bf16),
            pltpu.VMEM((low, width), bf16),
            pltpu.VMEM((high, width), bf16),
            compact,
            compact,
            pltpu.VMEM((depth, row_count, width), jnp.float32),
            dense,
            dense,
            dense,
            compact,
            compact,
            pltpu.VMEM((low, width), bf16),
            pltpu.VMEM((high, width), bf16),
            pltpu.VMEM((capacity, width), bf16),
            pltpu.SemaphoreType.DMA((36, depth)),
            pltpu.SemaphoreType.DMA((36, depth)),
            pltpu.SemaphoreType.DMA,
        ],
        compiler_params=pltpu.CompilerParams(
            collective_id=0, has_side_effects=True, vmem_limit_bytes=60 * 2**20
        ),
    )(normed, listed, w_gate[0], w_up[0], w_down[0])


def on_device(
    mixer_input, mixer_gain, group_weight, mixer_scale,
    expert_input, expert_gain, routes, route_weight, w_gate, w_up, w_down,
):
    devices = lax.axis_size(("ep", "tp"))
    gathered_bytes = 2 * devices * expert_input.size
    square = lax.axis_size("ep") == 4 and lax.axis_size("tp") == 4 * len(ORDERS)
    plan = dense_plan if square and gathered_bytes <= vmem_share else routed_plan
    expert_out = plan(expert_input, expert_gain, routes, route_weight, w_gate, w_up, w_down)
    return (mixer(mixer_input, mixer_gain, group_weight, mixer_scale), expert_out)


def solution(mesh):
    placed = (
        P(("ep", "tp"), None),
        P(),
        P(),
        P(),
        P(("ep", "tp"), None),
        P(),
        P(("ep", "tp"), None),
        P(("ep", "tp"), None),
        P("ep", None, "tp"),
        P("ep", None, "tp"),
        P("ep", "tp", None),
    )
    return jax.shard_map(
        on_device,
        mesh=mesh,
        in_specs=placed,
        out_specs=(P(("ep", "tp"), None), P(("ep", "tp"), None)),
        check_vma=False,
    )
```

```python
import functools
import math

import jax
import jax.numpy as jnp
from jax import lax
from jax.experimental import pallas as pl
from jax.experimental.pallas import tpu as pltpu
from jax.sharding import PartitionSpec as P

epsilon = 1e-06
vmem_share = 2**24
edge = 8


def padded_2(value, sides, width):
    for axis, dim in sides:
        size, length = (lax.axis_size(axis), value.shape[dim])
        up = [(i, (i + 1) % size) for i in range(size - 1)]
        down = [(j, i) for i, j in up]
        last = lax.slice_in_dim(value, length - width, length, axis=dim)
        leading = lax.slice_in_dim(value, 0, width, axis=dim)
        before = lax.ppermute(last, axis, up)
        after = lax.ppermute(leading, axis, down)
        value = jnp.concatenate([before, value, after], axis=dim)
    return value


def normalize(row_values, gain):
    values = row_values.astype(jnp.float32)
    scaled = values * lax.rsqrt(jnp.mean(values * values, axis=-1, keepdims=True) + epsilon)
    return (scaled * gain).astype(jnp.bfloat16)


def pool_groups(padded, start_row, row_count, seq_length):
    group_width = padded.shape[1] // 4
    position = start_row + jnp.arange(row_count, dtype=jnp.int32)
    centre = padded[8 : 8 + row_count]
    pooled_parts = []
    for group_index in range(4):
        window = 2 ** (group_index + 1)
        reach_left = window // 2
        reach_right = window - 1 - reach_left
        group_cols = padded[:, group_index * group_width : (group_index + 1) * group_width]
        window_sum = group_cols[8 - reach_left : 8 - reach_left + row_count]
        for offset in range(1 - reach_left, reach_right + 1):
            window_sum = window_sum + group_cols[8 + offset : 8 + offset + row_count]
        cover = (
            jnp.minimum(position + reach_right + 1, seq_length)
            - jnp.maximum(position - reach_left, 0)
        ).astype(jnp.float32)
        pooled_parts.append(
            window_sum / cover[:, None]
            - centre[:, group_index * group_width : (group_index + 1) * group_width]
        )
    return jnp.stack(pooled_parts, axis=1).astype(jnp.bfloat16)


def mixer(mixer_input, mixer_gain, group_weight, mixer_scale):
    row_count = mixer_input.shape[0]
    normed = normalize(mixer_input, mixer_gain)
    padded = padded_2(normed, ((("ep", "tp"), 0),), 8)
    start_row = lax.axis_index(("ep", "tp")) * row_count
    seq_length = row_count * lax.axis_size(("ep", "tp"))
    pooled = pool_groups(padded.astype(jnp.float32), start_row, row_count, seq_length)
    mixed_groups = jnp.einsum(
        "tgi,gio->tgo", pooled, group_weight, preferred_element_type=jnp.float32
    )
    return (mixed_groups.reshape(row_count, -1) * mixer_scale).astype(jnp.bfloat16)


def routed_plan(expert_input, expert_gain, routes, route_weight, w_gate, w_up, w_down):
    row_count = expert_input.shape[0]
    top_count = routes.shape[1]
    experts = lax.axis_size("ep") * w_gate.shape[0]
    capacity = 3 * top_count * row_count // (2 * experts)
    normed = normalize(expert_input, expert_gain)
    flat_route = routes.reshape(-1)
    onehot = (flat_route[:, None] == jnp.arange(experts, dtype=jnp.int32)[None, :]).astype(
        jnp.int32
    )
    before = jnp.cumsum(onehot, axis=0) - onehot
    slot_index = flat_route * capacity + jnp.sum(before * onehot, axis=1)
    places = (
        slot_index.reshape(row_count, top_count)[None, :, :]
        == jnp.arange(experts * capacity, dtype=jnp.int32)[:, None, None]
    )
    dispatch = jnp.any(places, axis=2).astype(jnp.bfloat16)
    outgoing = jnp.dot(dispatch, normed, preferred_element_type=jnp.float32).astype(jnp.bfloat16)
    arrived = lax.all_to_all(outgoing, "ep", split_axis=0, concat_axis=0, tiled=True)
    down_w = w_down[0]
    paired = jnp.stack((w_gate[0], w_up[0]), axis=0)
    portion = lax.all_gather(paired, "tp", axis=2, tiled=True)
    gate_part = jnp.dot(arrived, portion[0], preferred_element_type=jnp.float32)
    up_part = jnp.dot(arrived, portion[1], preferred_element_type=jnp.float32)
    hidden = (jax.nn.silu(gate_part) * up_part).astype(jnp.bfloat16)
    block_width = down_w.shape[0]
    portion = lax.all_gather(down_w, "tp", axis=0, tiled=True)
    blocks = portion.shape[0] // block_width
    hidden_part = hidden
    hidden_part = hidden_part.reshape(hidden_part.shape[0], blocks, block_width)
    block_terms = jnp.einsum(
        "rkf,kfd->krd",
        hidden_part,
        portion.reshape(blocks, block_width, portion.shape[1]),
        preferred_element_type=jnp.float32,
    )
    rounded = lax.optimization_barrier(block_terms.astype(jnp.bfloat16)).astype(jnp.float32)
    result = jnp.sum(rounded, axis=0)
    returned = lax.all_to_all(
        result.astype(jnp.bfloat16), "ep", split_axis=0, concat_axis=0, tiled=True
    )
    picked = (
        jnp.take(returned, slot_index, axis=0).astype(jnp.float32).reshape(row_count, top_count, -1)
    )
    expert_out = jnp.sum(picked * route_weight[:, :, None], axis=1).astype(jnp.bfloat16)
    return expert_out


ORDERS = (
    (
        ("D", 0, 0), ("D", 0, 1), ("X", 0, 0), ("M", 0, 0), ("D", 1, 1), ("Y", 0, 0), ("I", 0, 0),
        ("D", 1, 0), ("M", 1, 0), ("D", 2, 0), ("D", 2, 1), ("G", 0, 0), ("M", 2, 0), ("I", 1, 0),
        ("C", 1, 1), ("C", 1, 2), ("C", 2, 0), ("G", 1, 0), ("P", 1, 1), ("P", 1, 2), ("C", 0, 3),
        ("C", 0, 2), ("D", 3, 1), ("C", 1, 3), ("I", 2, 0), ("C", 0, 1), ("D", 3, 0), ("M", 3, 0),
        ("C", 1, 0), ("F", 1, 0), ("P", 0, 1), ("C", 2, 1), ("C", 0, 0), ("F", 1, 1), ("P", 0, 2),
        ("E", 1, 0), ("G", 2, 0), ("S", 1, 1), ("C", 2, 2), ("C", 2, 3), ("P", 2, 1), ("I", 3, 0),
        ("F", 2, 0), ("C", 3, 2), ("P", 2, 2), ("G", 3, 0), ("C", 3, 1), ("P", 3, 2), ("F", 2, 1),
        ("C", 3, 3), ("E", 0, 0), ("F", 3, 0), ("F", 3, 1), ("C", 3, 0), ("P", 3, 1), ("H", 0, 0),
        ("E", 2, 0), ("S", 2, 3), ("S", 2, 2), ("E", 3, 0), ("S", 3, 1), ("S", 3, 2), ("S", 3, 0),
        ("S", 3, 3), ("Q", 0, 0), ("F", 0, 0), ("S", 2, 0), ("Q", 0, 1), ("Q", 0, 3), ("Q", 0, 2),
        ("S", 2, 1), ("S", 1, 3), ("S", 1, 0), ("S", 1, 2), ("F", 0, 1), ("V", 0, 0), ("S", 0, 1),
        ("V", 0, 1), ("S", 0, 3), ("S", 0, 2), ("S", 0, 0), ("Z", 0, 0),
    ),
    (
        ("D", 1, 1), ("D", 1, 0), ("X", 1, 0), ("Y", 1, 0), ("D", 2, 1), ("D", 0, 0), ("D", 0, 1),
        ("D", 2, 0), ("G", 1, 0), ("M", 0, 0), ("M", 2, 0), ("D", 3, 1), ("M", 1, 0), ("C", 1, 3),
        ("D", 3, 0), ("I", 2, 0), ("G", 0, 0), ("C", 2, 1), ("C", 2, 2), ("G", 2, 0), ("C", 1, 0),
        ("M", 3, 0), ("I", 1, 0), ("P", 2, 1), ("I", 0, 0), ("C", 1, 2), ("P", 2, 2), ("G", 3, 0),
        ("C", 2, 3), ("C", 0, 2), ("I", 3, 0), ("C", 0, 1), ("C", 3, 2), ("C", 2, 0), ("C", 3, 1),
        ("P", 0, 2), ("F", 2, 0), ("C", 3, 3), ("P", 3, 1), ("E", 2, 0), ("P", 0, 1), ("F", 2, 1),
        ("P", 3, 2), ("C", 1, 1), ("F", 1, 0), ("F", 3, 0), ("C", 0, 0), ("C", 0, 3), ("F", 3, 1),
        ("P", 1, 1), ("C", 3, 0), ("S", 2, 3), ("F", 1, 1), ("E", 3, 0), ("S", 2, 2), ("F", 0, 0),
        ("P", 1, 2), ("H", 1, 0), ("S", 3, 1), ("E", 0, 0), ("F", 0, 1), ("S", 3, 2), ("Q", 1, 0),
        ("V", 1, 0), ("S", 0, 1), ("S", 3, 0), ("S", 0, 2), ("S", 3, 3), ("S", 0, 0), ("Q", 1, 3),
        ("S", 2, 0), ("Q", 1, 2), ("Q", 1, 1), ("V", 1, 1), ("S", 0, 3), ("S", 2, 1), ("E", 1, 0),
        ("S", 1, 3), ("S", 1, 1), ("S", 1, 0), ("S", 1, 2), ("Z", 1, 0),
    ),
)


def coded_orders(depth, kinds):
    base = len(kinds) * 4 * depth + 1
    per_word = 1
    while base ** (per_word + 1) < 2**31:
        per_word += 1
    idle = base - 1
    words = []
    for order in ORDERS:
        codes = [(kinds.index(kind) * depth + at) * 4 + q for kind, at, q in order]
        codes += [idle] * (-len(codes) % per_word)
        words.append([
            sum(code * base**n for n, code in enumerate(codes[first : first + per_word]))
            for first in range(0, len(codes), per_word)
        ])
    return words, per_word, base


def stream_kernel(
    depth, capacity, experts,
    input_ref, gain_ref, routes_ref, weight_ref, mixer_gain_ref, mixer_scale_ref,
    gate_hbm, up_hbm, down_hbm, mixer_hbm, group_hbm, mixed_ref, out_ref,
    gate_ref, up_ref, down_ref, mixer_ref, group_ref, mix, tok, tables, blk, part, from_core, out_right, out_left, out_far, relay_right, relay_left,
    from_right, from_left, local, dense, dense_above, dense_below,
    far_above, far_below, home_left, home_right, far_back,
    send_sem, recv_sem, local_sem,
):
    column, line = lax.axis_index("ep"), lax.axis_index("tp")
    level, core = line // 2, line % 2
    other = 1 - core
    rows = out_ref.shape[0]
    half, quarter = rows // 2, rows // 4
    low = -(-capacity // 32) * 16
    high = capacity - low
    piece = math.gcd(quarter, capacity)
    step_rows = math.gcd(low, high)
    right_column, left_column, far_column = (2 * column + 1) % 5, (3 * column + 2) % 5, 3 - column
    right, left = (right_column, line), (left_column, line)
    beside = (column, level * 2 + other)
    above, below = (column, line + 2), (column, line - 2)
    has_above, has_below = level < depth - 1, level > 0
    f32, bf16 = jnp.float32, jnp.bfloat16

    def link(src, dst, kind, at, target):
        return pltpu.make_async_remote_copy(
            src_ref=src, dst_ref=dst, send_sem=send_sem.at[kind, at],
            recv_sem=recv_sem.at[kind, at], device_id=target,
            device_id_type=pl.DeviceIdType.MESH,
        )

    def part_of(h):
        return pl.ds(pl.multiple_of(h * half, half), half)

    def up(at, h):
        return link(tok.at[at, part_of(h)], tok.at[at, part_of(h)], h, at, above)

    def down(at, h):
        return link(tok.at[at, part_of(h)], tok.at[at, part_of(h)], 2 + h, at, below)

    def table_up(at):
        return link(tables.at[at], tables.at[at], 4, at, above)

    def table_down(at):
        return link(tables.at[at], tables.at[at], 5, at, below)

    def to_right(at):
        return link(out_right.at[at], blk.at[at, 1, core], 6, at, right)

    def to_left(at):
        return link(out_left.at[at], blk.at[at, 2, core], 7, at, left)

    def far_right():
        return link(out_far.at[pl.ds(0, low)], relay_right, 8, 0, right)

    def far_left():
        return link(out_far.at[pl.ds(low, high)], relay_left, 9, 0, left)

    def on_right():
        return link(relay_right, blk.at[level, 3, core, pl.ds(0, low)], 10, 0, right)

    def on_left():
        return link(relay_left, blk.at[level, 3, core, pl.ds(low, high)], 11, 0, left)

    def far_up(at):
        return link(blk.at[at, 3, core], blk.at[at, 3, core], 12, at, above)

    def far_down(at):
        return link(blk.at[at, 3, core], blk.at[at, 3, core], 13, at, below)

    def share(at, q):
        return link(blk.at[at, q, core], blk.at[at, q, core], 14 + q, at, beside)

    def shared_in(at, q):
        return link(blk.at[at, q, other], blk.at[at, q, other], 14 + q, at, beside)

    def give(at, q):
        return link(part.at[at, q, other], from_core.at[at, q], 18 + q, at, beside)

    def back_left(at):
        return link(part.at[at, 1, core], from_right.at[at], 22, at, left)

    def back_right(at):
        return link(part.at[at, 2, core], from_left.at[at], 23, at, right)

    def fourth(h):
        return pl.ds(pl.multiple_of(h * quarter, quarter), quarter)

    def sum_down(at, h):
        return link(dense.at[at, fourth(h)], dense_above.at[at, fourth(h)], 24 + h, at, below)

    def sum_up(at, h):
        return link(dense.at[at, fourth(h)], dense_below.at[at, fourth(h)], 28 + h, at, above)

    cuts = (pl.ds(0, low), pl.ds(low, high))

    def far_sum_down(at, h):
        return link(part.at[at, 3, core, cuts[h]], far_above.at[at, cuts[h]], 32 + h, at, below)

    def far_sum_up(at, h):
        return link(part.at[at, 3, core, cuts[h]], far_below.at[at, cuts[h]], 34 + h, at, above)

    def home_low():
        return link(part.at[level, 3, core, cuts[0]], home_left, 36, 0, left)

    def home_high():
        return link(part.at[level, 3, core, cuts[1]], home_right, 37, 0, right)

    def last_low():
        return link(home_left, far_back.at[cuts[0]], 38, 0, left)

    def last_high():
        return link(home_right, far_back.at[cuts[1]], 39, 0, right)

    place = column * 2 * depth + line
    last_place = lax.axis_size("ep") * 2 * depth - 1
    first_line, last_line = line == 0, line == 2 * depth - 1
    following = (column + jnp.where(last_line, 1, 0), jnp.where(last_line, 0, line + 1))
    preceding = (column - jnp.where(first_line, 1, 0), jnp.where(first_line, 2 * depth - 1, line - 1))
    has_following, has_preceding = place < last_place, place > 0

    def to_following():
        return link(mix.at[pl.ds(rows, edge)], mix.at[pl.ds(0, edge)], 40, 0, following)

    def to_preceding():
        return link(
            mix.at[pl.ds(edge, edge)], mix.at[pl.ds(edge + rows, edge)], 41, 0, preceding
        )

    loads = [
        pltpu.make_async_copy(src, dst, local_sem.at[n])
        for n, (src, dst) in enumerate((
            (gate_hbm, gate_ref), (up_hbm, up_ref), (down_hbm, down_ref),
            (mixer_hbm, mixer_ref), (group_hbm, group_ref),
        ))
    ]
    def by_piece(start, count, width, body):
        def one(i, carry):
            body(pl.ds(pl.multiple_of(start + i * width, width), width))
            return carry

        lax.fori_loop(0, count // width, one, 0)

    barrier = pltpu.get_barrier_semaphore()

    def greet(target):
        pl.semaphore_signal(
            barrier, inc=1, device_id=target, device_id_type=pl.DeviceIdType.MESH
        )

    greet(right)
    greet(left)
    greet(beside)
    pl.when(has_above)(lambda: greet(above))
    pl.when(has_below)(lambda: greet(below))
    for load in loads:
        load.start()

    def normed(values, gains):
        values = values.astype(f32)
        mean = jnp.sum(values * values, axis=1, keepdims=True) / values.shape[1]
        return (values * lax.rsqrt(mean + epsilon) * gains).astype(bf16)

    def own_rows(span):
        tok[level, span] = normed(input_ref[span], gain_ref[...])

    by_piece(0, rows, piece, own_rows)
    sort = lax.broadcasted_iota(jnp.int32, (tables.shape[1], rows), 0)
    first = sort % experts == routes_ref[0:1, :]
    second = sort % experts == routes_ref[1:2, :]
    weights = jnp.where(first, weight_ref[0:1, :], 0.0) + jnp.where(second, weight_ref[1:2, :], 0.0)
    named = first | second
    earlier = lax.broadcasted_iota(jnp.int32, (rows, rows), 0) < lax.broadcasted_iota(
        jnp.int32, (rows, rows), 1
    )
    turns = jnp.dot(
        jnp.where(named, 1.0, 0.0).astype(bf16), jnp.where(earlier, 1.0, 0.0).astype(bf16),
        preferred_element_type=f32,
    )
    turns = jnp.where(named, turns, -1.0).astype(bf16)
    coarse = weights.astype(bf16)
    fine = (weights - coarse.astype(f32)).astype(bf16)
    group = sort // experts
    listed = jnp.where(
        group == 0, turns.astype(f32), jnp.where(group == 1, coarse.astype(f32), fine.astype(f32))
    )
    tables[level, :, pl.ds(0, rows)] = listed.astype(bf16)
    tables[level, :, pl.ds(rows, tables.shape[2] - rows)] = jnp.zeros(
        (tables.shape[1], tables.shape[2] - rows), bf16
    )
    pl.semaphore_wait(barrier, 3 + jnp.where(has_above, 1, 0) + jnp.where(has_below, 1, 0))

    def table(at):
        listed = tables[at, :, pl.ds(0, rows)].astype(f32)
        listing = lax.broadcasted_iota(jnp.int32, listed.shape, 0)
        index = lax.broadcasted_iota(jnp.int32, (capacity, rows), 0).astype(f32)

        def row_of(at_row):
            return jnp.sum(jnp.where(listing == at_row, listed, 0.0), axis=0, keepdims=True)

        def hits(expert):
            return index == row_of(expert)

        return row_of, hits

    def picked(at, chosen):
        _, hits = table(at)
        picks = [jnp.where(hits(expert), 1.0, 0.0).astype(bf16) for expert in chosen]
        return jnp.dot(
            jnp.concatenate(picks, axis=0), tok[at], preferred_element_type=f32
        ).astype(bf16)

    def placed(at, chosen, results):
        row_of, hits = table(at)
        total = None
        for kind in (1, 2):
            weights = [
                jnp.where(hits(expert), row_of(kind * experts + expert), 0.0).astype(bf16)
                for expert in chosen
            ]
            term = lax.dot_general(
                jnp.concatenate(weights, axis=0), results,
                (((0,), (0,)), ((), ())), preferred_element_type=f32,
            )
            total = term if total is None else total + term
        return total

    def compute(at, q):
        gathered = jnp.concatenate([blk[at, q, 0], blk[at, q, 1]], axis=0)
        gate_part = jnp.dot(gathered, gate_ref[...], preferred_element_type=f32)
        up_part = jnp.dot(gathered, up_ref[...], preferred_element_type=f32)
        hidden = (gate_part / (1.0 + jnp.exp(-gate_part)) * up_part).astype(bf16)
        partial = jnp.dot(hidden, down_ref[...], preferred_element_type=f32).astype(bf16)
        for lane in range(2):
            part[at, q, lane] = partial[lane * capacity : (lane + 1) * capacity]

    def paired(at, q):
        give(at, q).wait_recv()

        def body(span):
            total = part[at, q, core, span].astype(f32) + from_core[at, q, span].astype(f32)
            part[at, q, core, span] = total.astype(bf16)

        by_piece(0, capacity, piece, body)

    def with_incoming(above_too, below_too, action):
        both = above_too & below_too
        pl.when(both)(lambda: action(True, True))
        pl.when(above_too & jnp.logical_not(both))(lambda: action(True, False))
        pl.when(below_too & jnp.logical_not(both))(lambda: action(False, True))
        pl.when(jnp.logical_not(above_too | below_too))(lambda: action(False, False))

    def far_total(at, h):
        above_too, below_too = (at <= level) & has_above, (at >= level) & has_below
        pl.when(above_too)(lambda: far_sum_down(at, h).wait_recv())
        pl.when(below_too)(lambda: far_sum_up(at, h).wait_recv())

        def action(from_up, from_down):
            def body(span):
                total = part[at, 3, core, span].astype(f32) + from_core[at, 3, span].astype(f32)
                if from_up:
                    total = total + far_above[at, span].astype(f32)
                if from_down:
                    total = total + far_below[at, span].astype(f32)
                part[at, 3, core, span] = total.astype(bf16)

            by_piece((0, low)[h], (low, high)[h], step_rows, body)

        with_incoming(above_too, below_too, action)
        pl.when(at < level)(lambda: far_sum_down(at, h).start())
        pl.when(at > level)(lambda: far_sum_up(at, h).start())
        pl.when(at == level)(lambda: (home_low, home_high)[h]().start())

    def far_step(at, h):
        pl.when(h == 0)(lambda: give(at, 3).wait_recv())
        pl.when(h == 0)(lambda: far_total(at, 0))
        pl.when(h == 1)(lambda: far_total(at, 1))

    def dense_step(at, h):
        above_too, below_too = (at <= level) & has_above, (at >= level) & has_below
        pl.when(above_too)(lambda: sum_down(at, h).wait_recv())
        pl.when(below_too)(lambda: sum_up(at, h).wait_recv())

        def action(from_up, from_down):
            def body(span):
                total = local[at, span]
                if from_up:
                    total = total + dense_above[at, span].astype(f32)
                if from_down:
                    total = total + dense_below[at, span].astype(f32)
                dense[at, span] = total.astype(bf16)

            by_piece(h * quarter, quarter, piece, body)

        with_incoming(above_too, below_too, action)
        pl.when(at < level)(lambda: sum_down(at, h).start())
        pl.when(at > level)(lambda: sum_up(at, h).start())

    def expand(at, _):
        give(at, 0).wait_recv()
        back_left(at).wait_recv()
        back_right(at).wait_recv()
        own = (part[at, 0, core].astype(f32) + from_core[at, 0].astype(f32)).astype(bf16)
        results = jnp.concatenate([own, from_right[at], from_left[at]], axis=0)
        local[at] = placed(at, (column, right_column, left_column), results)

    def arrive(at, h):
        upward, downward = (at <= level) & has_above, (at >= level) & has_below

        @pl.when(h == 0)
        def _():
            pl.when(at < level)(lambda: table_up(at).wait_recv())
            pl.when(at > level)(lambda: table_down(at).wait_recv())
            pl.when(upward)(lambda: table_up(at).start())
            pl.when(downward)(lambda: table_down(at).start())

        pl.when(at < level)(lambda: up(at, h).wait_recv())
        pl.when(at > level)(lambda: down(at, h).wait_recv())
        pl.when(upward)(lambda: up(at, h).start())
        pl.when(downward)(lambda: down(at, h).start())

    def far_out(at, _):
        out_far[...] = picked(at, (far_column,))
        far_right().start()
        far_left().start()
        for load in loads[:3]:
            load.wait()

    def relay(at, _):
        far_right().wait_recv()
        on_right().start()
        far_left().wait_recv()
        on_left().start()

    def sides_out(at, _):
        sent = picked(at, (right_column, left_column, column))
        out_right[at] = sent[:capacity]
        out_left[at] = sent[capacity : 2 * capacity]
        to_right(at).start()
        to_left(at).start()
        blk[at, 0, core] = sent[2 * capacity :]
        share(at, 0).start()

    def sides_in(at, _):
        to_right(at).wait_recv()
        share(at, 1).start()
        to_left(at).wait_recv()
        share(at, 2).start()

    def far_in(at, _):
        @pl.when(at == level)
        def _():
            on_right().wait_recv()
            on_left().wait_recv()

        pl.when(at < level)(lambda: far_up(at).wait_recv())
        pl.when(at > level)(lambda: far_down(at).wait_recv())
        pl.when((at <= level) & has_above)(lambda: far_up(at).start())
        pl.when((at >= level) & has_below)(lambda: far_down(at).start())
        share(at, 3).start()

    def multiply(at, q):
        shared_in(at, q).wait_recv()
        compute(at, q)
        give(at, q).start()

    def back(at, q):
        paired(at, q)
        pl.when(q == 1)(lambda: back_left(at).start())
        pl.when(q == 2)(lambda: back_right(at).start())

    def home_relay(at, h):
        @pl.when(h == 0)
        def _():
            home_low().wait_recv()
            last_low().start()

        @pl.when(h == 1)
        def _():
            home_high().wait_recv()
            last_high().start()

    def finish(at, _):
        last_low().wait_recv()
        last_high().wait_recv()
        total = placed(level, (far_column,), far_back[...])
        out_ref[...] = (dense[level].astype(f32) + total).astype(bf16)

    def mixer_rows(at, _):
        for load in loads[3:]:
            load.wait()

        def body(i, carry):
            start = pl.multiple_of(i * piece, piece)
            values = normed(mixer_ref[pl.ds(start, piece)], mixer_gain_ref[...])
            mix[pl.ds(pl.multiple_of(start + edge, edge), piece)] = values.astype(f32)
            return carry

        lax.fori_loop(0, rows // piece, body, 0)
        zeros = jnp.zeros((edge, mix.shape[1]), f32)

        @pl.when(jnp.logical_not(has_preceding))
        def _():
            mix[pl.ds(0, edge)] = zeros

        @pl.when(jnp.logical_not(has_following))
        def _():
            mix[pl.ds(edge + rows, edge)] = zeros

        pl.when(has_following)(lambda: to_following().start())
        pl.when(has_preceding)(lambda: to_preceding().start())

    def mixer_group(number):
        width = group_ref.shape[1]
        span = pl.ds(number * width, width)
        window = 2 ** (number + 1)
        values = mix[:, span]
        length = values.shape[0]
        total = values
        for level_of_sum in range(number + 1):
            total = total + pltpu.roll(total, length - 2**level_of_sum, 0)
        total = pltpu.roll(total, window // 2, 0)[edge : edge + rows]
        position = place * rows + lax.broadcasted_iota(jnp.int32, (rows, width), 0)
        ahead = jnp.minimum(position + window // 2, (last_place + 1) * rows)
        cover = (ahead - jnp.maximum(position - window // 2, 0)).astype(f32)
        pooled = (total / cover - values[edge : edge + rows]).astype(bf16)
        product = jnp.dot(pooled, group_ref[number], preferred_element_type=f32)
        mixed_ref[:, span] = (product * mixer_scale_ref[:, span]).astype(bf16)

    def mixer_step(at, q):
        @pl.when(q == 0)
        def _():
            pl.when(has_preceding)(lambda: to_following().wait_recv())
            pl.when(has_following)(lambda: to_preceding().wait_recv())

        for number in range(4):
            pl.when(q == number)(functools.partial(mixer_group, number))

    actions = dict(
        D=arrive, M=sides_out, I=sides_in, G=far_in,
        C=multiply, P=back, F=far_step, S=dense_step,
        E=expand, X=far_out, Y=relay, V=home_relay, Z=finish,
        H=mixer_rows, Q=mixer_step,
    )
    kinds = list(actions)
    words, per_word, base = coded_orders(depth, kinds)
    mirrored = level >= depth // 2
    row = jnp.where(mirrored, depth - 1 - level, level)

    def one_word(place, carry):
        word = 0
        for at, listing in enumerate(words):
            for turn, value in enumerate(listing):
                word = word + jnp.where((row == at) & (place == turn), value, 0)

        def one_step(_, rest):
            code = rest % base
            kind, at, q = code // (4 * depth), code // 4 % depth, code % 4
            at = jnp.where(mirrored, depth - 1 - at, at)
            for first in range(0, len(kinds), 4):

                @pl.when((kind >= first) & (kind < first + 4))
                def _():
                    for number in range(first, min(first + 4, len(kinds))):
                        pl.when(kind == number)(
                            functools.partial(actions[kinds[number]], at, q)
                        )

            return rest // base

        lax.fori_loop(0, per_word, one_step, word)
        return carry

    lax.fori_loop(0, len(words[0]), one_word, 0)

    def drain(at, carry):
        upward, downward = (at <= level) & has_above, (at >= level) & has_below

        def settle(use, copy, *more):
            pl.when(use)(lambda: copy(at, *more).wait_send())

        settle(upward, table_up)
        settle(downward, table_down)
        settle(upward, far_up)
        settle(downward, far_down)
        for h in range(2):
            settle(upward, up, h)
            settle(downward, down, h)
            settle(at < level, far_sum_down, h)
            settle(at > level, far_sum_up, h)
        for h in range(4):
            settle(at < level, sum_down, h)
            settle(at > level, sum_up, h)
        for copy in (to_right, to_left, back_left, back_right):
            copy(at).wait_send()
        for q in range(4):
            share(at, q).wait_send()
            give(at, q).wait_send()
        return carry

    lax.fori_loop(0, depth, drain, 0)
    for copy in (
        far_right, far_left, on_right, on_left, home_low, home_high, last_low, last_high
    ):
        copy().wait_send()
    pl.when(has_following)(lambda: to_following().wait_send())
    pl.when(has_preceding)(lambda: to_preceding().wait_send())


def dense_plan(
    mixer_input, mixer_gain, group_weight, mixer_scale,
    expert_input, expert_gain, routes, route_weight, w_gate, w_up, w_down,
):
    row_count, width = expert_input.shape
    experts = lax.axis_size("ep")
    depth = lax.axis_size("tp") // 2
    capacity = 3 * routes.shape[1] * row_count // (2 * experts)
    pad = -(-3 * experts // 16) * 16
    lanes = -(-row_count // 128) * 128
    bf16, f32 = jnp.bfloat16, jnp.float32
    low = -(-capacity // 32) * 16
    high = capacity - low
    vmem, anywhere = pl.BlockSpec(memory_space=pltpu.VMEM), pl.BlockSpec(memory_space=pl.ANY)
    compact = pltpu.VMEM((depth, capacity, width), bf16)
    dense = pltpu.VMEM((depth, row_count, width), bf16)
    result = jax.ShapeDtypeStruct((row_count, width), bf16)
    stationary = (w_gate[0], w_up[0], w_down[0], mixer_input, group_weight)
    return pl.pallas_call(
        functools.partial(stream_kernel, depth, capacity, experts),
        out_shape=(result, result),
        in_specs=[vmem] * 6 + [anywhere] * 5,
        out_specs=(vmem, vmem),
        scratch_shapes=[
            *(pltpu.VMEM(array.shape, bf16) for array in stationary),
            pltpu.VMEM((row_count + 2 * edge, width), f32),
            dense,
            pltpu.VMEM((depth, pad, lanes), bf16),
            pltpu.VMEM((depth, 4, 2, capacity, width), bf16),
            pltpu.VMEM((depth, 4, 2, capacity, width), bf16),
            pltpu.VMEM((depth, 4, capacity, width), bf16),
            compact,
            compact,
            pltpu.VMEM((capacity, width), bf16),
            pltpu.VMEM((low, width), bf16),
            pltpu.VMEM((high, width), bf16),
            compact,
            compact,
            pltpu.VMEM((depth, row_count, width), f32),
            dense,
            dense,
            dense,
            compact,
            compact,
            pltpu.VMEM((low, width), bf16),
            pltpu.VMEM((high, width), bf16),
            pltpu.VMEM((capacity, width), bf16),
            pltpu.SemaphoreType.DMA((42, depth)),
            pltpu.SemaphoreType.DMA((42, depth)),
            pltpu.SemaphoreType.DMA((len(stationary),)),
        ],
        compiler_params=pltpu.CompilerParams(
            collective_id=0, has_side_effects=True, vmem_limit_bytes=60 * 2**20
        ),
    )(
        expert_input, expert_gain.reshape(1, -1), routes.T, route_weight.T,
        mixer_gain.reshape(1, -1), mixer_scale.reshape(1, -1), *stationary,
    )


def on_device(
    mixer_input, mixer_gain, group_weight, mixer_scale,
    expert_input, expert_gain, routes, route_weight, w_gate, w_up, w_down,
):
    devices = lax.axis_size(("ep", "tp"))
    gathered_bytes = 2 * devices * expert_input.size
    square = lax.axis_size("ep") == 4 and lax.axis_size("tp") == 4 * len(ORDERS)
    if square and gathered_bytes <= vmem_share:
        return dense_plan(
            mixer_input, mixer_gain, group_weight, mixer_scale,
            expert_input, expert_gain, routes, route_weight, w_gate, w_up, w_down,
        )
    expert_out = routed_plan(
        expert_input, expert_gain, routes, route_weight, w_gate, w_up, w_down
    )
    return (mixer(mixer_input, mixer_gain, group_weight, mixer_scale), expert_out)


def solution(mesh):
    placed = (
        P(("ep", "tp"), None),
        P(),
        P(),
        P(),
        P(("ep", "tp"), None),
        P(),
        P(("ep", "tp"), None),
        P(("ep", "tp"), None),
        P("ep", None, "tp"),
        P("ep", None, "tp"),
        P("ep", "tp", None),
    )
    return jax.shard_map(
        on_device,
        mesh=mesh,
        in_specs=placed,
        out_specs=(P(("ep", "tp"), None), P(("ep", "tp"), None)),
        check_vma=False,
    )
```

```python
import functools
import math

import jax
import jax.numpy as jnp
from jax import lax
from jax.experimental import pallas as pl
from jax.experimental.pallas import tpu as pltpu
from jax.sharding import PartitionSpec as P

epsilon = 1e-06
vmem_share = 2**24
edge = 8


def padded_2(value, sides, width):
    for axis, dim in sides:
        size, length = (lax.axis_size(axis), value.shape[dim])
        up = [(i, (i + 1) % size) for i in range(size - 1)]
        down = [(j, i) for i, j in up]
        last = lax.slice_in_dim(value, length - width, length, axis=dim)
        leading = lax.slice_in_dim(value, 0, width, axis=dim)
        before = lax.ppermute(last, axis, up)
        after = lax.ppermute(leading, axis, down)
        value = jnp.concatenate([before, value, after], axis=dim)
    return value


def normalize(row_values, gain):
    values = row_values.astype(jnp.float32)
    scaled = values * lax.rsqrt(jnp.mean(values * values, axis=-1, keepdims=True) + epsilon)
    return (scaled * gain).astype(jnp.bfloat16)


def pool_groups(padded, start_row, row_count, seq_length):
    group_width = padded.shape[1] // 4
    position = start_row + jnp.arange(row_count, dtype=jnp.int32)
    centre = padded[8 : 8 + row_count]
    pooled_parts = []
    for group_index in range(4):
        window = 2 ** (group_index + 1)
        reach_left = window // 2
        reach_right = window - 1 - reach_left
        group_cols = padded[:, group_index * group_width : (group_index + 1) * group_width]
        window_sum = group_cols[8 - reach_left : 8 - reach_left + row_count]
        for offset in range(1 - reach_left, reach_right + 1):
            window_sum = window_sum + group_cols[8 + offset : 8 + offset + row_count]
        cover = (
            jnp.minimum(position + reach_right + 1, seq_length)
            - jnp.maximum(position - reach_left, 0)
        ).astype(jnp.float32)
        pooled_parts.append(
            window_sum / cover[:, None]
            - centre[:, group_index * group_width : (group_index + 1) * group_width]
        )
    return jnp.stack(pooled_parts, axis=1).astype(jnp.bfloat16)


def mixer(mixer_input, mixer_gain, group_weight, mixer_scale):
    row_count = mixer_input.shape[0]
    normed = normalize(mixer_input, mixer_gain)
    padded = padded_2(normed, ((("ep", "tp"), 0),), 8)
    start_row = lax.axis_index(("ep", "tp")) * row_count
    seq_length = row_count * lax.axis_size(("ep", "tp"))
    pooled = pool_groups(padded.astype(jnp.float32), start_row, row_count, seq_length)
    mixed_groups = jnp.einsum(
        "tgi,gio->tgo", pooled, group_weight, preferred_element_type=jnp.float32
    )
    return (mixed_groups.reshape(row_count, -1) * mixer_scale).astype(jnp.bfloat16)


def routed_plan(expert_input, expert_gain, routes, route_weight, w_gate, w_up, w_down):
    row_count = expert_input.shape[0]
    top_count = routes.shape[1]
    experts = lax.axis_size("ep") * w_gate.shape[0]
    capacity = 3 * top_count * row_count // (2 * experts)
    normed = normalize(expert_input, expert_gain)
    flat_route = routes.reshape(-1)
    onehot = (flat_route[:, None] == jnp.arange(experts, dtype=jnp.int32)[None, :]).astype(
        jnp.int32
    )
    before = jnp.cumsum(onehot, axis=0) - onehot
    slot_index = flat_route * capacity + jnp.sum(before * onehot, axis=1)
    places = (
        slot_index.reshape(row_count, top_count)[None, :, :]
        == jnp.arange(experts * capacity, dtype=jnp.int32)[:, None, None]
    )
    dispatch = jnp.any(places, axis=2).astype(jnp.bfloat16)
    outgoing = jnp.dot(dispatch, normed, preferred_element_type=jnp.float32).astype(jnp.bfloat16)
    arrived = lax.all_to_all(outgoing, "ep", split_axis=0, concat_axis=0, tiled=True)
    down_w = w_down[0]
    paired = jnp.stack((w_gate[0], w_up[0]), axis=0)
    portion = lax.all_gather(paired, "tp", axis=2, tiled=True)
    gate_part = jnp.dot(arrived, portion[0], preferred_element_type=jnp.float32)
    up_part = jnp.dot(arrived, portion[1], preferred_element_type=jnp.float32)
    hidden = (jax.nn.silu(gate_part) * up_part).astype(jnp.bfloat16)
    block_width = down_w.shape[0]
    portion = lax.all_gather(down_w, "tp", axis=0, tiled=True)
    blocks = portion.shape[0] // block_width
    hidden_part = hidden
    hidden_part = hidden_part.reshape(hidden_part.shape[0], blocks, block_width)
    block_terms = jnp.einsum(
        "rkf,kfd->krd",
        hidden_part,
        portion.reshape(blocks, block_width, portion.shape[1]),
        preferred_element_type=jnp.float32,
    )
    rounded = lax.optimization_barrier(block_terms.astype(jnp.bfloat16)).astype(jnp.float32)
    result = jnp.sum(rounded, axis=0)
    returned = lax.all_to_all(
        result.astype(jnp.bfloat16), "ep", split_axis=0, concat_axis=0, tiled=True
    )
    picked = (
        jnp.take(returned, slot_index, axis=0).astype(jnp.float32).reshape(row_count, top_count, -1)
    )
    expert_out = jnp.sum(picked * route_weight[:, :, None], axis=1).astype(jnp.bfloat16)
    return expert_out


ORDERS = (
    (
        ("D", 0, 1), ("D", 0, 0), ("X", 0, 0), ("Y", 0, 0), ("M", 0, 0), ("C", 0, 0), ("D", 1, 1),
        ("D", 1, 0), ("M", 1, 0), ("G", 0, 0), ("C", 0, 3), ("I", 0, 0), ("D", 2, 0), ("D", 2, 1),
        ("M", 2, 0), ("C", 0, 2), ("I", 1, 0), ("C", 2, 0), ("C", 1, 0), ("K", 0, 0), ("D", 3, 0),
        ("D", 3, 1), ("M", 3, 0), ("C", 0, 1), ("I", 2, 0), ("C", 1, 2), ("C", 2, 1), ("G", 1, 0),
        ("C", 2, 2), ("P", 2, 1), ("C", 1, 3), ("P", 2, 2), ("I", 3, 0), ("K", 1, 0), ("C", 1, 1),
        ("F", 1, 0), ("G", 3, 0), ("F", 1, 1), ("C", 3, 2), ("C", 3, 3), ("C", 3, 1), ("F", 3, 0),
        ("F", 3, 1), ("K", 3, 0), ("E", 2, 0), ("S", 2, 1), ("G", 2, 0), ("P", 3, 1), ("S", 2, 2),
        ("S", 2, 0), ("P", 3, 2), ("C", 2, 3), ("F", 2, 0), ("K", 2, 0), ("V", 3, 0), ("P", 1, 1),
        ("C", 3, 0), ("V", 3, 1), ("P", 1, 2), ("F", 2, 1), ("L", 2, 0), ("F", 0, 0), ("S", 2, 3),
        ("H", 0, 0), ("P", 0, 2), ("E", 3, 0), ("S", 3, 0), ("S", 3, 2), ("Q", 0, 0), ("F", 0, 1),
        ("S", 3, 1), ("L", 3, 0), ("S", 3, 3), ("Q", 0, 1), ("P", 0, 1), ("E", 1, 0), ("S", 1, 1),
        ("S", 1, 2), ("L", 1, 0), ("S", 1, 0), ("Q", 0, 3), ("S", 1, 3), ("Q", 0, 2), ("V", 0, 0),
        ("V", 0, 1), ("E", 0, 0), ("S", 0, 1), ("L", 0, 0), ("S", 0, 2), ("S", 0, 0), ("S", 0, 3),
        ("Z", 0, 0),
    ),
    (
        ("D", 1, 0), ("D", 1, 1), ("X", 1, 0), ("M", 1, 0), ("D", 0, 1), ("D", 2, 0), ("Y", 1, 0),
        ("D", 2, 1), ("M", 2, 0), ("D", 0, 0), ("C", 1, 0), ("I", 1, 0), ("D", 3, 1), ("C", 1, 1),
        ("M", 0, 0), ("C", 1, 2), ("D", 3, 0), ("C", 2, 0), ("M", 3, 0), ("G", 0, 0), ("C", 0, 0),
        ("I", 2, 0), ("G", 1, 0), ("P", 1, 2), ("P", 1, 1), ("C", 2, 1), ("C", 0, 3), ("I", 0, 0),
        ("C", 2, 2), ("G", 3, 0), ("C", 0, 1), ("C", 0, 2), ("C", 3, 3), ("K", 0, 0), ("P", 2, 1),
        ("C", 3, 0), ("G", 2, 0), ("F", 3, 0), ("I", 3, 0), ("C", 1, 3), ("F", 3, 1), ("C", 2, 3),
        ("P", 2, 2), ("C", 3, 1), ("C", 3, 2), ("P", 0, 1), ("K", 1, 0), ("H", 1, 0), ("E", 1, 0),
        ("K", 2, 0), ("F", 0, 0), ("K", 3, 0), ("P", 3, 1), ("P", 3, 2), ("P", 0, 2), ("E", 2, 0),
        ("L", 2, 0), ("F", 0, 1), ("S", 2, 1), ("L", 1, 0), ("S", 2, 0), ("S", 2, 2), ("F", 2, 0),
        ("Q", 1, 0), ("F", 2, 1), ("E", 0, 0), ("E", 3, 0), ("S", 3, 0), ("F", 1, 0), ("Q", 1, 1),
        ("S", 3, 2), ("F", 1, 1), ("L", 0, 0), ("L", 3, 0), ("Q", 1, 3), ("S", 3, 1), ("S", 0, 0),
        ("Q", 1, 2), ("S", 3, 3), ("S", 0, 2), ("S", 2, 3), ("S", 0, 1), ("V", 1, 1), ("V", 1, 0),
        ("S", 0, 3), ("S", 1, 0), ("S", 1, 2), ("S", 1, 3), ("S", 1, 1), ("Z", 1, 0),
    ),
)


def coded_orders(depth, kinds):
    base = len(kinds) * 4 * depth + 1
    per_word = 1
    while base ** (per_word + 1) < 2**31:
        per_word += 1
    idle = base - 1
    longest = max(map(len, ORDERS))
    longest += -longest % per_word
    words = []
    for order in ORDERS:
        codes = [(kinds.index(kind) * depth + at) * 4 + q for kind, at, q in order]
        codes += [idle] * (longest - len(codes))
        words.append([
            sum(code * base**n for n, code in enumerate(codes[first : first + per_word]))
            for first in range(0, len(codes), per_word)
        ])
    return words, per_word, base


def stream_kernel(
    depth, capacity, experts,
    input_ref, gain_ref, routes_ref, weight_ref, mixer_gain_ref, mixer_scale_ref,
    gate_hbm, up_hbm, down_hbm, mixer_hbm, group_hbm, mixed_ref, out_ref,
    gate_ref, up_ref, down_ref, mixer_ref, group_ref, mix, tok, tables, blk, part, from_core, out_right, out_left, out_far, relay_right, relay_left,
    from_right, from_left, local, dense, dense_above, dense_below,
    far_above, far_below, home_left, home_right, far_back,
    send_sem, recv_sem, local_sem,
):
    column, line = lax.axis_index("ep"), lax.axis_index("tp")
    level, core = line // 2, line % 2
    other = 1 - core
    rows = out_ref.shape[0]
    half, quarter = rows // 2, rows // 4
    low = -(-capacity // 32) * 16
    high = capacity - low
    piece = math.gcd(quarter, capacity)
    step_rows = math.gcd(low, high)
    right_column, left_column, far_column = (2 * column + 1) % 5, (3 * column + 2) % 5, 3 - column
    right, left = (right_column, line), (left_column, line)
    beside = (column, level * 2 + other)
    above, below = (column, line + 2), (column, line - 2)
    has_above, has_below = level < depth - 1, level > 0
    f32, bf16 = jnp.float32, jnp.bfloat16

    def link(src, dst, kind, at, target):
        return pltpu.make_async_remote_copy(
            src_ref=src, dst_ref=dst, send_sem=send_sem.at[kind, at],
            recv_sem=recv_sem.at[kind, at], device_id=target,
            device_id_type=pl.DeviceIdType.MESH,
        )

    def part_of(h):
        return pl.ds(pl.multiple_of(h * half, half), half)

    def up(at, h):
        return link(tok.at[at, part_of(h)], tok.at[at, part_of(h)], h, at, above)

    def down(at, h):
        return link(tok.at[at, part_of(h)], tok.at[at, part_of(h)], 2 + h, at, below)

    def table_up(at):
        return link(tables.at[at], tables.at[at], 4, at, above)

    def table_down(at):
        return link(tables.at[at], tables.at[at], 5, at, below)

    def to_right(at):
        return link(out_right.at[at], blk.at[at, 1, core], 6, at, right)

    def to_left(at):
        return link(out_left.at[at], blk.at[at, 2, core], 7, at, left)

    def far_right():
        return link(out_far.at[pl.ds(0, low)], relay_right, 8, 0, right)

    def far_left():
        return link(out_far.at[pl.ds(low, high)], relay_left, 9, 0, left)

    def on_right():
        return link(relay_right, blk.at[level, 3, core, pl.ds(0, low)], 10, 0, right)

    def on_left():
        return link(relay_left, blk.at[level, 3, core, pl.ds(low, high)], 11, 0, left)

    def far_up(at):
        return link(blk.at[at, 3, core], blk.at[at, 3, core], 12, at, above)

    def far_down(at):
        return link(blk.at[at, 3, core], blk.at[at, 3, core], 13, at, below)

    def share(at, q):
        return link(blk.at[at, q, core], blk.at[at, q, core], 14 + q, at, beside)

    def shared_in(at, q):
        return link(blk.at[at, q, other], blk.at[at, q, other], 14 + q, at, beside)

    def give(at, q):
        return link(part.at[at, q, other], from_core.at[at, q], 18 + q, at, beside)

    def back_left(at):
        return link(part.at[at, 1, core], from_right.at[at], 22, at, left)

    def back_right(at):
        return link(part.at[at, 2, core], from_left.at[at], 23, at, right)

    def fourth(h):
        return pl.ds(pl.multiple_of(h * quarter, quarter), quarter)

    def sum_down(at, h):
        return link(dense.at[at, fourth(h)], dense_above.at[at, fourth(h)], 24 + h, at, below)

    def sum_up(at, h):
        return link(dense.at[at, fourth(h)], dense_below.at[at, fourth(h)], 28 + h, at, above)

    cuts = (pl.ds(0, low), pl.ds(low, high))

    def far_sum_down(at, h):
        return link(part.at[at, 3, core, cuts[h]], far_above.at[at, cuts[h]], 32 + h, at, below)

    def far_sum_up(at, h):
        return link(part.at[at, 3, core, cuts[h]], far_below.at[at, cuts[h]], 34 + h, at, above)

    def home_low(at):
        return link(part.at[at, 3, core, cuts[0]], home_left.at[at], 36, at, left)

    def home_high(at):
        return link(part.at[at, 3, core, cuts[1]], home_right.at[at], 37, at, right)

    def last_low(at):
        return link(home_left.at[at], far_back.at[at, cuts[0]], 38, at, left)

    def last_high(at):
        return link(home_right.at[at], far_back.at[at, cuts[1]], 39, at, right)

    def crosses(at):
        return (at == level) | (at - level >= depth - 1) | (level - at >= depth - 1)

    place = column * 2 * depth + line
    last_place = lax.axis_size("ep") * 2 * depth - 1
    first_line, last_line = line == 0, line == 2 * depth - 1
    following = (column + jnp.where(last_line, 1, 0), jnp.where(last_line, 0, line + 1))
    preceding = (column - jnp.where(first_line, 1, 0), jnp.where(first_line, 2 * depth - 1, line - 1))
    has_following, has_preceding = place < last_place, place > 0

    def to_following():
        return link(mix.at[pl.ds(rows, edge)], mix.at[pl.ds(0, edge)], 40, 0, following)

    def to_preceding():
        return link(
            mix.at[pl.ds(edge, edge)], mix.at[pl.ds(edge + rows, edge)], 41, 0, preceding
        )

    loads = [
        pltpu.make_async_copy(src, dst, local_sem.at[n])
        for n, (src, dst) in enumerate((
            (gate_hbm, gate_ref), (up_hbm, up_ref), (down_hbm, down_ref),
            (mixer_hbm, mixer_ref), (group_hbm, group_ref),
        ))
    ]
    def by_piece(start, count, width, body):
        def one(i, carry):
            body(pl.ds(pl.multiple_of(start + i * width, width), width))
            return carry

        lax.fori_loop(0, count // width, one, 0)

    barrier = pltpu.get_barrier_semaphore()

    def greet(target):
        pl.semaphore_signal(
            barrier, inc=1, device_id=target, device_id_type=pl.DeviceIdType.MESH
        )

    greet(right)
    greet(left)
    greet(beside)
    pl.when(has_above)(lambda: greet(above))
    pl.when(has_below)(lambda: greet(below))
    for load in loads:
        load.start()

    def normed(values, gains):
        values = values.astype(f32)
        mean = jnp.sum(values * values, axis=1, keepdims=True) / values.shape[1]
        return (values * lax.rsqrt(mean + epsilon) * gains).astype(bf16)

    def own_rows(span):
        tok[level, span] = normed(input_ref[span], gain_ref[...])

    by_piece(0, rows, piece, own_rows)
    sort = lax.broadcasted_iota(jnp.int32, (tables.shape[1], rows), 0)
    first = sort % experts == routes_ref[0:1, :]
    second = sort % experts == routes_ref[1:2, :]
    weights = jnp.where(first, weight_ref[0:1, :], 0.0) + jnp.where(second, weight_ref[1:2, :], 0.0)
    named = first | second
    earlier = lax.broadcasted_iota(jnp.int32, (rows, rows), 0) < lax.broadcasted_iota(
        jnp.int32, (rows, rows), 1
    )
    turns = jnp.dot(
        jnp.where(named, 1.0, 0.0).astype(bf16), jnp.where(earlier, 1.0, 0.0).astype(bf16),
        preferred_element_type=f32,
    )
    turns = jnp.where(named, turns, -1.0).astype(bf16)
    coarse = weights.astype(bf16)
    fine = (weights - coarse.astype(f32)).astype(bf16)
    group = sort // experts
    listed = jnp.where(
        group == 0, turns.astype(f32), jnp.where(group == 1, coarse.astype(f32), fine.astype(f32))
    )
    tables[level, :, pl.ds(0, rows)] = listed.astype(bf16)
    tables[level, :, pl.ds(rows, tables.shape[2] - rows)] = jnp.zeros(
        (tables.shape[1], tables.shape[2] - rows), bf16
    )
    pl.semaphore_wait(barrier, 3 + jnp.where(has_above, 1, 0) + jnp.where(has_below, 1, 0))

    def table(at):
        listed = tables[at, :, pl.ds(0, rows)].astype(f32)
        listing = lax.broadcasted_iota(jnp.int32, listed.shape, 0)
        index = lax.broadcasted_iota(jnp.int32, (capacity, rows), 0).astype(f32)

        def row_of(at_row):
            return jnp.sum(jnp.where(listing == at_row, listed, 0.0), axis=0, keepdims=True)

        def hits(expert):
            return index == row_of(expert)

        return row_of, hits

    def picked(at, chosen):
        _, hits = table(at)
        picks = [jnp.where(hits(expert), 1.0, 0.0).astype(bf16) for expert in chosen]
        return jnp.dot(
            jnp.concatenate(picks, axis=0), tok[at], preferred_element_type=f32
        ).astype(bf16)

    def placed(at, chosen, results):
        row_of, hits = table(at)
        total = None
        for kind in (1, 2):
            weights = [
                jnp.where(hits(expert), row_of(kind * experts + expert), 0.0).astype(bf16)
                for expert in chosen
            ]
            term = lax.dot_general(
                jnp.concatenate(weights, axis=0), results,
                (((0,), (0,)), ((), ())), preferred_element_type=f32,
            )
            total = term if total is None else total + term
        return total

    def compute(at, q):
        gathered = jnp.concatenate([blk[at, q, 0], blk[at, q, 1]], axis=0)
        gate_part = jnp.dot(gathered, gate_ref[...], preferred_element_type=f32)
        up_part = jnp.dot(gathered, up_ref[...], preferred_element_type=f32)
        hidden = (gate_part / (1.0 + jnp.exp(-gate_part)) * up_part).astype(bf16)
        partial = jnp.dot(hidden, down_ref[...], preferred_element_type=f32).astype(bf16)
        for lane in range(2):
            part[at, q, lane] = partial[lane * capacity : (lane + 1) * capacity]

    def paired(at, q):
        give(at, q).wait_recv()

        def body(span):
            total = part[at, q, core, span].astype(f32) + from_core[at, q, span].astype(f32)
            part[at, q, core, span] = total.astype(bf16)

        by_piece(0, capacity, piece, body)

    def with_incoming(above_too, below_too, action):
        both = above_too & below_too
        pl.when(both)(lambda: action(True, True))
        pl.when(above_too & jnp.logical_not(both))(lambda: action(True, False))
        pl.when(below_too & jnp.logical_not(both))(lambda: action(False, True))
        pl.when(jnp.logical_not(above_too | below_too))(lambda: action(False, False))

    def far_total(at, h):
        above_too = (at <= level) & has_above & (level + 1 - at < depth - 1)
        below_too = (at >= level) & has_below & (at - level + 1 < depth - 1)
        over = crosses(at)
        above_too, below_too = (
            above_too & ((at == level) | jnp.logical_not(over)),
            below_too & ((at == level) | jnp.logical_not(over)),
        )
        pl.when(above_too)(lambda: far_sum_down(at, h).wait_recv())
        pl.when(below_too)(lambda: far_sum_up(at, h).wait_recv())

        def action(from_up, from_down):
            def body(span):
                total = part[at, 3, core, span].astype(f32) + from_core[at, 3, span].astype(f32)
                if from_up:
                    total = total + far_above[at, span].astype(f32)
                if from_down:
                    total = total + far_below[at, span].astype(f32)
                part[at, 3, core, span] = total.astype(bf16)

            by_piece((0, low)[h], (low, high)[h], step_rows, body)

        with_incoming(above_too, below_too, action)
        chained = jnp.logical_not(over)
        pl.when(chained & (at < level))(lambda: far_sum_down(at, h).start())
        pl.when(chained & (at > level))(lambda: far_sum_up(at, h).start())
        pl.when(over)(lambda: (home_low, home_high)[h](at).start())

    def far_step(at, h):
        pl.when(h == 0)(lambda: give(at, 3).wait_recv())
        pl.when(h == 0)(lambda: far_total(at, 0))
        pl.when(h == 1)(lambda: far_total(at, 1))

    def dense_step(at, h):
        above_too, below_too = (at <= level) & has_above, (at >= level) & has_below
        pl.when(above_too)(lambda: sum_down(at, h).wait_recv())
        pl.when(below_too)(lambda: sum_up(at, h).wait_recv())

        def action(from_up, from_down):
            def body(span):
                total = local[at, span]
                if from_up:
                    total = total + dense_above[at, span].astype(f32)
                if from_down:
                    total = total + dense_below[at, span].astype(f32)
                dense[at, span] = total.astype(bf16)

            by_piece(h * quarter, quarter, piece, body)

        with_incoming(above_too, below_too, action)
        pl.when(at < level)(lambda: sum_down(at, h).start())
        pl.when(at > level)(lambda: sum_up(at, h).start())

    def expand(at, _):
        give(at, 0).wait_recv()
        back_left(at).wait_recv()
        back_right(at).wait_recv()
        own = (part[at, 0, core].astype(f32) + from_core[at, 0].astype(f32)).astype(bf16)
        results = [own, from_right[at], from_left[at]]
        chosen = (column, right_column, left_column)
        four = crosses(at) & (at != level)

        @pl.when(four)
        def _():
            last_low(at).wait_recv()
            last_high(at).wait_recv()
            every = jnp.concatenate([*results, far_back[at]], axis=0)
            local[at] = placed(at, (*chosen, far_column), every)

        @pl.when(jnp.logical_not(four))
        def _():
            local[at] = placed(at, chosen, jnp.concatenate(results, axis=0))

    def arrive(at, h):
        upward, downward = (at <= level) & has_above, (at >= level) & has_below

        @pl.when(h == 0)
        def _():
            pl.when(at < level)(lambda: table_up(at).wait_recv())
            pl.when(at > level)(lambda: table_down(at).wait_recv())
            pl.when(upward)(lambda: table_up(at).start())
            pl.when(downward)(lambda: table_down(at).start())

        pl.when(at < level)(lambda: up(at, h).wait_recv())
        pl.when(at > level)(lambda: down(at, h).wait_recv())
        pl.when(upward)(lambda: up(at, h).start())
        pl.when(downward)(lambda: down(at, h).start())

    def far_out(at, _):
        out_far[...] = picked(at, (far_column,))
        far_right().start()
        far_left().start()
        for load in loads[:3]:
            load.wait()

    def relay(at, _):
        far_right().wait_recv()
        on_right().start()
        far_left().wait_recv()
        on_left().start()

    def sides_out(at, _):
        sent = picked(at, (right_column, left_column, column))
        out_right[at] = sent[:capacity]
        out_left[at] = sent[capacity : 2 * capacity]
        to_right(at).start()
        to_left(at).start()
        blk[at, 0, core] = sent[2 * capacity :]
        share(at, 0).start()

    def sides_in(at, _):
        to_right(at).wait_recv()
        share(at, 1).start()
        to_left(at).wait_recv()
        share(at, 2).start()

    def far_in(at, _):
        @pl.when(at == level)
        def _():
            on_right().wait_recv()
            on_left().wait_recv()

        pl.when(at < level)(lambda: far_up(at).wait_recv())
        pl.when(at > level)(lambda: far_down(at).wait_recv())
        pl.when((at <= level) & has_above)(lambda: far_up(at).start())
        pl.when((at >= level) & has_below)(lambda: far_down(at).start())
        share(at, 3).start()

    def multiply(at, q):
        shared_in(at, q).wait_recv()
        compute(at, q)
        give(at, q).start()

    def back(at, q):
        paired(at, q)
        pl.when(q == 1)(lambda: back_left(at).start())
        pl.when(q == 2)(lambda: back_right(at).start())

    def home_relay(at, h):
        @pl.when(h == 0)
        def _():
            home_low(at).wait_recv()
            last_low(at).start()

        @pl.when(h == 1)
        def _():
            home_high(at).wait_recv()
            last_high(at).start()

    def finish(at, _):
        last_low(level).wait_recv()
        last_high(level).wait_recv()
        total = placed(level, (far_column,), far_back[level])
        out_ref[...] = (dense[level].astype(f32) + total).astype(bf16)

    def mixer_rows(at, _):
        for load in loads[3:]:
            load.wait()

        def body(i, carry):
            start = pl.multiple_of(i * piece, piece)
            values = normed(mixer_ref[pl.ds(start, piece)], mixer_gain_ref[...])
            mix[pl.ds(pl.multiple_of(start + edge, edge), piece)] = values.astype(f32)
            return carry

        lax.fori_loop(0, rows // piece, body, 0)
        zeros = jnp.zeros((edge, mix.shape[1]), f32)

        @pl.when(jnp.logical_not(has_preceding))
        def _():
            mix[pl.ds(0, edge)] = zeros

        @pl.when(jnp.logical_not(has_following))
        def _():
            mix[pl.ds(edge + rows, edge)] = zeros

        pl.when(has_following)(lambda: to_following().start())
        pl.when(has_preceding)(lambda: to_preceding().start())

    def mixer_group(number):
        width = group_ref.shape[1]
        span = pl.ds(number * width, width)
        window = 2 ** (number + 1)
        values = mix[:, span]
        length = values.shape[0]
        total = values
        for level_of_sum in range(number + 1):
            total = total + pltpu.roll(total, length - 2**level_of_sum, 0)
        total = pltpu.roll(total, window // 2, 0)[edge : edge + rows]
        position = place * rows + lax.broadcasted_iota(jnp.int32, (rows, width), 0)
        ahead = jnp.minimum(position + window // 2, (last_place + 1) * rows)
        cover = (ahead - jnp.maximum(position - window // 2, 0)).astype(f32)
        pooled = (total / cover - values[edge : edge + rows]).astype(bf16)
        product = jnp.dot(pooled, group_ref[number], preferred_element_type=f32)
        mixed_ref[:, span] = (product * mixer_scale_ref[:, span]).astype(bf16)

    def mixer_step(at, q):
        @pl.when(q == 0)
        def _():
            pl.when(has_preceding)(lambda: to_following().wait_recv())
            pl.when(has_following)(lambda: to_preceding().wait_recv())

        for number in range(4):
            pl.when(q == number)(functools.partial(mixer_group, number))

    def settle(use, copy, *more):
        pl.when(use)(lambda: copy(*more).wait_send())

    def settle_out(at, _):
        upward, downward = (at <= level) & has_above, (at >= level) & has_below
        for copy in (table_up, far_up):
            settle(upward, copy, at)
        for copy in (table_down, far_down):
            settle(downward, copy, at)
        for h in range(2):
            settle(upward, up, at, h)
            settle(downward, down, at, h)
        for copy in (to_right, to_left):
            copy(at).wait_send()
        for q in range(4):
            share(at, q).wait_send()

        @pl.when(at == level)
        def _():
            for copy in (far_right, far_left, on_right, on_left):
                copy().wait_send()

    def settle_back(at, _):
        for copy in (back_left, back_right):
            copy(at).wait_send()
        for q in range(4):
            give(at, q).wait_send()

    actions = dict(
        D=arrive, M=sides_out, I=sides_in, G=far_in,
        C=multiply, P=back, F=far_step, S=dense_step,
        E=expand, X=far_out, Y=relay, V=home_relay, Z=finish,
        H=mixer_rows, Q=mixer_step, K=settle_out, L=settle_back,
    )
    kinds = list(actions)
    words, per_word, base = coded_orders(depth, kinds)
    mirrored = level >= depth // 2
    row = jnp.where(mirrored, depth - 1 - level, level)

    def one_word(place, carry):
        word = 0
        for at, listing in enumerate(words):
            for turn, value in enumerate(listing):
                word = word + jnp.where((row == at) & (place == turn), value, 0)

        def one_step(_, rest):
            code = rest % base
            kind, at, q = code // (4 * depth), code // 4 % depth, code % 4
            at = jnp.where(mirrored, depth - 1 - at, at)
            for first in range(0, len(kinds), 4):

                @pl.when((kind >= first) & (kind < first + 4))
                def _():
                    for number in range(first, min(first + 4, len(kinds))):
                        pl.when(kind == number)(
                            functools.partial(actions[kinds[number]], at, q)
                        )

            return rest // base

        lax.fori_loop(0, per_word, one_step, word)
        return carry

    lax.fori_loop(0, len(words[0]), one_word, 0)

    def drain(at, carry):
        over = crosses(at)
        chained = jnp.logical_not(over)

        @pl.when(at < level)
        def _():
            for h in range(4):
                sum_down(at, h).wait_send()
            for h in range(2):
                settle(chained, far_sum_down, at, h)

        @pl.when(at > level)
        def _():
            for h in range(4):
                sum_up(at, h).wait_send()
            for h in range(2):
                settle(chained, far_sum_up, at, h)

        @pl.when(over)
        def _():
            for copy in (home_low, home_high, last_low, last_high):
                copy(at).wait_send()

        return carry

    lax.fori_loop(0, depth, drain, 0)
    pl.when(has_following)(lambda: to_following().wait_send())
    pl.when(has_preceding)(lambda: to_preceding().wait_send())


def dense_plan(
    mixer_input, mixer_gain, group_weight, mixer_scale,
    expert_input, expert_gain, routes, route_weight, w_gate, w_up, w_down,
):
    row_count, width = expert_input.shape
    experts = lax.axis_size("ep")
    depth = lax.axis_size("tp") // 2
    capacity = 3 * routes.shape[1] * row_count // (2 * experts)
    pad = -(-3 * experts // 16) * 16
    lanes = -(-row_count // 128) * 128
    bf16, f32 = jnp.bfloat16, jnp.float32
    low = -(-capacity // 32) * 16
    high = capacity - low
    vmem, anywhere = pl.BlockSpec(memory_space=pltpu.VMEM), pl.BlockSpec(memory_space=pl.ANY)
    compact = pltpu.VMEM((depth, capacity, width), bf16)
    dense = pltpu.VMEM((depth, row_count, width), bf16)
    held = pltpu.VMEM((row_count, width), bf16)
    stationary = (w_gate[0], w_up[0], w_down[0], mixer_input, group_weight)
    return pl.pallas_call(
        functools.partial(stream_kernel, depth, capacity, experts),
        out_shape=(held, held),
        in_specs=[vmem] * 6 + [anywhere] * 5,
        out_specs=(vmem, vmem),
        scratch_shapes=[
            *(pltpu.VMEM(array.shape, bf16) for array in stationary),
            pltpu.VMEM((row_count + 2 * edge, width), f32),
            dense,
            pltpu.VMEM((depth, pad, lanes), bf16),
            pltpu.VMEM((depth, 4, 2, capacity, width), bf16),
            pltpu.VMEM((depth, 4, 2, capacity, width), bf16),
            pltpu.VMEM((depth, 4, capacity, width), bf16),
            compact,
            compact,
            pltpu.VMEM((capacity, width), bf16),
            pltpu.VMEM((low, width), bf16),
            pltpu.VMEM((high, width), bf16),
            compact,
            compact,
            pltpu.VMEM((depth, row_count, width), f32),
            dense,
            dense,
            dense,
            compact,
            compact,
            pltpu.VMEM((depth, low, width), bf16),
            pltpu.VMEM((depth, high, width), bf16),
            compact,
            pltpu.SemaphoreType.DMA((42, depth)),
            pltpu.SemaphoreType.DMA((42, depth)),
            pltpu.SemaphoreType.DMA((len(stationary),)),
        ],
        compiler_params=pltpu.CompilerParams(
            collective_id=0, has_side_effects=True, vmem_limit_bytes=60 * 2**20
        ),
    )(
        expert_input, expert_gain.reshape(1, -1), routes.T, route_weight.T,
        mixer_gain.reshape(1, -1), mixer_scale.reshape(1, -1), *stationary,
    )


def on_device(
    mixer_input, mixer_gain, group_weight, mixer_scale,
    expert_input, expert_gain, routes, route_weight, w_gate, w_up, w_down,
):
    devices = lax.axis_size(("ep", "tp"))
    gathered_bytes = 2 * devices * expert_input.size
    square = lax.axis_size("ep") == 4 and lax.axis_size("tp") == 4 * len(ORDERS)
    if square and gathered_bytes <= vmem_share:
        return dense_plan(
            mixer_input, mixer_gain, group_weight, mixer_scale,
            expert_input, expert_gain, routes, route_weight, w_gate, w_up, w_down,
        )
    expert_out = routed_plan(
        expert_input, expert_gain, routes, route_weight, w_gate, w_up, w_down
    )
    return (mixer(mixer_input, mixer_gain, group_weight, mixer_scale), expert_out)


def solution(mesh):
    placed = (
        P(("ep", "tp"), None),
        P(),
        P(),
        P(),
        P(("ep", "tp"), None),
        P(),
        P(("ep", "tp"), None),
        P(("ep", "tp"), None),
        P("ep", None, "tp"),
        P("ep", None, "tp"),
        P("ep", "tp", None),
    )
    return jax.shard_map(
        on_device,
        mesh=mesh,
        in_specs=placed,
        out_specs=(P(("ep", "tp"), None), P(("ep", "tp"), None)),
        check_vma=False,
    )
```

```python
import functools
import math

import jax
import jax.numpy as jnp
from jax import lax
from jax.experimental import pallas as pl
from jax.experimental.pallas import tpu as pltpu
from jax.sharding import PartitionSpec as P

epsilon = 1e-06
vmem_share = 2**24
edge = 8


def padded_2(value, sides, width):
    for axis, dim in sides:
        size, length = (lax.axis_size(axis), value.shape[dim])
        up = [(i, (i + 1) % size) for i in range(size - 1)]
        down = [(j, i) for i, j in up]
        last = lax.slice_in_dim(value, length - width, length, axis=dim)
        leading = lax.slice_in_dim(value, 0, width, axis=dim)
        before = lax.ppermute(last, axis, up)
        after = lax.ppermute(leading, axis, down)
        value = jnp.concatenate([before, value, after], axis=dim)
    return value


def normalize(row_values, gain):
    values = row_values.astype(jnp.float32)
    scaled = values * lax.rsqrt(jnp.mean(values * values, axis=-1, keepdims=True) + epsilon)
    return (scaled * gain).astype(jnp.bfloat16)


def pool_groups(padded, start_row, row_count, seq_length):
    group_width = padded.shape[1] // 4
    position = start_row + jnp.arange(row_count, dtype=jnp.int32)
    centre = padded[8 : 8 + row_count]
    pooled_parts = []
    for group_index in range(4):
        window = 2 ** (group_index + 1)
        reach_left = window // 2
        reach_right = window - 1 - reach_left
        group_cols = padded[:, group_index * group_width : (group_index + 1) * group_width]
        window_sum = group_cols[8 - reach_left : 8 - reach_left + row_count]
        for offset in range(1 - reach_left, reach_right + 1):
            window_sum = window_sum + group_cols[8 + offset : 8 + offset + row_count]
        cover = (
            jnp.minimum(position + reach_right + 1, seq_length)
            - jnp.maximum(position - reach_left, 0)
        ).astype(jnp.float32)
        pooled_parts.append(
            window_sum / cover[:, None]
            - centre[:, group_index * group_width : (group_index + 1) * group_width]
        )
    return jnp.stack(pooled_parts, axis=1).astype(jnp.bfloat16)


def mixer(mixer_input, mixer_gain, group_weight, mixer_scale):
    row_count = mixer_input.shape[0]
    normed = normalize(mixer_input, mixer_gain)
    padded = padded_2(normed, ((("ep", "tp"), 0),), 8)
    start_row = lax.axis_index(("ep", "tp")) * row_count
    seq_length = row_count * lax.axis_size(("ep", "tp"))
    pooled = pool_groups(padded.astype(jnp.float32), start_row, row_count, seq_length)
    mixed_groups = jnp.einsum(
        "tgi,gio->tgo", pooled, group_weight, preferred_element_type=jnp.float32
    )
    return (mixed_groups.reshape(row_count, -1) * mixer_scale).astype(jnp.bfloat16)


def routed_plan(expert_input, expert_gain, routes, route_weight, w_gate, w_up, w_down):
    row_count = expert_input.shape[0]
    top_count = routes.shape[1]
    experts = lax.axis_size("ep") * w_gate.shape[0]
    capacity = 3 * top_count * row_count // (2 * experts)
    normed = normalize(expert_input, expert_gain)
    flat_route = routes.reshape(-1)
    onehot = (flat_route[:, None] == jnp.arange(experts, dtype=jnp.int32)[None, :]).astype(
        jnp.int32
    )
    before = jnp.cumsum(onehot, axis=0) - onehot
    slot_index = flat_route * capacity + jnp.sum(before * onehot, axis=1)
    places = (
        slot_index.reshape(row_count, top_count)[None, :, :]
        == jnp.arange(experts * capacity, dtype=jnp.int32)[:, None, None]
    )
    dispatch = jnp.any(places, axis=2).astype(jnp.bfloat16)
    outgoing = jnp.dot(dispatch, normed, preferred_element_type=jnp.float32).astype(jnp.bfloat16)
    arrived = lax.all_to_all(outgoing, "ep", split_axis=0, concat_axis=0, tiled=True)
    down_w = w_down[0]
    paired = jnp.stack((w_gate[0], w_up[0]), axis=0)
    portion = lax.all_gather(paired, "tp", axis=2, tiled=True)
    gate_part = jnp.dot(arrived, portion[0], preferred_element_type=jnp.float32)
    up_part = jnp.dot(arrived, portion[1], preferred_element_type=jnp.float32)
    hidden = (jax.nn.silu(gate_part) * up_part).astype(jnp.bfloat16)
    block_width = down_w.shape[0]
    portion = lax.all_gather(down_w, "tp", axis=0, tiled=True)
    blocks = portion.shape[0] // block_width
    hidden_part = hidden
    hidden_part = hidden_part.reshape(hidden_part.shape[0], blocks, block_width)
    block_terms = jnp.einsum(
        "rkf,kfd->krd",
        hidden_part,
        portion.reshape(blocks, block_width, portion.shape[1]),
        preferred_element_type=jnp.float32,
    )
    rounded = lax.optimization_barrier(block_terms.astype(jnp.bfloat16)).astype(jnp.float32)
    result = jnp.sum(rounded, axis=0)
    returned = lax.all_to_all(
        result.astype(jnp.bfloat16), "ep", split_axis=0, concat_axis=0, tiled=True
    )
    picked = (
        jnp.take(returned, slot_index, axis=0).astype(jnp.float32).reshape(row_count, top_count, -1)
    )
    expert_out = jnp.sum(picked * route_weight[:, :, None], axis=1).astype(jnp.bfloat16)
    return expert_out


ORDERS = (
    (
        ("D", 0, 1), ("D", 0, 0), ("X", 0, 0), ("M", 0, 0), ("Y", 0, 0), ("D", 1, 0), ("D", 1, 1),
        ("M", 1, 0), ("I", 0, 0), ("C", 1, 0), ("G", 0, 0), ("C", 0, 2), ("C", 0, 1), ("D", 2, 0),
        ("D", 2, 1), ("M", 2, 0), ("I", 1, 0), ("K", 0, 0), ("C", 1, 1), ("D", 3, 1), ("C", 2, 0),
        ("D", 3, 0), ("M", 3, 0), ("I", 2, 0), ("C", 1, 2), ("C", 2, 1), ("C", 2, 2), ("C", 0, 3),
        ("G", 1, 0), ("P", 2, 2), ("P", 2, 1), ("I", 3, 0), ("C", 1, 3), ("C", 3, 1), ("F", 1, 0),
        ("C", 3, 2), ("F", 1, 1), ("P", 3, 1), ("K", 1, 0), ("G", 3, 0), ("C", 0, 0), ("P", 3, 2),
        ("C", 3, 3), ("E", 2, 0), ("S", 2, 3), ("C", 3, 0), ("S", 2, 2), ("S", 2, 1), ("G", 2, 0),
        ("F", 3, 0), ("F", 3, 1), ("C", 2, 3), ("F", 2, 0), ("K", 3, 0), ("V", 3, 0), ("K", 2, 0),
        ("L", 3, 0), ("V", 3, 1), ("P", 1, 2), ("F", 2, 1), ("H", 0, 0), ("S", 2, 0), ("P", 1, 1),
        ("F", 0, 0), ("E", 3, 0), ("S", 3, 1), ("S", 3, 3), ("S", 3, 2), ("F", 0, 1), ("S", 3, 0),
        ("Q", 0, 0), ("P", 0, 2), ("Q", 0, 3), ("E", 1, 0), ("S", 1, 1), ("P", 0, 1), ("V", 0, 1),
        ("S", 1, 3), ("L", 2, 0), ("L", 1, 0), ("S", 1, 0), ("V", 0, 0), ("Q", 0, 2), ("Q", 0, 1),
        ("S", 1, 2), ("E", 0, 0), ("S", 0, 1), ("S", 0, 3), ("S", 0, 2), ("L", 0, 0), ("S", 0, 0),
        ("Z", 0, 0),
    ),
    (
        ("D", 1, 0), ("D", 1, 1), ("X", 1, 0), ("M", 1, 0), ("D", 0, 1), ("C", 1, 0), ("Y", 1, 0),
        ("D", 2, 0), ("D", 0, 0), ("D", 2, 1), ("M", 2, 0), ("M", 0, 0), ("I", 1, 0), ("D", 3, 1),
        ("C", 1, 1), ("C", 1, 2), ("D", 3, 0), ("C", 2, 0), ("M", 3, 0), ("P", 1, 2), ("I", 2, 0),
        ("C", 3, 0), ("G", 0, 0), ("P", 1, 1), ("C", 2, 2), ("G", 1, 0), ("C", 2, 1), ("I", 0, 0),
        ("C", 0, 0), ("C", 0, 2), ("G", 3, 0), ("C", 0, 1), ("P", 2, 2), ("I", 3, 0), ("C", 3, 3),
        ("C", 0, 3), ("P", 0, 2), ("C", 3, 2), ("G", 2, 0), ("F", 3, 0), ("P", 2, 1), ("F", 3, 1),
        ("P", 0, 1), ("C", 3, 1), ("P", 3, 1), ("K", 1, 0), ("C", 1, 3), ("L", 1, 0), ("C", 2, 3),
        ("K", 3, 0), ("F", 0, 0), ("E", 1, 0), ("F", 0, 1), ("K", 2, 0), ("E", 2, 0), ("H", 1, 0),
        ("S", 2, 3), ("L", 2, 0), ("P", 3, 2), ("S", 2, 1), ("S", 2, 2), ("F", 2, 0), ("F", 2, 1),
        ("E", 3, 0), ("L", 0, 0), ("Q", 1, 0), ("E", 0, 0), ("K", 0, 0), ("F", 1, 0), ("L", 3, 0),
        ("S", 3, 1), ("Q", 1, 2), ("Q", 1, 1), ("F", 1, 1), ("S", 3, 3), ("S", 3, 2), ("S", 0, 1),
        ("V", 1, 0), ("S", 3, 0), ("S", 0, 3), ("S", 0, 2), ("S", 1, 1), ("S", 2, 0), ("V", 1, 1),
        ("Q", 1, 3), ("S", 0, 0), ("S", 1, 3), ("S", 1, 0), ("S", 1, 2), ("Z", 1, 0),
    ),
)


def coded_orders(depth, kinds):
    base = len(kinds) * 4 * depth + 1
    per_word = 1
    while base ** (per_word + 1) < 2**31:
        per_word += 1
    idle = base - 1
    longest = max(map(len, ORDERS))
    longest += -longest % per_word
    words = []
    for order in ORDERS:
        codes = [(kinds.index(kind) * depth + at) * 4 + q for kind, at, q in order]
        codes += [idle] * (longest - len(codes))
        words.append([
            sum(code * base**n for n, code in enumerate(codes[first : first + per_word]))
            for first in range(0, len(codes), per_word)
        ])
    return words, per_word, base


def slot_tables(depth):
    def offsets(**sizes):
        table, count = {}, 0
        for name, size in sizes.items():
            table[name], count = count, count + size
        return dict(table, count=count)

    sends = offsets(
        rows=depth + 1, table=depth + 1, farther=depth + 1, sides=depth, share=depth,
        give=depth, back=depth, sum=depth, farsum=depth, far=1, on=1, home=2, last=2, halo=2,
    )
    receives = offsets(
        rows=2 * depth, table=depth, farther=depth, sides=depth, share=4 * depth,
        give=4 * depth, back=depth, sum=4 * depth + 4, farsum=2 * depth + 2,
        far=1, on=1, home=4, last=2, halo=2,
    )
    return sends, receives


def stream_kernel(
    depth, capacity, experts, stores,
    *refs,
):
    stored, refs = refs[:stores], refs[stores:]
    mixed_ref, out_ref, *refs = refs
    held, refs = refs[:stores], refs[stores:]
    (
        input_ref, gain_ref, routes_ref, weight_ref, gate_ref, up_ref, down_ref,
        mixer_ref, group_ref, mixer_gain_ref, mixer_scale_ref,
    ) = held
    (
        mix, tok, tables, blk, part, from_core, sides, out_far, passing,
        from_sides, local, dense, dense_above, dense_below,
        far_above, far_below, home, far_back,
        send_sem, recv_sem, local_sem,
    ) = refs
    column, line = lax.axis_index("ep"), lax.axis_index("tp")
    level, core = line // 2, line % 2
    other = 1 - core
    rows = out_ref.shape[0]
    half, quarter = rows // 2, rows // 4
    low = -(-capacity // 32) * 16
    high = capacity - low
    piece = math.gcd(quarter, capacity)
    step_rows = math.gcd(low, high)
    right_column, left_column, far_column = (2 * column + 1) % 5, (3 * column + 2) % 5, 3 - column
    right, left = (right_column, line), (left_column, line)
    beside = (column, level * 2 + other)
    above, below = (column, line + 2), (column, line - 2)
    has_above, has_below = level < depth - 1, level > 0
    f32, bf16 = jnp.float32, jnp.bfloat16

    def link(src, dst, sent, got, target):
        return pltpu.make_async_remote_copy(
            src_ref=src, dst_ref=dst, send_sem=send_sem.at[sent],
            recv_sem=recv_sem.at[got], device_id=target,
            device_id_type=pl.DeviceIdType.MESH,
        )

    sends, receives = slot_tables(depth)

    def twin(at, where):
        return jnp.where(at == where, depth, at)

    def part_of(h):
        return pl.ds(pl.multiple_of(h * half, half), half)

    def fourth(h):
        return pl.ds(pl.multiple_of(h * quarter, quarter), quarter)

    cuts = (pl.ds(0, low), pl.ds(low, high))

    def up(at, h):
        span = tok.at[at, part_of(h)]
        return link(span, span, sends["rows"] + at, receives["rows"] + 2 * at + h, above)

    def down(at, h):
        span, sent = tok.at[at, part_of(h)], sends["rows"] + twin(at, level)
        return link(span, span, sent, receives["rows"] + 2 * at + h, below)

    def all_up(at):
        return link(tok.at[at], tok.at[at], sends["rows"] + at, receives["rows"], above)

    def all_down(at):
        sent = sends["rows"] + twin(at, level)
        return link(tok.at[at], tok.at[at], sent, receives["rows"], below)

    def table_up(at):
        table = tables.at[at]
        return link(table, table, sends["table"] + at, receives["table"] + at, above)

    def table_down(at):
        table, sent = tables.at[at], sends["table"] + twin(at, level)
        return link(table, table, sent, receives["table"] + at, below)

    def to_right(at):
        sent, got = sends["sides"] + at, receives["sides"] + at
        return link(sides.at[at, 0], blk.at[at, 1, core], sent, got, right)

    def to_left(at):
        sent, got = sends["sides"] + at, receives["sides"] + at
        return link(sides.at[at, 1], blk.at[at, 2, core], sent, got, left)

    def all_sides(at):
        sent, got = sends["sides"] + at, receives["sides"] + at
        return link(sides.at[at], blk.at[at, pl.ds(1, 2), core], sent, got, right)

    def far_right():
        span = cuts[0]
        return link(out_far.at[span], passing.at[span], sends["far"], receives["far"], right)

    def far_left():
        span = cuts[1]
        return link(out_far.at[span], passing.at[span], sends["far"], receives["far"], left)

    def all_far():
        return link(out_far, passing, sends["far"], receives["far"], right)

    def on_right():
        there = blk.at[level, 3, core, cuts[0]]
        return link(passing.at[cuts[0]], there, sends["on"], receives["on"], right)

    def on_left():
        there = blk.at[level, 3, core, cuts[1]]
        return link(passing.at[cuts[1]], there, sends["on"], receives["on"], left)

    def all_on():
        return link(passing, blk.at[level, 3, core], sends["on"], receives["on"], right)

    def far_up(at):
        block = blk.at[at, 3, core]
        return link(block, block, sends["farther"] + at, receives["farther"] + at, above)

    def far_down(at):
        block, sent = blk.at[at, 3, core], sends["farther"] + twin(at, level)
        return link(block, block, sent, receives["farther"] + at, below)

    def share(at, q):
        block = blk.at[at, q, core]
        return link(block, block, sends["share"] + at, receives["share"] + 4 * at + q, beside)

    def shared_in(at, q):
        block = blk.at[at, q, other]
        return link(block, block, sends["share"] + at, receives["share"] + 4 * at + q, beside)

    def all_shared(at):
        blocks = blk.at[at, pl.ds(0, 4), core]
        return link(blocks, blocks, sends["share"] + at, receives["share"], beside)

    def give(at, q):
        sent, got = sends["give"] + at, receives["give"] + 4 * at + q
        return link(part.at[at, q, other], from_core.at[at, q], sent, got, beside)

    def all_given(at):
        given = part.at[at, pl.ds(0, 4), other]
        return link(given, from_core.at[at], sends["give"] + at, receives["give"], beside)

    def back_left(at):
        sent, got = sends["back"] + at, receives["back"] + at
        return link(part.at[at, 1, core], from_sides.at[at, 0], sent, got, left)

    def back_right(at):
        sent, got = sends["back"] + at, receives["back"] + at
        return link(part.at[at, 2, core], from_sides.at[at, 1], sent, got, right)

    def all_back(at):
        sent, got = sends["back"] + at, receives["back"] + at
        return link(part.at[at, pl.ds(1, 2), core], from_sides.at[at], sent, got, left)

    def sum_down(at, h):
        span, got = fourth(h), receives["sum"] + 4 * at + h
        return link(dense.at[at, span], dense_above.at[at, span], sends["sum"] + at, got, below)

    def sum_up(at, h, receiver):
        span, got = fourth(h), receives["sum"] + 4 * twin(at, receiver) + h
        return link(dense.at[at, span], dense_below.at[at, span], sends["sum"] + at, got, above)

    def all_summed(at):
        sent = sends["sum"] + at
        return link(dense.at[at], dense_above.at[at], sent, receives["sum"], below)

    def far_sum_down(at, h):
        span, sent, got = cuts[h], sends["farsum"] + at, receives["farsum"] + 2 * at + h
        return link(part.at[at, 3, core, span], far_above.at[at, span], sent, got, below)

    def far_sum_up(at, h, receiver):
        span, sent = cuts[h], sends["farsum"] + at
        got = receives["farsum"] + 2 * twin(at, receiver) + h
        return link(part.at[at, 3, core, span], far_below.at[at, span], sent, got, above)

    def all_far_summed(at):
        sent = sends["farsum"] + at
        return link(part.at[at, 3, core], far_above.at[at], sent, receives["farsum"], below)

    def pocket(at):
        return jnp.where(at == level, 0, 1)

    def home_low(at):
        n, span = pocket(at), cuts[0]
        sent, got = sends["home"] + n, receives["home"] + 2 * n
        return link(part.at[at, 3, core, span], home.at[n, span], sent, got, left)

    def home_high(at):
        n, span = pocket(at), cuts[1]
        sent, got = sends["home"] + n, receives["home"] + 2 * n + 1
        return link(part.at[at, 3, core, span], home.at[n, span], sent, got, right)

    def all_home(at):
        n = pocket(at)
        return link(part.at[at, 3, core], home.at[n], sends["home"] + n, receives["home"], left)

    def last_low(at):
        n, span = pocket(at), cuts[0]
        sent, got = sends["last"] + n, receives["last"] + n
        return link(home.at[n, span], far_back.at[n, span], sent, got, left)

    def last_high(at):
        n, span = pocket(at), cuts[1]
        sent, got = sends["last"] + n, receives["last"] + n
        return link(home.at[n, span], far_back.at[n, span], sent, got, right)

    def all_last(at):
        n = pocket(at)
        return link(home.at[n], far_back.at[n], sends["last"] + n, receives["last"] + n, left)

    def crosses(at):
        return (at == level) | (at - level >= depth - 1) | (level - at >= depth - 1)

    place = column * 2 * depth + line
    last_place = lax.axis_size("ep") * 2 * depth - 1
    first_line, last_line = line == 0, line == 2 * depth - 1
    following = (column + jnp.where(last_line, 1, 0), jnp.where(last_line, 0, line + 1))
    preceding = (column - jnp.where(first_line, 1, 0), jnp.where(first_line, 2 * depth - 1, line - 1))
    has_following, has_preceding = place < last_place, place > 0

    halo, halo_in = sends["halo"], receives["halo"]

    def to_following():
        return link(mix.at[pl.ds(rows, edge)], mix.at[pl.ds(0, edge)], halo, halo_in, following)

    def to_preceding():
        return link(
            mix.at[pl.ds(edge, edge)], mix.at[pl.ds(edge + rows, edge)], halo + 1, halo_in + 1, preceding
        )

    loads = [
        pltpu.make_async_copy(src, dst, local_sem.at[n])
        for n, (src, dst) in enumerate(zip(stored, held))
    ]
    def by_piece(start, count, width, body):
        def one(i, carry):
            body(pl.ds(pl.multiple_of(start + i * width, width), width))
            return carry

        lax.fori_loop(0, count // width, one, 0)

    barrier = pltpu.get_barrier_semaphore()

    def greet(target):
        pl.semaphore_signal(
            barrier, inc=1, device_id=target, device_id_type=pl.DeviceIdType.MESH
        )

    greet(right)
    greet(left)
    greet(beside)
    pl.when(has_above)(lambda: greet(above))
    pl.when(has_below)(lambda: greet(below))
    for load in loads:
        load.start()
    for load in loads[:4]:
        load.wait()

    def normed(values, gains):
        values = values.astype(f32)
        mean = jnp.sum(values * values, axis=1, keepdims=True) / values.shape[1]
        return (values * lax.rsqrt(mean + epsilon) * gains).astype(bf16)

    def own_rows(span):
        tok[level, span] = normed(input_ref[span], gain_ref[...])

    by_piece(0, rows, piece, own_rows)
    sort = lax.broadcasted_iota(jnp.int32, (tables.shape[1], rows), 0)
    first = sort % experts == routes_ref[0:1, :]
    second = sort % experts == routes_ref[1:2, :]
    weights = jnp.where(first, weight_ref[0:1, :], 0.0) + jnp.where(second, weight_ref[1:2, :], 0.0)
    named = first | second
    earlier = lax.broadcasted_iota(jnp.int32, (rows, rows), 0) < lax.broadcasted_iota(
        jnp.int32, (rows, rows), 1
    )
    turns = jnp.dot(
        jnp.where(named, 1.0, 0.0).astype(bf16), jnp.where(earlier, 1.0, 0.0).astype(bf16),
        preferred_element_type=f32,
    )
    turns = jnp.where(named, turns, -1.0).astype(bf16)
    coarse = weights.astype(bf16)
    fine = (weights - coarse.astype(f32)).astype(bf16)
    group = sort // experts
    listed = jnp.where(
        group == 0, turns.astype(f32), jnp.where(group == 1, coarse.astype(f32), fine.astype(f32))
    )
    tables[level, :, pl.ds(0, rows)] = listed.astype(bf16)
    tables[level, :, pl.ds(rows, tables.shape[2] - rows)] = jnp.zeros(
        (tables.shape[1], tables.shape[2] - rows), bf16
    )
    pl.semaphore_wait(barrier, 3 + jnp.where(has_above, 1, 0) + jnp.where(has_below, 1, 0))

    def table(at):
        listed = tables[at, :, pl.ds(0, rows)].astype(f32)
        listing = lax.broadcasted_iota(jnp.int32, listed.shape, 0)
        index = lax.broadcasted_iota(jnp.int32, (capacity, rows), 0).astype(f32)

        def row_of(at_row):
            return jnp.sum(jnp.where(listing == at_row, listed, 0.0), axis=0, keepdims=True)

        def hits(expert):
            return index == row_of(expert)

        return row_of, hits

    def picked(at, chosen):
        _, hits = table(at)
        picks = [jnp.where(hits(expert), 1.0, 0.0).astype(bf16) for expert in chosen]
        return jnp.dot(
            jnp.concatenate(picks, axis=0), tok[at], preferred_element_type=f32
        ).astype(bf16)

    def placed(at, chosen, results):
        row_of, hits = table(at)
        total = None
        for kind in (1, 2):
            weights = [
                jnp.where(hits(expert), row_of(kind * experts + expert), 0.0).astype(bf16)
                for expert in chosen
            ]
            term = lax.dot_general(
                jnp.concatenate(weights, axis=0), results,
                (((0,), (0,)), ((), ())), preferred_element_type=f32,
            )
            total = term if total is None else total + term
        return total

    def compute(at, q):
        gathered = jnp.concatenate([blk[at, q, 0], blk[at, q, 1]], axis=0)
        gate_part = jnp.dot(gathered, gate_ref[...], preferred_element_type=f32)
        up_part = jnp.dot(gathered, up_ref[...], preferred_element_type=f32)
        hidden = (gate_part / (1.0 + jnp.exp(-gate_part)) * up_part).astype(bf16)
        partial = jnp.dot(hidden, down_ref[...], preferred_element_type=f32).astype(bf16)
        for lane in range(2):
            part[at, q, lane] = partial[lane * capacity : (lane + 1) * capacity]

    def paired(at, q):
        give(at, q).wait_recv()

        def body(span):
            total = part[at, q, core, span].astype(f32) + from_core[at, q, span].astype(f32)
            part[at, q, core, span] = total.astype(bf16)

        by_piece(0, capacity, piece, body)

    def with_incoming(above_too, below_too, action):
        both = above_too & below_too
        pl.when(both)(lambda: action(True, True))
        pl.when(above_too & jnp.logical_not(both))(lambda: action(True, False))
        pl.when(below_too & jnp.logical_not(both))(lambda: action(False, True))
        pl.when(jnp.logical_not(above_too | below_too))(lambda: action(False, False))

    def far_total(at, h):
        above_too = (at <= level) & has_above & (level + 1 - at < depth - 1)
        below_too = (at >= level) & has_below & (at - level + 1 < depth - 1)
        over = crosses(at)
        above_too, below_too = (
            above_too & ((at == level) | jnp.logical_not(over)),
            below_too & ((at == level) | jnp.logical_not(over)),
        )
        pl.when(above_too)(lambda: far_sum_down(at, h).wait_recv())
        pl.when(below_too)(lambda: far_sum_up(at, h, level).wait_recv())

        def action(from_up, from_down):
            def body(span):
                total = part[at, 3, core, span].astype(f32) + from_core[at, 3, span].astype(f32)
                if from_up:
                    total = total + far_above[at, span].astype(f32)
                if from_down:
                    total = total + far_below[at, span].astype(f32)
                part[at, 3, core, span] = total.astype(bf16)

            by_piece((0, low)[h], (low, high)[h], step_rows, body)

        with_incoming(above_too, below_too, action)
        chained = jnp.logical_not(over)
        pl.when(chained & (at < level))(lambda: far_sum_down(at, h).start())
        pl.when(chained & (at > level))(lambda: far_sum_up(at, h, level + 1).start())
        pl.when(over)(lambda: (home_low, home_high)[h](at).start())

    def far_step(at, h):
        pl.when(h == 0)(lambda: give(at, 3).wait_recv())
        pl.when(h == 0)(lambda: far_total(at, 0))
        pl.when(h == 1)(lambda: far_total(at, 1))

    def dense_step(at, h):
        above_too, below_too = (at <= level) & has_above, (at >= level) & has_below
        pl.when(above_too)(lambda: sum_down(at, h).wait_recv())
        pl.when(below_too)(lambda: sum_up(at, h, level).wait_recv())

        def action(from_up, from_down):
            def body(span):
                total = local[at, span]
                if from_up:
                    total = total + dense_above[at, span].astype(f32)
                if from_down:
                    total = total + dense_below[at, span].astype(f32)
                dense[at, span] = total.astype(bf16)

            by_piece(h * quarter, quarter, piece, body)

        with_incoming(above_too, below_too, action)
        pl.when(at < level)(lambda: sum_down(at, h).start())
        pl.when(at > level)(lambda: sum_up(at, h, level + 1).start())

    def expand(at, _):
        give(at, 0).wait_recv()
        all_back(at).wait_recv()
        own = (part[at, 0, core].astype(f32) + from_core[at, 0].astype(f32)).astype(bf16)
        results = [own, from_sides[at, 0], from_sides[at, 1]]
        chosen = (column, right_column, left_column)
        four = crosses(at) & (at != level)

        @pl.when(four)
        def _():
            all_last(at).wait_recv()
            every = jnp.concatenate([*results, far_back[1]], axis=0)
            local[at] = placed(at, (*chosen, far_column), every)

        @pl.when(jnp.logical_not(four))
        def _():
            local[at] = placed(at, chosen, jnp.concatenate(results, axis=0))

    def arrive(at, h):
        upward, downward = (at <= level) & has_above, (at >= level) & has_below

        @pl.when(h == 0)
        def _():
            pl.when(at < level)(lambda: table_up(at).wait_recv())
            pl.when(at > level)(lambda: table_down(at).wait_recv())
            pl.when(upward)(lambda: table_up(at).start())
            pl.when(downward)(lambda: table_down(at).start())

        pl.when(at < level)(lambda: up(at, h).wait_recv())
        pl.when(at > level)(lambda: down(at, h).wait_recv())
        pl.when(upward)(lambda: up(at, h).start())
        pl.when(downward)(lambda: down(at, h).start())

    def far_out(at, _):
        out_far[...] = picked(at, (far_column,))
        far_right().start()
        far_left().start()
        for load in loads[4:7]:
            load.wait()

    def relay(at, _):
        all_far().wait_recv()
        on_right().start()
        on_left().start()

    def sides_out(at, _):
        sent = picked(at, (right_column, left_column, column))
        sides[at, 0] = sent[:capacity]
        sides[at, 1] = sent[capacity : 2 * capacity]
        to_right(at).start()
        to_left(at).start()
        blk[at, 0, core] = sent[2 * capacity :]
        share(at, 0).start()

    def sides_in(at, _):
        all_sides(at).wait_recv()
        share(at, 1).start()
        share(at, 2).start()

    def far_in(at, _):
        pl.when(at == level)(lambda: all_on().wait_recv())
        pl.when(at < level)(lambda: far_up(at).wait_recv())
        pl.when(at > level)(lambda: far_down(at).wait_recv())
        pl.when((at <= level) & has_above)(lambda: far_up(at).start())
        pl.when((at >= level) & has_below)(lambda: far_down(at).start())
        share(at, 3).start()

    def multiply(at, q):
        shared_in(at, q).wait_recv()
        compute(at, q)
        give(at, q).start()

    def back(at, q):
        paired(at, q)
        pl.when(q == 1)(lambda: back_left(at).start())
        pl.when(q == 2)(lambda: back_right(at).start())

    def home_relay(at, h):
        @pl.when(h == 0)
        def _():
            home_low(at).wait_recv()
            last_low(at).start()

        @pl.when(h == 1)
        def _():
            home_high(at).wait_recv()
            last_high(at).start()

    def finish(at, _):
        all_last(level).wait_recv()
        total = placed(level, (far_column,), far_back[0])
        out_ref[...] = (dense[level].astype(f32) + total).astype(bf16)

    def mixer_rows(at, _):
        for load in loads[7:]:
            load.wait()

        def body(i, carry):
            start = pl.multiple_of(i * piece, piece)
            values = normed(mixer_ref[pl.ds(start, piece)], mixer_gain_ref[...])
            mix[pl.ds(pl.multiple_of(start + edge, edge), piece)] = values.astype(f32)
            return carry

        lax.fori_loop(0, rows // piece, body, 0)
        zeros = jnp.zeros((edge, mix.shape[1]), f32)

        @pl.when(jnp.logical_not(has_preceding))
        def _():
            mix[pl.ds(0, edge)] = zeros

        @pl.when(jnp.logical_not(has_following))
        def _():
            mix[pl.ds(edge + rows, edge)] = zeros

        pl.when(has_following)(lambda: to_following().start())
        pl.when(has_preceding)(lambda: to_preceding().start())

    def mixer_group(number):
        width = group_ref.shape[1]
        span = pl.ds(number * width, width)
        window = 2 ** (number + 1)
        values = mix[:, span]
        length = values.shape[0]
        total = values
        for level_of_sum in range(number + 1):
            total = total + pltpu.roll(total, length - 2**level_of_sum, 0)
        total = pltpu.roll(total, window // 2, 0)[edge : edge + rows]
        position = place * rows + lax.broadcasted_iota(jnp.int32, (rows, width), 0)
        ahead = jnp.minimum(position + window // 2, (last_place + 1) * rows)
        cover = (ahead - jnp.maximum(position - window // 2, 0)).astype(f32)
        pooled = (total / cover - values[edge : edge + rows]).astype(bf16)
        product = jnp.dot(pooled, group_ref[number], preferred_element_type=f32)
        mixed_ref[:, span] = (product * mixer_scale_ref[:, span]).astype(bf16)

    def mixer_step(at, q):
        @pl.when(q == 0)
        def _():
            pl.when(has_preceding)(lambda: to_following().wait_recv())
            pl.when(has_following)(lambda: to_preceding().wait_recv())

        for number in range(4):
            pl.when(q == number)(functools.partial(mixer_group, number))

    def settle(use, copy, *more):
        pl.when(use)(lambda: copy(*more).wait_send())

    def settle_out(at, _):
        upward, downward = (at <= level) & has_above, (at >= level) & has_below
        for copy in (table_up, far_up, all_up):
            settle(upward, copy, at)
        for copy in (table_down, far_down, all_down):
            settle(downward, copy, at)
        all_sides(at).wait_send()
        all_shared(at).wait_send()

        @pl.when(at == level)
        def _():
            all_far().wait_send()
            all_on().wait_send()

    def settle_back(at, _):
        all_back(at).wait_send()
        all_given(at).wait_send()

    actions = dict(
        D=arrive, M=sides_out, I=sides_in, G=far_in,
        C=multiply, P=back, F=far_step, S=dense_step,
        E=expand, X=far_out, Y=relay, V=home_relay, Z=finish,
        H=mixer_rows, Q=mixer_step, K=settle_out, L=settle_back,
    )
    kinds = list(actions)
    words, per_word, base = coded_orders(depth, kinds)
    mirrored = level >= depth // 2
    row = jnp.where(mirrored, depth - 1 - level, level)

    def one_word(place, carry):
        word = 0
        for at, listing in enumerate(words):
            for turn, value in enumerate(listing):
                word = word + jnp.where((row == at) & (place == turn), value, 0)

        def one_step(_, rest):
            code = rest % base
            kind, at, q = code // (4 * depth), code // 4 % depth, code % 4
            at = jnp.where(mirrored, depth - 1 - at, at)
            for first in range(0, len(kinds), 4):

                @pl.when((kind >= first) & (kind < first + 4))
                def _():
                    for number in range(first, min(first + 4, len(kinds))):
                        pl.when(kind == number)(
                            functools.partial(actions[kinds[number]], at, q)
                        )

            return rest // base

        lax.fori_loop(0, per_word, one_step, word)
        return carry

    lax.fori_loop(0, len(words[0]), one_word, 0)

    def drain(at, carry):
        over = crosses(at)
        settle(at != level, all_summed, at)
        settle(jnp.logical_not(over), all_far_summed, at)
        settle(over, all_home, at)
        settle(over, all_last, at)
        return carry

    lax.fori_loop(0, depth, drain, 0)
    pl.when(has_following)(lambda: to_following().wait_send())
    pl.when(has_preceding)(lambda: to_preceding().wait_send())


def dense_plan(
    mixer_input, mixer_gain, group_weight, mixer_scale,
    expert_input, expert_gain, routes, route_weight, w_gate, w_up, w_down,
):
    row_count, width = expert_input.shape
    experts = lax.axis_size("ep")
    depth = lax.axis_size("tp") // 2
    capacity = 3 * routes.shape[1] * row_count // (2 * experts)
    pad = -(-3 * experts // 16) * 16
    lanes = -(-row_count // 128) * 128
    bf16, f32 = jnp.bfloat16, jnp.float32
    sends, receives = slot_tables(depth)
    vmem, anywhere = pl.BlockSpec(memory_space=pltpu.VMEM), pl.BlockSpec(memory_space=pl.ANY)
    compact = pltpu.VMEM((depth, capacity, width), bf16)
    dense = pltpu.VMEM((depth, row_count, width), bf16)
    held = pltpu.VMEM((row_count, width), bf16)
    stored = (
        expert_input, expert_gain.reshape(1, -1), routes.T, route_weight.T,
        w_gate[0], w_up[0], w_down[0], mixer_input, group_weight,
        mixer_gain.reshape(1, -1), mixer_scale.reshape(1, -1),
    )
    return pl.pallas_call(
        functools.partial(stream_kernel, depth, capacity, experts, len(stored)),
        out_shape=(held, held),
        in_specs=[anywhere] * len(stored),
        out_specs=(vmem, vmem),
        scratch_shapes=[
            *(pltpu.VMEM(array.shape, array.dtype) for array in stored),
            pltpu.VMEM((row_count + 2 * edge, width), f32),
            dense,
            pltpu.VMEM((depth, pad, lanes), bf16),
            pltpu.VMEM((depth, 4, 2, capacity, width), bf16),
            pltpu.VMEM((depth, 4, 2, capacity, width), bf16),
            pltpu.VMEM((depth, 4, capacity, width), bf16),
            pltpu.VMEM((depth, 2, capacity, width), bf16),
            pltpu.VMEM((capacity, width), bf16),
            pltpu.VMEM((capacity, width), bf16),
            pltpu.VMEM((depth, 2, capacity, width), bf16),
            pltpu.VMEM((depth, row_count, width), f32),
            dense,
            dense,
            dense,
            compact,
            compact,
            pltpu.VMEM((2, capacity, width), bf16),
            pltpu.VMEM((2, capacity, width), bf16),
            pltpu.SemaphoreType.DMA((sends["count"],)),
            pltpu.SemaphoreType.DMA((receives["count"],)),
            pltpu.SemaphoreType.DMA((len(stored),)),
        ],
        compiler_params=pltpu.CompilerParams(
            collective_id=0, has_side_effects=True, vmem_limit_bytes=60 * 2**20
        ),
    )(*stored)


def on_device(
    mixer_input, mixer_gain, group_weight, mixer_scale,
    expert_input, expert_gain, routes, route_weight, w_gate, w_up, w_down,
):
    devices = lax.axis_size(("ep", "tp"))
    gathered_bytes = 2 * devices * expert_input.size
    square = lax.axis_size("ep") == 4 and lax.axis_size("tp") == 4 * len(ORDERS)
    if square and gathered_bytes <= vmem_share:
        return dense_plan(
            mixer_input, mixer_gain, group_weight, mixer_scale,
            expert_input, expert_gain, routes, route_weight, w_gate, w_up, w_down,
        )
    expert_out = routed_plan(
        expert_input, expert_gain, routes, route_weight, w_gate, w_up, w_down
    )
    return (mixer(mixer_input, mixer_gain, group_weight, mixer_scale), expert_out)


def solution(mesh):
    placed = (
        P(("ep", "tp"), None),
        P(),
        P(),
        P(),
        P(("ep", "tp"), None),
        P(),
        P(("ep", "tp"), None),
        P(("ep", "tp"), None),
        P("ep", None, "tp"),
        P("ep", None, "tp"),
        P("ep", "tp", None),
    )
    return jax.shard_map(
        on_device,
        mesh=mesh,
        in_specs=placed,
        out_specs=(P(("ep", "tp"), None), P(("ep", "tp"), None)),
        check_vma=False,
    )
```

```python
import functools
import math

import jax
import jax.numpy as jnp
from jax import lax
from jax.experimental import pallas as pl
from jax.experimental.pallas import tpu as pltpu
from jax.sharding import PartitionSpec as P

epsilon = 1e-06
vmem_share = 2**24
edge = 8


def padded_2(value, sides, width):
    for axis, dim in sides:
        size, length = (lax.axis_size(axis), value.shape[dim])
        up = [(i, (i + 1) % size) for i in range(size - 1)]
        down = [(j, i) for i, j in up]
        last = lax.slice_in_dim(value, length - width, length, axis=dim)
        leading = lax.slice_in_dim(value, 0, width, axis=dim)
        before = lax.ppermute(last, axis, up)
        after = lax.ppermute(leading, axis, down)
        value = jnp.concatenate([before, value, after], axis=dim)
    return value


def normalize(row_values, gain):
    values = row_values.astype(jnp.float32)
    scaled = values * lax.rsqrt(jnp.mean(values * values, axis=-1, keepdims=True) + epsilon)
    return (scaled * gain).astype(jnp.bfloat16)


def pool_groups(padded, start_row, row_count, seq_length):
    group_width = padded.shape[1] // 4
    position = start_row + jnp.arange(row_count, dtype=jnp.int32)
    centre = padded[8 : 8 + row_count]
    pooled_parts = []
    for group_index in range(4):
        window = 2 ** (group_index + 1)
        reach_left = window // 2
        reach_right = window - 1 - reach_left
        group_cols = padded[:, group_index * group_width : (group_index + 1) * group_width]
        window_sum = group_cols[8 - reach_left : 8 - reach_left + row_count]
        for offset in range(1 - reach_left, reach_right + 1):
            window_sum = window_sum + group_cols[8 + offset : 8 + offset + row_count]
        cover = (
            jnp.minimum(position + reach_right + 1, seq_length)
            - jnp.maximum(position - reach_left, 0)
        ).astype(jnp.float32)
        pooled_parts.append(
            window_sum / cover[:, None]
            - centre[:, group_index * group_width : (group_index + 1) * group_width]
        )
    return jnp.stack(pooled_parts, axis=1).astype(jnp.bfloat16)


def mixer(mixer_input, mixer_gain, group_weight, mixer_scale):
    row_count = mixer_input.shape[0]
    normed = normalize(mixer_input, mixer_gain)
    padded = padded_2(normed, ((("ep", "tp"), 0),), 8)
    start_row = lax.axis_index(("ep", "tp")) * row_count
    seq_length = row_count * lax.axis_size(("ep", "tp"))
    pooled = pool_groups(padded.astype(jnp.float32), start_row, row_count, seq_length)
    mixed_groups = jnp.einsum(
        "tgi,gio->tgo", pooled, group_weight, preferred_element_type=jnp.float32
    )
    return (mixed_groups.reshape(row_count, -1) * mixer_scale).astype(jnp.bfloat16)


def routed_plan(expert_input, expert_gain, routes, route_weight, w_gate, w_up, w_down):
    row_count = expert_input.shape[0]
    top_count = routes.shape[1]
    experts = lax.axis_size("ep") * w_gate.shape[0]
    capacity = 3 * top_count * row_count // (2 * experts)
    normed = normalize(expert_input, expert_gain)
    flat_route = routes.reshape(-1)
    onehot = (flat_route[:, None] == jnp.arange(experts, dtype=jnp.int32)[None, :]).astype(
        jnp.int32
    )
    before = jnp.cumsum(onehot, axis=0) - onehot
    slot_index = flat_route * capacity + jnp.sum(before * onehot, axis=1)
    places = (
        slot_index.reshape(row_count, top_count)[None, :, :]
        == jnp.arange(experts * capacity, dtype=jnp.int32)[:, None, None]
    )
    dispatch = jnp.any(places, axis=2).astype(jnp.bfloat16)
    outgoing = jnp.dot(dispatch, normed, preferred_element_type=jnp.float32).astype(jnp.bfloat16)
    arrived = lax.all_to_all(outgoing, "ep", split_axis=0, concat_axis=0, tiled=True)
    down_w = w_down[0]
    paired = jnp.stack((w_gate[0], w_up[0]), axis=0)
    portion = lax.all_gather(paired, "tp", axis=2, tiled=True)
    gate_part = jnp.dot(arrived, portion[0], preferred_element_type=jnp.float32)
    up_part = jnp.dot(arrived, portion[1], preferred_element_type=jnp.float32)
    hidden = (jax.nn.silu(gate_part) * up_part).astype(jnp.bfloat16)
    block_width = down_w.shape[0]
    portion = lax.all_gather(down_w, "tp", axis=0, tiled=True)
    blocks = portion.shape[0] // block_width
    hidden_part = hidden
    hidden_part = hidden_part.reshape(hidden_part.shape[0], blocks, block_width)
    block_terms = jnp.einsum(
        "rkf,kfd->krd",
        hidden_part,
        portion.reshape(blocks, block_width, portion.shape[1]),
        preferred_element_type=jnp.float32,
    )
    rounded = lax.optimization_barrier(block_terms.astype(jnp.bfloat16)).astype(jnp.float32)
    result = jnp.sum(rounded, axis=0)
    returned = lax.all_to_all(
        result.astype(jnp.bfloat16), "ep", split_axis=0, concat_axis=0, tiled=True
    )
    picked = (
        jnp.take(returned, slot_index, axis=0).astype(jnp.float32).reshape(row_count, top_count, -1)
    )
    expert_out = jnp.sum(picked * route_weight[:, :, None], axis=1).astype(jnp.bfloat16)
    return expert_out


ORDERS = (
    (
        ("D", 0, 1), ("D", 0, 0), ("X", 0, 0), ("M", 0, 0), ("Y", 0, 0), ("D", 1, 0), ("D", 1, 1),
        ("M", 1, 0), ("I", 0, 0), ("C", 1, 0), ("G", 0, 0), ("C", 0, 2), ("C", 0, 1), ("D", 2, 0),
        ("D", 2, 1), ("M", 2, 0), ("I", 1, 0), ("K", 0, 0), ("C", 1, 1), ("D", 3, 1), ("C", 2, 0),
        ("D", 3, 0), ("M", 3, 0), ("I", 2, 0), ("C", 1, 2), ("C", 2, 1), ("C", 2, 2), ("C", 0, 3),
        ("G", 1, 0), ("P", 2, 2), ("P", 2, 1), ("I", 3, 0), ("C", 1, 3), ("C", 3, 1), ("F", 1, 0),
        ("C", 3, 2), ("F", 1, 1), ("P", 3, 1), ("K", 1, 0), ("G", 3, 0), ("C", 0, 0), ("P", 3, 2),
        ("C", 3, 3), ("E", 2, 0), ("S", 2, 3), ("C", 3, 0), ("S", 2, 2), ("S", 2, 1), ("G", 2, 0),
        ("F", 3, 0), ("F", 3, 1), ("C", 2, 3), ("F", 2, 0), ("K", 3, 0), ("V", 3, 0), ("K", 2, 0),
        ("L", 3, 0), ("V", 3, 1), ("P", 1, 2), ("F", 2, 1), ("H", 0, 0), ("S", 2, 0), ("P", 1, 1),
        ("F", 0, 0), ("E", 3, 0), ("S", 3, 1), ("S", 3, 3), ("S", 3, 2), ("F", 0, 1), ("S", 3, 0),
        ("Q", 0, 0), ("P", 0, 2), ("Q", 0, 3), ("E", 1, 0), ("S", 1, 1), ("P", 0, 1), ("V", 0, 1),
        ("S", 1, 3), ("L", 2, 0), ("L", 1, 0), ("S", 1, 0), ("V", 0, 0), ("Q", 0, 2), ("Q", 0, 1),
        ("S", 1, 2), ("E", 0, 0), ("S", 0, 1), ("S", 0, 3), ("S", 0, 2), ("L", 0, 0), ("S", 0, 0),
        ("Z", 0, 0),
    ),
    (
        ("D", 1, 0), ("D", 1, 1), ("X", 1, 0), ("M", 1, 0), ("D", 0, 1), ("C", 1, 0), ("Y", 1, 0),
        ("D", 2, 0), ("D", 0, 0), ("D", 2, 1), ("M", 2, 0), ("M", 0, 0), ("I", 1, 0), ("D", 3, 1),
        ("C", 1, 1), ("C", 1, 2), ("D", 3, 0), ("C", 2, 0), ("M", 3, 0), ("P", 1, 2), ("I", 2, 0),
        ("C", 3, 0), ("G", 0, 0), ("P", 1, 1), ("C", 2, 2), ("G", 1, 0), ("C", 2, 1), ("I", 0, 0),
        ("C", 0, 0), ("C", 0, 2), ("G", 3, 0), ("C", 0, 1), ("P", 2, 2), ("I", 3, 0), ("C", 3, 3),
        ("C", 0, 3), ("P", 0, 2), ("C", 3, 2), ("G", 2, 0), ("F", 3, 0), ("P", 2, 1), ("F", 3, 1),
        ("P", 0, 1), ("C", 3, 1), ("P", 3, 1), ("K", 1, 0), ("C", 1, 3), ("L", 1, 0), ("C", 2, 3),
        ("K", 3, 0), ("F", 0, 0), ("E", 1, 0), ("F", 0, 1), ("K", 2, 0), ("E", 2, 0), ("H", 1, 0),
        ("S", 2, 3), ("L", 2, 0), ("P", 3, 2), ("S", 2, 1), ("S", 2, 2), ("F", 2, 0), ("F", 2, 1),
        ("E", 3, 0), ("L", 0, 0), ("Q", 1, 0), ("E", 0, 0), ("K", 0, 0), ("F", 1, 0), ("L", 3, 0),
        ("S", 3, 1), ("Q", 1, 2), ("Q", 1, 1), ("F", 1, 1), ("S", 3, 3), ("S", 3, 2), ("S", 0, 1),
        ("V", 1, 0), ("S", 3, 0), ("S", 0, 3), ("S", 0, 2), ("S", 1, 1), ("S", 2, 0), ("V", 1, 1),
        ("Q", 1, 3), ("S", 0, 0), ("S", 1, 3), ("S", 1, 0), ("S", 1, 2), ("Z", 1, 0),
    ),
)


def coded_orders(depth, kinds):
    depth_bits = (depth - 1).bit_length()
    base = 1 << (len(kinds) << (2 + depth_bits)).bit_length()
    per_word = 1
    while base ** (per_word + 1) < 2**31:
        per_word += 1
    idle = base - 1
    longest = max(map(len, ORDERS))
    longest += -longest % per_word
    words = []
    for order in ORDERS:
        codes = [((kinds.index(kind) << depth_bits) + at) * 4 + q for kind, at, q in order]
        codes += [idle] * (longest - len(codes))
        words.append([
            sum(code * base**n for n, code in enumerate(codes[first : first + per_word]))
            for first in range(0, len(codes), per_word)
        ])
    return words, per_word, base


def slot_tables(depth):
    def offsets(**sizes):
        table, count = {}, 0
        for name, size in sizes.items():
            table[name], count = count, count + size
        return dict(table, count=count)

    sends = offsets(
        rows=depth + 1, table=depth + 1, farther=depth + 1, sides=depth, share=depth,
        give=depth, back=depth, sum=depth, farsum=depth, far=1, on=1, home=2, last=2, halo=2,
    )
    receives = offsets(
        rows=2 * depth, table=depth, farther=depth, sides=depth, share=4 * depth,
        give=4 * depth, back=depth, sum=4 * depth + 4, farsum=2 * depth + 2,
        far=1, on=1, home=4, last=2, halo=2,
    )
    return sends, receives


def stream_kernel(
    depth, capacity, experts, stores,
    *refs,
):
    stored, refs = refs[:stores], refs[stores:]
    mixed_ref, out_ref, *refs = refs
    held, refs = refs[:stores], refs[stores:]
    (
        input_ref, gain_ref, routes_ref, weight_ref, gate_ref, up_ref, down_ref,
        mixer_ref, group_ref, mixer_gain_ref, mixer_scale_ref,
    ) = held
    (
        mix, tok, tables, blk, part, from_core, sides, out_far, passing,
        from_sides, local, dense, dense_above, dense_below,
        far_above, far_below, home, far_back,
        send_sem, recv_sem, local_sem,
    ) = refs
    column, line = lax.axis_index("ep"), lax.axis_index("tp")
    level, core = line // 2, line % 2
    other = 1 - core
    rows = out_ref.shape[0]
    half, quarter = rows // 2, rows // 4
    low = -(-capacity // 32) * 16
    high = capacity - low
    piece = math.gcd(quarter, capacity)
    step_rows = math.gcd(low, high)
    right_column, left_column, far_column = (2 * column + 1) % 5, (3 * column + 2) % 5, 3 - column
    right, left = (right_column, line), (left_column, line)
    beside = (column, level * 2 + other)
    above, below = (column, line + 2), (column, line - 2)
    has_above, has_below = level < depth - 1, level > 0
    f32, bf16 = jnp.float32, jnp.bfloat16

    def link(src, dst, sent, got, target):
        return pltpu.make_async_remote_copy(
            src_ref=src, dst_ref=dst, send_sem=send_sem.at[sent],
            recv_sem=recv_sem.at[got], device_id=target,
            device_id_type=pl.DeviceIdType.MESH,
        )

    sends, receives = slot_tables(depth)

    def twin(at, where):
        return jnp.where(at == where, depth, at)

    def part_of(h):
        return pl.ds(pl.multiple_of(h * half, half), half)

    def fourth(h):
        return pl.ds(pl.multiple_of(h * quarter, quarter), quarter)

    cuts = (pl.ds(0, low), pl.ds(low, high))

    def up(at, h):
        span = tok.at[at, part_of(h)]
        return link(span, span, sends["rows"] + at, receives["rows"] + 2 * at + h, above)

    def down(at, h):
        span, sent = tok.at[at, part_of(h)], sends["rows"] + twin(at, level)
        return link(span, span, sent, receives["rows"] + 2 * at + h, below)

    def all_up(at):
        return link(tok.at[at], tok.at[at], sends["rows"] + at, receives["rows"], above)

    def all_down(at):
        sent = sends["rows"] + twin(at, level)
        return link(tok.at[at], tok.at[at], sent, receives["rows"], below)

    def table_up(at):
        table = tables.at[at]
        return link(table, table, sends["table"] + at, receives["table"] + at, above)

    def table_down(at):
        table, sent = tables.at[at], sends["table"] + twin(at, level)
        return link(table, table, sent, receives["table"] + at, below)

    def to_right(at):
        sent, got = sends["sides"] + at, receives["sides"] + at
        return link(sides.at[at, 0], blk.at[at, 1, core], sent, got, right)

    def to_left(at):
        sent, got = sends["sides"] + at, receives["sides"] + at
        return link(sides.at[at, 1], blk.at[at, 2, core], sent, got, left)

    def all_sides(at):
        sent, got = sends["sides"] + at, receives["sides"] + at
        return link(sides.at[at], blk.at[at, pl.ds(1, 2), core], sent, got, right)

    def far_right():
        span = cuts[0]
        return link(out_far.at[span], passing.at[span], sends["far"], receives["far"], right)

    def far_left():
        span = cuts[1]
        return link(out_far.at[span], passing.at[span], sends["far"], receives["far"], left)

    def all_far():
        return link(out_far, passing, sends["far"], receives["far"], right)

    def on_right():
        there = blk.at[level, 3, core, cuts[0]]
        return link(passing.at[cuts[0]], there, sends["on"], receives["on"], right)

    def on_left():
        there = blk.at[level, 3, core, cuts[1]]
        return link(passing.at[cuts[1]], there, sends["on"], receives["on"], left)

    def all_on():
        return link(passing, blk.at[level, 3, core], sends["on"], receives["on"], right)

    def far_up(at):
        block = blk.at[at, 3, core]
        return link(block, block, sends["farther"] + at, receives["farther"] + at, above)

    def far_down(at):
        block, sent = blk.at[at, 3, core], sends["farther"] + twin(at, level)
        return link(block, block, sent, receives["farther"] + at, below)

    def share(at, q):
        block = blk.at[at, q, core]
        return link(block, block, sends["share"] + at, receives["share"] + 4 * at + q, beside)

    def shared_in(at, q):
        block = blk.at[at, q, other]
        return link(block, block, sends["share"] + at, receives["share"] + 4 * at + q, beside)

    def all_shared(at):
        blocks = blk.at[at, pl.ds(0, 4), core]
        return link(blocks, blocks, sends["share"] + at, receives["share"], beside)

    def give(at, q):
        sent, got = sends["give"] + at, receives["give"] + 4 * at + q
        return link(part.at[at, q, other], from_core.at[at, q], sent, got, beside)

    def all_given(at):
        given = part.at[at, pl.ds(0, 4), other]
        return link(given, from_core.at[at], sends["give"] + at, receives["give"], beside)

    def back_left(at):
        sent, got = sends["back"] + at, receives["back"] + at
        return link(part.at[at, 1, core], from_sides.at[at, 0], sent, got, left)

    def back_right(at):
        sent, got = sends["back"] + at, receives["back"] + at
        return link(part.at[at, 2, core], from_sides.at[at, 1], sent, got, right)

    def all_back(at):
        sent, got = sends["back"] + at, receives["back"] + at
        return link(part.at[at, pl.ds(1, 2), core], from_sides.at[at], sent, got, left)

    def sum_down(at, h):
        span, got = fourth(h), receives["sum"] + 4 * at + h
        return link(dense.at[at, span], dense_above.at[at, span], sends["sum"] + at, got, below)

    def sum_up(at, h, receiver):
        span, got = fourth(h), receives["sum"] + 4 * twin(at, receiver) + h
        return link(dense.at[at, span], dense_below.at[at, span], sends["sum"] + at, got, above)

    def all_summed(at):
        sent = sends["sum"] + at
        return link(dense.at[at], dense_above.at[at], sent, receives["sum"], below)

    def far_sum_down(at, h):
        span, sent, got = cuts[h], sends["farsum"] + at, receives["farsum"] + 2 * at + h
        return link(part.at[at, 3, core, span], far_above.at[at, span], sent, got, below)

    def far_sum_up(at, h, receiver):
        span, sent = cuts[h], sends["farsum"] + at
        got = receives["farsum"] + 2 * twin(at, receiver) + h
        return link(part.at[at, 3, core, span], far_below.at[at, span], sent, got, above)

    def all_far_summed(at):
        sent = sends["farsum"] + at
        return link(part.at[at, 3, core], far_above.at[at], sent, receives["farsum"], below)

    def pocket(at):
        return jnp.where(at == level, 0, 1)

    def home_low(at):
        n, span = pocket(at), cuts[0]
        sent, got = sends["home"] + n, receives["home"] + 2 * n
        return link(part.at[at, 3, core, span], home.at[n, span], sent, got, left)

    def home_high(at):
        n, span = pocket(at), cuts[1]
        sent, got = sends["home"] + n, receives["home"] + 2 * n + 1
        return link(part.at[at, 3, core, span], home.at[n, span], sent, got, right)

    def all_home(at):
        n = pocket(at)
        return link(part.at[at, 3, core], home.at[n], sends["home"] + n, receives["home"], left)

    def last_low(at):
        n, span = pocket(at), cuts[0]
        sent, got = sends["last"] + n, receives["last"] + n
        return link(home.at[n, span], far_back.at[n, span], sent, got, left)

    def last_high(at):
        n, span = pocket(at), cuts[1]
        sent, got = sends["last"] + n, receives["last"] + n
        return link(home.at[n, span], far_back.at[n, span], sent, got, right)

    def all_last(at):
        n = pocket(at)
        return link(home.at[n], far_back.at[n], sends["last"] + n, receives["last"] + n, left)

    def crosses(at):
        return (at == level) | (at - level >= depth - 1) | (level - at >= depth - 1)

    place = column * 2 * depth + line
    last_place = lax.axis_size("ep") * 2 * depth - 1
    first_line, last_line = line == 0, line == 2 * depth - 1
    following = (column + jnp.where(last_line, 1, 0), jnp.where(last_line, 0, line + 1))
    preceding = (column - jnp.where(first_line, 1, 0), jnp.where(first_line, 2 * depth - 1, line - 1))
    has_following, has_preceding = place < last_place, place > 0

    halo, halo_in = sends["halo"], receives["halo"]

    def to_following():
        return link(mix.at[pl.ds(rows, edge)], mix.at[pl.ds(0, edge)], halo, halo_in, following)

    def to_preceding():
        return link(
            mix.at[pl.ds(edge, edge)], mix.at[pl.ds(edge + rows, edge)], halo + 1, halo_in + 1, preceding
        )

    loads = [
        pltpu.make_async_copy(src, dst, local_sem.at[n])
        for n, (src, dst) in enumerate(zip(stored, held))
    ]
    def by_piece(start, count, width, body):
        def one(i, carry):
            body(pl.ds(pl.multiple_of(start + i * width, width), width))
            return carry

        lax.fori_loop(0, count // width, one, 0)

    barrier = pltpu.get_barrier_semaphore()

    def greet(target):
        pl.semaphore_signal(
            barrier, inc=1, device_id=target, device_id_type=pl.DeviceIdType.MESH
        )

    greet(right)
    greet(left)
    greet(beside)
    pl.when(has_above)(lambda: greet(above))
    pl.when(has_below)(lambda: greet(below))
    for load in loads:
        load.start()
    for load in loads[:4]:
        load.wait()

    def normed(values, gains):
        values = values.astype(f32)
        mean = jnp.sum(values * values, axis=1, keepdims=True) / values.shape[1]
        return (values * lax.rsqrt(mean + epsilon) * gains).astype(bf16)

    def own_rows(span):
        tok[level, span] = normed(input_ref[span], gain_ref[...])

    by_piece(0, rows, piece, own_rows)
    sort = lax.broadcasted_iota(jnp.int32, (tables.shape[1], rows), 0)
    first = sort % experts == routes_ref[0:1, :]
    second = sort % experts == routes_ref[1:2, :]
    weights = jnp.where(first, weight_ref[0:1, :], 0.0) + jnp.where(second, weight_ref[1:2, :], 0.0)
    named = first | second
    earlier = lax.broadcasted_iota(jnp.int32, (rows, rows), 0) < lax.broadcasted_iota(
        jnp.int32, (rows, rows), 1
    )
    turns = jnp.dot(
        jnp.where(named, 1.0, 0.0).astype(bf16), jnp.where(earlier, 1.0, 0.0).astype(bf16),
        preferred_element_type=f32,
    )
    turns = jnp.where(named, turns, -1.0).astype(bf16)
    coarse = weights.astype(bf16)
    fine = (weights - coarse.astype(f32)).astype(bf16)
    group = sort // experts
    listed = jnp.where(
        group == 0, turns.astype(f32), jnp.where(group == 1, coarse.astype(f32), fine.astype(f32))
    )
    tables[level, :, pl.ds(0, rows)] = listed.astype(bf16)
    tables[level, :, pl.ds(rows, tables.shape[2] - rows)] = jnp.zeros(
        (tables.shape[1], tables.shape[2] - rows), bf16
    )
    pl.semaphore_wait(barrier, 3 + jnp.where(has_above, 1, 0) + jnp.where(has_below, 1, 0))

    def table(at):
        listed = tables[at, :, pl.ds(0, rows)].astype(f32)
        listing = lax.broadcasted_iota(jnp.int32, listed.shape, 0)
        index = lax.broadcasted_iota(jnp.int32, (capacity, rows), 0).astype(f32)

        def row_of(at_row):
            return jnp.sum(jnp.where(listing == at_row, listed, 0.0), axis=0, keepdims=True)

        def hits(expert):
            return index == row_of(expert)

        return row_of, hits

    def picked(at, chosen):
        _, hits = table(at)
        picks = [jnp.where(hits(expert), 1.0, 0.0).astype(bf16) for expert in chosen]
        return jnp.dot(
            jnp.concatenate(picks, axis=0), tok[at], preferred_element_type=f32
        ).astype(bf16)

    def placed(at, chosen, results):
        row_of, hits = table(at)
        total = None
        for kind in (1, 2):
            weights = [
                jnp.where(hits(expert), row_of(kind * experts + expert), 0.0).astype(bf16)
                for expert in chosen
            ]
            term = lax.dot_general(
                jnp.concatenate(weights, axis=0), results,
                (((0,), (0,)), ((), ())), preferred_element_type=f32,
            )
            total = term if total is None else total + term
        return total

    def compute(at, q):
        gathered = jnp.concatenate([blk[at, q, 0], blk[at, q, 1]], axis=0)
        gate_part = jnp.dot(gathered, gate_ref[...], preferred_element_type=f32)
        up_part = jnp.dot(gathered, up_ref[...], preferred_element_type=f32)
        hidden = (gate_part / (1.0 + jnp.exp(-gate_part)) * up_part).astype(bf16)
        partial = jnp.dot(hidden, down_ref[...], preferred_element_type=f32).astype(bf16)
        for lane in range(2):
            part[at, q, lane] = partial[lane * capacity : (lane + 1) * capacity]

    def paired(at, q):
        give(at, q).wait_recv()

        def body(span):
            total = part[at, q, core, span].astype(f32) + from_core[at, q, span].astype(f32)
            part[at, q, core, span] = total.astype(bf16)

        by_piece(0, capacity, piece, body)

    def with_incoming(above_too, below_too, action):
        both = above_too & below_too
        pl.when(both)(lambda: action(True, True))
        pl.when(above_too & jnp.logical_not(both))(lambda: action(True, False))
        pl.when(below_too & jnp.logical_not(both))(lambda: action(False, True))
        pl.when(jnp.logical_not(above_too | below_too))(lambda: action(False, False))

    def far_total(at, h):
        above_too = (at <= level) & has_above & (level + 1 - at < depth - 1)
        below_too = (at >= level) & has_below & (at - level + 1 < depth - 1)
        over = crosses(at)
        above_too, below_too = (
            above_too & ((at == level) | jnp.logical_not(over)),
            below_too & ((at == level) | jnp.logical_not(over)),
        )
        pl.when(above_too)(lambda: far_sum_down(at, h).wait_recv())
        pl.when(below_too)(lambda: far_sum_up(at, h, level).wait_recv())

        def action(from_up, from_down):
            def body(span):
                total = part[at, 3, core, span].astype(f32) + from_core[at, 3, span].astype(f32)
                if from_up:
                    total = total + far_above[at, span].astype(f32)
                if from_down:
                    total = total + far_below[at, span].astype(f32)
                part[at, 3, core, span] = total.astype(bf16)

            by_piece((0, low)[h], (low, high)[h], step_rows, body)

        with_incoming(above_too, below_too, action)
        chained = jnp.logical_not(over)
        pl.when(chained & (at < level))(lambda: far_sum_down(at, h).start())
        pl.when(chained & (at > level))(lambda: far_sum_up(at, h, level + 1).start())
        pl.when(over)(lambda: (home_low, home_high)[h](at).start())

    def far_step(at, h):
        pl.when(h == 0)(lambda: give(at, 3).wait_recv())
        pl.when(h == 0)(lambda: far_total(at, 0))
        pl.when(h == 1)(lambda: far_total(at, 1))

    def dense_step(at, h):
        above_too, below_too = (at <= level) & has_above, (at >= level) & has_below
        pl.when(above_too)(lambda: sum_down(at, h).wait_recv())
        pl.when(below_too)(lambda: sum_up(at, h, level).wait_recv())

        def action(from_up, from_down):
            def body(span):
                total = local[at, span]
                if from_up:
                    total = total + dense_above[at, span].astype(f32)
                if from_down:
                    total = total + dense_below[at, span].astype(f32)
                dense[at, span] = total.astype(bf16)

            by_piece(h * quarter, quarter, piece, body)

        with_incoming(above_too, below_too, action)
        pl.when(at < level)(lambda: sum_down(at, h).start())
        pl.when(at > level)(lambda: sum_up(at, h, level + 1).start())

    def expand(at, _):
        give(at, 0).wait_recv()
        all_back(at).wait_recv()
        own = (part[at, 0, core].astype(f32) + from_core[at, 0].astype(f32)).astype(bf16)
        results = [own, from_sides[at, 0], from_sides[at, 1]]
        chosen = (column, right_column, left_column)
        four = crosses(at) & (at != level)

        @pl.when(four)
        def _():
            all_last(at).wait_recv()
            every = jnp.concatenate([*results, far_back[1]], axis=0)
            local[at] = placed(at, (*chosen, far_column), every)

        @pl.when(jnp.logical_not(four))
        def _():
            local[at] = placed(at, chosen, jnp.concatenate(results, axis=0))

    def arrive(at, h):
        upward, downward = (at <= level) & has_above, (at >= level) & has_below

        @pl.when(h == 0)
        def _():
            pl.when(at < level)(lambda: table_up(at).wait_recv())
            pl.when(at > level)(lambda: table_down(at).wait_recv())
            pl.when(upward)(lambda: table_up(at).start())
            pl.when(downward)(lambda: table_down(at).start())

        pl.when(at < level)(lambda: up(at, h).wait_recv())
        pl.when(at > level)(lambda: down(at, h).wait_recv())
        pl.when(upward)(lambda: up(at, h).start())
        pl.when(downward)(lambda: down(at, h).start())

    def far_out(at, _):
        out_far[...] = picked(at, (far_column,))
        far_right().start()
        far_left().start()
        for load in loads[4:7]:
            load.wait()

    def relay(at, _):
        all_far().wait_recv()
        on_right().start()
        on_left().start()

    def sides_out(at, _):
        sent = picked(at, (right_column, left_column, column))
        sides[at, 0] = sent[:capacity]
        sides[at, 1] = sent[capacity : 2 * capacity]
        to_right(at).start()
        to_left(at).start()
        blk[at, 0, core] = sent[2 * capacity :]
        share(at, 0).start()

    def sides_in(at, _):
        all_sides(at).wait_recv()
        share(at, 1).start()
        share(at, 2).start()

    def far_in(at, _):
        pl.when(at == level)(lambda: all_on().wait_recv())
        pl.when(at < level)(lambda: far_up(at).wait_recv())
        pl.when(at > level)(lambda: far_down(at).wait_recv())
        pl.when((at <= level) & has_above)(lambda: far_up(at).start())
        pl.when((at >= level) & has_below)(lambda: far_down(at).start())
        share(at, 3).start()

    def multiply(at, q):
        shared_in(at, q).wait_recv()
        compute(at, q)
        give(at, q).start()

    def back(at, q):
        paired(at, q)
        pl.when(q == 1)(lambda: back_left(at).start())
        pl.when(q == 2)(lambda: back_right(at).start())

    def home_relay(at, h):
        @pl.when(h == 0)
        def _():
            home_low(at).wait_recv()
            last_low(at).start()

        @pl.when(h == 1)
        def _():
            home_high(at).wait_recv()
            last_high(at).start()

    def finish(at, _):
        all_last(level).wait_recv()
        total = placed(level, (far_column,), far_back[0])
        out_ref[...] = (dense[level].astype(f32) + total).astype(bf16)

    def mixer_rows(at, _):
        for load in loads[7:]:
            load.wait()

        def body(i, carry):
            start = pl.multiple_of(i * piece, piece)
            values = normed(mixer_ref[pl.ds(start, piece)], mixer_gain_ref[...])
            mix[pl.ds(pl.multiple_of(start + edge, edge), piece)] = values.astype(f32)
            return carry

        lax.fori_loop(0, rows // piece, body, 0)
        zeros = jnp.zeros((edge, mix.shape[1]), f32)

        @pl.when(jnp.logical_not(has_preceding))
        def _():
            mix[pl.ds(0, edge)] = zeros

        @pl.when(jnp.logical_not(has_following))
        def _():
            mix[pl.ds(edge + rows, edge)] = zeros

        pl.when(has_following)(lambda: to_following().start())
        pl.when(has_preceding)(lambda: to_preceding().start())

    def mixer_group(number):
        width = group_ref.shape[1]
        span = pl.ds(number * width, width)
        window = 2 ** (number + 1)
        values = mix[:, span]
        length = values.shape[0]
        total = values
        for level_of_sum in range(number + 1):
            total = total + pltpu.roll(total, length - 2**level_of_sum, 0)
        total = pltpu.roll(total, window // 2, 0)[edge : edge + rows]
        position = place * rows + lax.broadcasted_iota(jnp.int32, (rows, width), 0)
        ahead = jnp.minimum(position + window // 2, (last_place + 1) * rows)
        cover = (ahead - jnp.maximum(position - window // 2, 0)).astype(f32)
        pooled = (total / cover - values[edge : edge + rows]).astype(bf16)
        product = jnp.dot(pooled, group_ref[number], preferred_element_type=f32)
        mixed_ref[:, span] = (product * mixer_scale_ref[:, span]).astype(bf16)

    def mixer_step(at, q):
        @pl.when(q == 0)
        def _():
            pl.when(has_preceding)(lambda: to_following().wait_recv())
            pl.when(has_following)(lambda: to_preceding().wait_recv())

        for number in range(4):
            pl.when(q == number)(functools.partial(mixer_group, number))

    def settle(use, copy, *more):
        pl.when(use)(lambda: copy(*more).wait_send())

    def settle_out(at, _):
        upward, downward = (at <= level) & has_above, (at >= level) & has_below
        for copy in (table_up, far_up, all_up):
            settle(upward, copy, at)
        for copy in (table_down, far_down, all_down):
            settle(downward, copy, at)
        all_sides(at).wait_send()
        all_shared(at).wait_send()

        @pl.when(at == level)
        def _():
            all_far().wait_send()
            all_on().wait_send()

    def settle_back(at, _):
        all_back(at).wait_send()
        all_given(at).wait_send()

    actions = dict(
        D=arrive, M=sides_out, I=sides_in, G=far_in,
        C=multiply, P=back, F=far_step, S=dense_step,
        E=expand, X=far_out, Y=relay, V=home_relay, Z=finish,
        H=mixer_rows, Q=mixer_step, K=settle_out, L=settle_back,
    )
    kinds = list(actions)
    words, per_word, base = coded_orders(depth, kinds)
    mirrored = level >= depth // 2
    row = jnp.where(mirrored, depth - 1 - level, level)

    depth_bits = (depth - 1).bit_length()

    def chosen_word(turn):
        level_words = [
            functools.reduce(
                lambda found, at: jnp.where(row == at, words[at][n], found),
                range(1, len(words)), words[0][n],
            )
            for n in range(len(words[0]))
        ]
        bit = 1
        while len(level_words) > 1:
            odd = lax.rem(lax.div(turn, bit), 2) == 1
            pairs = zip(level_words[::2], level_words[1::2] + level_words[-1:])
            level_words = [jnp.where(odd, late, soon) for soon, late in pairs]
            bit *= 2
        return level_words[0]

    def one_word(turn, carry):
        def one_step(_, rest):
            code = lax.rem(rest, base)
            kind = lax.div(code, 4 << depth_bits)
            at, q = lax.rem(lax.div(code, 4), 1 << depth_bits), lax.rem(code, 4)
            at = jnp.where(mirrored, depth - 1 - at, at)
            for first in range(0, len(kinds), 4):

                @pl.when((kind >= first) & (kind < first + 4))
                def _():
                    for number in range(first, min(first + 4, len(kinds))):
                        pl.when(kind == number)(
                            functools.partial(actions[kinds[number]], at, q)
                        )

            return lax.div(rest, base)

        lax.fori_loop(0, per_word, one_step, chosen_word(turn))
        return carry

    lax.fori_loop(0, len(words[0]), one_word, 0)

    def drain(at, carry):
        over = crosses(at)
        settle(at != level, all_summed, at)
        settle(jnp.logical_not(over), all_far_summed, at)
        settle(over, all_home, at)
        settle(over, all_last, at)
        return carry

    lax.fori_loop(0, depth, drain, 0)
    pl.when(has_following)(lambda: to_following().wait_send())
    pl.when(has_preceding)(lambda: to_preceding().wait_send())


def dense_plan(
    mixer_input, mixer_gain, group_weight, mixer_scale,
    expert_input, expert_gain, routes, route_weight, w_gate, w_up, w_down,
):
    row_count, width = expert_input.shape
    experts = lax.axis_size("ep")
    depth = lax.axis_size("tp") // 2
    capacity = 3 * routes.shape[1] * row_count // (2 * experts)
    pad = -(-3 * experts // 16) * 16
    lanes = -(-row_count // 128) * 128
    bf16, f32 = jnp.bfloat16, jnp.float32
    sends, receives = slot_tables(depth)
    vmem, anywhere = pl.BlockSpec(memory_space=pltpu.VMEM), pl.BlockSpec(memory_space=pl.ANY)
    compact = pltpu.VMEM((depth, capacity, width), bf16)
    dense = pltpu.VMEM((depth, row_count, width), bf16)
    held = pltpu.VMEM((row_count, width), bf16)
    stored = (
        expert_input, expert_gain.reshape(1, -1), routes.T, route_weight.T,
        w_gate[0], w_up[0], w_down[0], mixer_input, group_weight,
        mixer_gain.reshape(1, -1), mixer_scale.reshape(1, -1),
    )
    return pl.pallas_call(
        functools.partial(stream_kernel, depth, capacity, experts, len(stored)),
        out_shape=(held, held),
        in_specs=[anywhere] * len(stored),
        out_specs=(vmem, vmem),
        scratch_shapes=[
            *(pltpu.VMEM(array.shape, array.dtype) for array in stored),
            pltpu.VMEM((row_count + 2 * edge, width), f32),
            dense,
            pltpu.VMEM((depth, pad, lanes), bf16),
            pltpu.VMEM((depth, 4, 2, capacity, width), bf16),
            pltpu.VMEM((depth, 4, 2, capacity, width), bf16),
            pltpu.VMEM((depth, 4, capacity, width), bf16),
            pltpu.VMEM((depth, 2, capacity, width), bf16),
            pltpu.VMEM((capacity, width), bf16),
            pltpu.VMEM((capacity, width), bf16),
            pltpu.VMEM((depth, 2, capacity, width), bf16),
            pltpu.VMEM((depth, row_count, width), f32),
            dense,
            dense,
            dense,
            compact,
            compact,
            pltpu.VMEM((2, capacity, width), bf16),
            pltpu.VMEM((2, capacity, width), bf16),
            pltpu.SemaphoreType.DMA((sends["count"],)),
            pltpu.SemaphoreType.DMA((receives["count"],)),
            pltpu.SemaphoreType.DMA((len(stored),)),
        ],
        compiler_params=pltpu.CompilerParams(
            collective_id=0, has_side_effects=True, vmem_limit_bytes=60 * 2**20
        ),
    )(*stored)


def on_device(
    mixer_input, mixer_gain, group_weight, mixer_scale,
    expert_input, expert_gain, routes, route_weight, w_gate, w_up, w_down,
):
    devices = lax.axis_size(("ep", "tp"))
    gathered_bytes = 2 * devices * expert_input.size
    square = lax.axis_size("ep") == 4 and lax.axis_size("tp") == 4 * len(ORDERS)
    if square and gathered_bytes <= vmem_share:
        return dense_plan(
            mixer_input, mixer_gain, group_weight, mixer_scale,
            expert_input, expert_gain, routes, route_weight, w_gate, w_up, w_down,
        )
    expert_out = routed_plan(
        expert_input, expert_gain, routes, route_weight, w_gate, w_up, w_down
    )
    return (mixer(mixer_input, mixer_gain, group_weight, mixer_scale), expert_out)


def solution(mesh):
    placed = (
        P(("ep", "tp"), None),
        P(),
        P(),
        P(),
        P(("ep", "tp"), None),
        P(),
        P(("ep", "tp"), None),
        P(("ep", "tp"), None),
        P("ep", None, "tp"),
        P("ep", None, "tp"),
        P("ep", "tp", None),
    )
    return jax.shard_map(
        on_device,
        mesh=mesh,
        in_specs=placed,
        out_specs=(P(("ep", "tp"), None), P(("ep", "tp"), None)),
        check_vma=False,
    )
```
